32 devices in a mesh: grp: 2 (over x), sp: 4 (over y, core), tp: 4 (over z).
Axes of the slice: x: 2, y: 2, z: 4, core: 2. Of those that a mesh axis runs over, the one named last changes fastest.
Arguments:
- resid_in: bfloat16 [4096, 2048], P(('grp', 'sp', 'tp')), parts along dimension 0, may hold values from -6 to 6
- pool_input: bfloat16 [4096, 1024], P(('grp', 'sp'), 'tp'), parts along dimension 0, may hold values from -6 to 6
- pool_weight: bfloat16 [4, 256, 256], replicated, may hold values from -0.375 to 0.375
- pool_scale: float32 [1024], replicated, may hold values from 0.2 to 0.8
- out_weight: bfloat16 [1024, 2048], replicated, may hold values from -0.1875 to 0.1875
- mix_gain: float32 [2048], replicated, may hold values from 0.1 to 1.9
- ffn_gain: float32 [2048], replicated, may hold values from 0.1 to 1.9
- w_gate: bfloat16 [32, 2048, 1024], P('sp', None, 'tp'), may hold values from -0.375 to 0.375
- w_up: bfloat16 [32, 2048, 1024], P('sp', None, 'tp'), may hold values from -0.375 to 0.375
- w_down: bfloat16 [32, 1024, 2048], P('sp', 'tp'), may hold values from -0.1875 to 0.1875
- routes: int32 [4096, 2], P(('grp', 'sp', 'tp')), parts along dimension 0, may hold values from 0 to 31, all different within a row; in each aligned block of 128 rows (0 to 127, 128 to 255, ...) at most 9 rows name the same one
- route_weight: float32 [4096, 2], P(('grp', 'sp', 'tp')), parts along dimension 0, may hold values from 0.1 to 1
- post_gain: float32 [2048], replicated, may hold values from 0.1 to 1.9
Outputs:
- layer_out: bfloat16 [4096, 2048], P(('grp', 'sp', 'tp')), parts along dimension 0
The draws below stay inside these ranges and needn't reach their ends.
There are 2 independent parts, one for each index of `grp`. The reference program is written for one: setup_inputs(seed, part) draws one part's arguments, and reference() takes and returns one part's arrays. A program takes and returns all parts, laid end to end along the dimension named above; an argument that names none is the same for every part. Nothing has to cross between parts.
Inputs may be any that keep to these rules, and one draw needn't show every extreme that they name: `routes`: each row names 2 different experts. The rows of one device name any one expert at most 9 times, and in every draw some device's rows name some expert exactly 9 times.
All inputs are finite; a program needn't handle non-finite values.
Results may differ from the reference program's by a relative error of at most 0.011.
Values may be sent and summed in bfloat16 or wider, within the bound.
A program may use at most 128 MiB of HBM per device.

```python
import math
import jax
import jax.numpy as jnp
import numpy as np
from jax import lax

D = 2048
POOL_WIDTH = 1024
GROUPS = 4
GROUP_DIM = 256
FF = 1024
EXPERTS = 32
TOP = 2
TOK_DEV = 128
CAP = 9
SEQ = 2048
N_TP = 4


def shard_levels(key, shape, cuts, smallest, high):
    gain, own = 1.0, jax.random.fold_in(key, 6)
    for axis_at, shards_of in cuts:
        draws = jnp.exp(jax.random.uniform(jax.random.fold_in(own, axis_at), (shards_of,), jnp.float32, smallest / len(cuts), high / len(cuts)))
        gain = gain * jnp.repeat(draws, shape[axis_at] // shards_of).reshape([-1 if axis == axis_at else 1 for axis in range(len(shape))])
    return gain


def assign_block(own_key, own, number, rows, number_of, top, bound, skew):
    order = jax.random.permutation(own_key, number_of)
    packed, ordinary = shares(number_of, rows * top, bound, skew, True), shares(number_of, rows * top, bound, skew, False)
    places = jnp.arange(number_of)

    def named(sizes, offset_by):
        used = int((sizes > 0).sum())
        fixed = max(1, used // 4)
        passed = fixed + (places - fixed + offset_by * (used - fixed)) % max(1, number_of - fixed)
        return jnp.zeros((number_of,), jnp.int32).at[order[jnp.where(places < fixed, places, passed)]].set(jnp.asarray(sizes, jnp.int32))

    sizes = jnp.where(number % 4 == 0, named(packed, number // 4), named(ordinary, number - number // 4 - 1))
    mixed = jax.random.permutation(jax.random.fold_in(own, 3), number_of)
    source_of, sink = mixed[0:number_of // 2 * 2:2], mixed[1:number_of // 2 * 2:2]
    margin = jnp.minimum(sizes[source_of] - 1, bound - sizes[sink]) // 2
    margin = jnp.where((source_of == order[0]) | (sink == order[0]) | (sizes[sink] == 0), 0, jnp.maximum(margin, 0))
    passed = jax.random.randint(jax.random.fold_in(own, 4), (number_of // 2,), 0, 1 << 20) % (margin + 1)
    sizes = sizes.at[source_of].add(-passed).at[sink].add(passed)
    labels = jnp.searchsorted(jnp.cumsum(sizes), jnp.arange(rows * top), side="right").astype(jnp.int32)
    listing = labels.reshape(top, rows).T
    listing = listing[jax.random.permutation(jax.random.fold_in(own, 1), rows)]
    offset_by = jax.random.randint(jax.random.fold_in(own, 2), (rows, 1), 0, top)
    return jnp.take_along_axis(listing, (jnp.arange(top)[None, :] + offset_by) % top, axis=1)


def shares(count, total, limit, slope, full):
    portions = [(1 << 20) // math.isqrt(standing ** slope) + 1 for standing in range(1, count + 1)]
    largest = limit if full else min(limit, max(-(-total // count), total * portions[0] // sum(portions)))
    least = 1 if total - largest >= count - 1 else 0
    given, surplus = [largest] + [least] * (count - 1), total - largest - least * (count - 1)
    while surplus > 0:
        candidates = [i for i in range(1, count) if given[i] < largest] or [i for i in range(1, count) if given[i] < limit]
        pool, budget = sum([portions[i] for i in candidates]), surplus
        for i in candidates:
            more = min(limit - given[i], max(1, budget * portions[i] // pool), surplus)
            given[i] = given[i] + more
            surplus = surplus - more
    return np.array(given)


def gaussian(stream_key, extent, width, limit, split=(), kind=jnp.bfloat16):
    gain = shard_levels(stream_key, extent, split, -0.22, 0.18) if split else 1.0
    array = jax.random.normal(stream_key, extent, jnp.float32) * width * gain
    return jnp.minimum(jnp.maximum(array, -limit), limit).astype(kind)


def setup_inputs(seed: int = 0, part: int = 0) -> dict:
    seeds = jax.random.split(jax.random.key(seed), 14)
    own_keys = jax.random.split(jax.random.fold_in(seeds[13], part), 14)
    resid_in = gaussian(own_keys[0], (SEQ, D), 1.0, 6.0, ((0, 16),))
    pool_input = gaussian(own_keys[1], (SEQ, POOL_WIDTH), 1.0, 6.0, ((0, 4), (1, 4)))
    pool_weight = gaussian(seeds[2], (GROUPS, GROUP_DIM, GROUP_DIM), GROUP_DIM ** -0.5, 0.375)
    pool_scale = jnp.clip(jax.random.uniform(seeds[3], (POOL_WIDTH,), jnp.float32, 0.2, 0.8), 0.2, 0.8)
    out_weight = gaussian(seeds[4], (POOL_WIDTH, D), POOL_WIDTH ** -0.5, 0.1875)
    mix_gain = jnp.clip(1.0 + 0.18 * jax.random.normal(seeds[5], (D,), jnp.float32), 0.1, 1.9)
    ffn_gain = jnp.clip(1.0 + 0.18 * jax.random.normal(seeds[6], (D,), jnp.float32), 0.1, 1.9)
    w_gate = gaussian(seeds[7], (EXPERTS, D, FF), (D // 8) ** -0.5, 0.375, ((0, 4), (2, 4)))
    w_up = gaussian(seeds[8], (EXPERTS, D, FF), (D // 8) ** -0.5, 0.375, ((0, 4), (2, 4)))
    w_down = gaussian(seeds[9], (EXPERTS, FF, D), FF ** -0.5, 0.1875, ((0, 4), (1, 4)))
    routes_keys = jax.random.split(jax.random.fold_in(own_keys[10], 1), SEQ // TOK_DEV)
    routes_turns = jax.random.permutation(jax.random.fold_in(own_keys[10], 3), SEQ // TOK_DEV)
    routes = jax.vmap(lambda own, number: assign_block(jax.random.fold_in(own_keys[10], 2), own, number, TOK_DEV, EXPERTS, TOP, CAP, 1))(routes_keys, routes_turns).reshape((SEQ, TOP))
    route_weight = jnp.clip(jnp.exp(math.log(1.0) - 2.3025851 * jax.random.uniform(own_keys[11], (SEQ, TOP), jnp.float32) ** shard_levels(own_keys[11], (SEQ, TOP), ((0, 16),), -0.2, 0.2)), 0.1, 1.0)
    post_gain = jnp.clip(1.0 + 0.18 * jax.random.normal(seeds[12], (D,), jnp.float32), 0.1, 1.9)
    return {"resid_in": resid_in, "pool_input": pool_input, "pool_weight": pool_weight, "pool_scale": pool_scale, "out_weight": out_weight, "mix_gain": mix_gain, "ffn_gain": ffn_gain, "w_gate": w_gate, "w_up": w_up, "w_down": w_down, "routes": routes, "route_weight": route_weight, "post_gain": post_gain}


pool_windows = (2, 4, 8, 16)
reach_back = 15
norm_eps = 1e-06
clamp_limit = 7.0
glu_alpha = 1.702

def rms_scale(values, gain_vec):
    inverse = lax.rsqrt(lax.optimization_barrier(jnp.mean(values * values, axis=-1, keepdims=True)) + norm_eps)
    return values * inverse * gain_vec

def clamped_unit(gate_pre, upward):
    gate_clip = jnp.minimum(gate_pre, clamp_limit)
    linear = jnp.clip(upward, -clamp_limit, clamp_limit)
    return gate_clip * jax.nn.sigmoid(glu_alpha * gate_clip) * (linear + 1.0)

def reference(resid_in, pool_input, pool_weight, pool_scale, out_weight, mix_gain, ffn_gain, w_gate, w_up, w_down, routes, route_weight, post_gain):
    source = pool_input.astype(jnp.float32)
    positions = jnp.arange(SEQ, dtype=jnp.int32)
    pieces = []
    for group_level, win_len in enumerate(pool_windows):
        group_cols = source[:, group_level * GROUP_DIM:(group_level + 1) * GROUP_DIM]
        padded = jnp.concatenate([jnp.zeros((reach_back, GROUP_DIM), jnp.float32), group_cols], axis=0)
        running = jnp.zeros((SEQ, GROUP_DIM), jnp.float32)
        for offset in range(win_len):
            running = running + padded[reach_back - offset:reach_back - offset + SEQ]
        divisor = jnp.minimum(positions + 1, win_len).astype(jnp.float32)[:, None]
        pieces.append(running / divisor - group_cols)
    mixed_rows = jnp.concatenate(pieces, axis=1).astype(jnp.bfloat16)
    pooled = jnp.einsum('tgc,gcd->tgd', mixed_rows.reshape(SEQ, GROUPS, GROUP_DIM).astype(jnp.float32), pool_weight.astype(jnp.float32))
    pooled = (pooled * pool_scale.reshape(GROUPS, GROUP_DIM)).astype(jnp.bfloat16).reshape(SEQ, POOL_WIDTH)
    mix_out = jnp.dot(pooled, out_weight, preferred_element_type=jnp.float32)
    residual = (resid_in.astype(jnp.float32) + rms_scale(mix_out, mix_gain)).astype(jnp.bfloat16)
    normed = rms_scale(residual.astype(jnp.float32), ffn_gain).astype(jnp.bfloat16)
    flat_route = routes.reshape(-1).astype(jnp.int32)
    total = SEQ * TOP
    sort_order = jnp.argsort(flat_route, stable=True).astype(jnp.int32)
    token_of = (sort_order // TOP).astype(jnp.int32)
    counts = lax.optimization_barrier(jnp.sum((flat_route[:, None] == jnp.arange(EXPERTS, dtype=jnp.int32)[None, :]).astype(jnp.int32), axis=0))
    starts = (jnp.cumsum(counts) - counts).astype(jnp.int32)
    most_rows = SEQ // TOK_DEV * CAP
    block_ff = FF // N_TP

    def one_expert(expert):
        row_index = jnp.minimum(starts[expert] + jnp.arange(most_rows, dtype=jnp.int32), total - 1)
        taken_rows = normed[token_of[row_index]]
        gate_pre = jnp.dot(taken_rows, w_gate[expert], preferred_element_type=jnp.float32)
        upward = jnp.dot(taken_rows, w_up[expert], preferred_element_type=jnp.float32)
        activated = clamped_unit(gate_pre, upward).astype(jnp.bfloat16)
        partials = jnp.einsum('rnf,nfd->rnd', activated.reshape(most_rows, N_TP, block_ff).astype(jnp.float32), w_down[expert].reshape(N_TP, block_ff, D).astype(jnp.float32))
        partials = lax.optimization_barrier(partials.astype(jnp.bfloat16))
        return lax.optimization_barrier(jnp.sum(partials.astype(jnp.float32), axis=1)).astype(jnp.bfloat16)
    expert_outs = lax.map(one_expert, jnp.arange(EXPERTS, dtype=jnp.int32))
    sorted_e = flat_route[sort_order]
    local_pos = (jnp.arange(total, dtype=jnp.int32) - starts[sorted_e]).astype(jnp.int32)
    picked = expert_outs[sorted_e, local_pos]
    assigned = jnp.zeros((total, D), jnp.bfloat16).at[sort_order].set(picked)
    expert_mix = lax.optimization_barrier(jnp.sum(assigned.reshape(SEQ, TOP, D).astype(jnp.float32) * route_weight[:, :, None], axis=1))
    return (residual.astype(jnp.float32) + rms_scale(expert_mix, post_gain)).astype(jnp.bfloat16)
```

```python
import functools

import jax
import jax.numpy as jnp
from jax import lax
from jax.experimental import pallas as pl
from jax.experimental.pallas import tpu as pltpu
from jax.sharding import PartitionSpec as P

GROUPS = 4
GROUP_DIM = 256
TOP = 2
CAP = 9


pool_windows = (2, 4, 8, 16)
reach_back = 15
norm_eps = 1e-06
clamp_limit = 7.0
glu_alpha = 1.702


def passed_along(x, axis, by):
    size = lax.axis_size(axis)
    pairs = [(i, i + by) for i in range(size) if 0 <= i + by < size]
    return lax.ppermute(x, axis, pairs)


def rms_scale(values, gain_vec):
    inverse = lax.rsqrt(jnp.mean(values * values, axis=-1, keepdims=True) + norm_eps)
    return values * inverse * gain_vec


def clamped_unit(gate_pre, upward):
    gate_clip = jnp.minimum(gate_pre, clamp_limit)
    linear = jnp.clip(upward, -clamp_limit, clamp_limit)
    return gate_clip * jax.nn.sigmoid(glu_alpha * gate_clip) * (linear + 1.0)


SLOT = 16
Y_FIRST = 16
Z_PART = 64
MESH = pl.DeviceIdType.MESH


def coords():
    return lax.axis_index("grp"), lax.axis_index("sp"), lax.axis_index("tp")


def routed_pool(pool_input, pool_weight, pool_scale):
    n_tp = lax.axis_size("tp")
    seg_rows, channels = pool_input.shape
    last_rows = pool_input[seg_rows - reach_back :]
    before = passed_along(last_rows, "sp", 1)
    extended = jnp.concatenate([before, pool_input], axis=0).astype(jnp.float32)
    first_chan = lax.axis_index("tp") * channels
    chan_group = (first_chan + lax.iota(jnp.int32, channels)) // GROUP_DIM
    positions = lax.axis_index("sp") * seg_rows + lax.iota(jnp.int32, seg_rows)
    window = jnp.zeros((channels,), jnp.int32)
    for group_level, win_len in enumerate(pool_windows):
        window = jnp.where(chan_group == group_level, win_len, window)
    running = jnp.zeros((seg_rows, channels), jnp.float32)
    window_sum = running
    for offset in range(pool_windows[-1]):
        running = running + extended[reach_back - offset : reach_back - offset + seg_rows]
        if offset + 1 in pool_windows:
            window_sum = jnp.where(window[None, :] == offset + 1, running, window_sum)
    divisor = jnp.minimum(positions[:, None] + 1, window[None, :]).astype(jnp.float32)
    mixed_rows = (window_sum / divisor - extended[reach_back:]).astype(jnp.bfloat16)
    token_mixed = lax.all_to_all(mixed_rows, "tp", split_axis=0, concat_axis=1, tiled=True)
    tok_rows = token_mixed.shape[0]
    pooled = jnp.einsum(
        "tgc,gcd->tgd",
        token_mixed.reshape(tok_rows, GROUPS, GROUP_DIM),
        pool_weight,
        preferred_element_type=jnp.float32,
    )
    pooled = (
        (pooled * pool_scale.reshape(GROUPS, GROUP_DIM)).astype(jnp.bfloat16).reshape(tok_rows, -1)
    )
    return pooled


def layer_kernel(n_tp, cuts, pool_ref, pw_ref, scale_ref, ow_ref, resid_ref, mgain_ref, fgain_ref,
                 pgain_ref, routes_ref, rweight_ref, wg_ref, wu_ref, wd_ref, out_ref,
                 pool, rows_in, pw, ow, residual, pooled, mix,
                 every, metas, picks, weights, held, wg, wu, wd,
                 work, from_core, za, zb, ya, yb,
                 psend, precv, hsend, hrecv, fsem,
                 send, recv, msend, mrecv, wsem,
                 csend, crecv, asend, arecv, bsend, brecv, ysend, yrecv, own):
    grp, sp, tp = coords()
    yy, core = sp // 2, sp % 2
    yo = 1 - yy
    y_other = yo * 2 + core
    c_other = yy * 2 + (1 - core)
    tok, width = residual.shape
    local_experts, buffers = wg_ref.shape[0], wg.shape[0]
    slots = local_experts * SLOT
    chunk = min(1024, width)
    others = [(a, b) for a in range(4) for b in range(n_tp) if (a, b) != (0, 0)]

    def weight_copies(e):
        at = lax.rem(e, buffers)
        return [pltpu.make_async_copy(w.at[e], buf.at[at], wsem.at[i, at])
                for i, (w, buf) in enumerate(((wg_ref, wg), (wu_ref, wu), (wd_ref, wd)))]

    loads = [pltpu.make_async_copy(a, b, fsem.at[i]) for i, (a, b) in enumerate(
        ((pool_ref, pool), (pw_ref, pw), (resid_ref, residual), (ow_ref, ow)))]
    for c in loads:
        c.start()
    barrier = pltpu.get_barrier_semaphore()
    for by in others:
        target = (grp, (sp + by[0]) % 4, (tp + by[1]) % n_tp)
        pl.semaphore_signal(barrier, inc=1, device_id=target, device_id_type=MESH)
    metas[sp, tp] = token_meta(routes_ref, rweight_ref, local_experts * 4)
    loads[0].wait()
    pl.semaphore_wait(barrier, len(others))

    def meta_copy(number, by):
        return pltpu.make_async_remote_copy(
            src_ref=metas.at[sp, tp], dst_ref=metas.at[sp, tp],
            send_sem=msend.at[number], recv_sem=mrecv.at[number],
            device_id=(grp, (sp + by[0]) % 4, (tp + by[1]) % n_tp), device_id_type=MESH)

    seg_rows, reach = pool.shape[0], SLOT
    first = tp == 0
    rest = tp > 0
    has_next = sp + 1 < 4

    def ends(to, whole, chan):
        if whole:
            at = pl.multiple_of(to * tok - reach, reach)
            return pool.at[pl.ds(at, tok + reach)], rows_in.at[chan]
        return pool.at[pl.ds(0, tok)], rows_in.at[chan, pl.ds(reach, tok)]

    def spread(by, whole):
        to = (tp + by) % n_tp
        src, dst = ends(to, whole, tp)
        return pltpu.make_async_remote_copy(
            src_ref=src, dst_ref=dst, send_sem=psend.at[by], recv_sem=precv.at[tp],
            device_id=(grp, sp, to), device_id_type=MESH)

    def landed(chan, whole):
        src, dst = ends(1 if whole else 0, whole, chan)
        return pltpu.make_async_remote_copy(
            src_ref=src, dst_ref=dst, send_sem=psend.at[0], recv_sem=precv.at[chan],
            device_id=(grp, sp, tp), device_id_type=MESH)

    def halo(chan):
        return pltpu.make_async_remote_copy(
            src_ref=pool.at[pl.ds(seg_rows - reach, reach)],
            dst_ref=rows_in.at[chan, pl.ds(0, reach)],
            send_sem=hsend.at[0], recv_sem=hrecv.at[chan],
            device_id=(grp, sp + 1, 0), device_id_type=MESH)

    def kept(whole):
        src, dst = ends(tp, whole, tp)
        return pltpu.make_async_copy(src, dst, own.at[0, 1])

    pl.when(has_next)(lambda: halo(tp).start())
    for by in range(1, n_tp):
        to_first = (tp + by) % n_tp == 0
        pl.when(to_first)(lambda by=by: spread(by, False).start())
        pl.when(jnp.logical_not(to_first))(lambda by=by: spread(by, True).start())
    pl.when(first)(lambda: kept(False).start())
    pl.when(rest)(lambda: kept(True).start())
    for number, by in enumerate(others):
        meta_copy(number, by).start()
    for e in range(min(buffers, local_experts)):
        for c in weight_copies(e):
            c.start()

    @pl.when(jnp.logical_and(first, sp == 0))
    def _():
        for chan in range(n_tp):
            rows_in[chan, pl.ds(0, reach)] = jnp.zeros((reach, rows_in.shape[2]), rows_in.dtype)

    loads[1].wait()
    start = (sp * n_tp + tp) * tok
    for group, window in enumerate(pool_windows):
        mine = tp == group
        if group:
            pl.when(mine)(lambda: kept(True).wait())
            pl.when(first)(lambda g=group: landed(g, False).wait_recv())
            pl.when(jnp.logical_and(rest, tp != group))(lambda g=group: landed(g, True).wait_recv())
        else:
            pl.when(mine)(lambda: kept(False).wait())
            pl.when(rest)(lambda: landed(0, True).wait_recv())
        pl.when(jnp.logical_and(first, sp > 0))(lambda g=group: halo(g).wait_recv())
        values = rows_in[group].astype(jnp.float32)
        total = values
        span = 1
        while span < window:
            total = total + jnp.concatenate([total[:span], total[:-span]], axis=0)
            span *= 2
        count = start + lax.broadcasted_iota(jnp.int32, (tok, values.shape[1]), 0) + 1
        divisor = jnp.minimum(count, window).astype(jnp.float32)
        mixed = (total[reach:] / divisor - values[reach:]).astype(jnp.bfloat16)
        product = jnp.dot(mixed, pw[group], preferred_element_type=jnp.float32)
        cols = slice(group * GROUP_DIM, (group + 1) * GROUP_DIM)
        pooled[:, cols] = (product * scale_ref[:, cols]).astype(jnp.bfloat16)
    loads[3].wait()

    def project(i, carry):
        at = pl.ds(pl.multiple_of(i * 512, 512), 512)
        mix[:, at] = jnp.dot(pooled[...], ow[:, at], preferred_element_type=jnp.float32)
        return carry

    lax.fori_loop(0, width // 512, project, 0)
    loads[2].wait()

    def norm_rows(part):
        begin, count = cuts[part]

        def body(i, carry):
            at = pl.ds(pl.multiple_of(begin + i * SLOT, SLOT), SLOT)
            after = residual[at].astype(jnp.float32) + rms_scale(mix[at], mgain_ref[...])
            after = after.astype(jnp.bfloat16)
            residual[at] = after
            every[sp, tp, at] = rms_scale(after.astype(jnp.float32), fgain_ref[...]).astype(jnp.bfloat16)
            return carry

        lax.fori_loop(0, count // SLOT, body, 0)

    def copy(s, t, part, way):
        target = [(grp, sp, tp + 1), (grp, sp, tp - 1), (grp, y_other, tp), (grp, c_other, tp)][way]
        first, count = cuts[part]
        piece = every.at[s, t, pl.ds(first, count)]
        return pltpu.make_async_remote_copy(
            src_ref=piece, dst_ref=piece,
            send_sem=send.at[s, t, part, way], recv_sem=recv.at[s, t, part],
            device_id=target, device_id_type=MESH)

    def arrived(s, t, part):
        copy(s, t, part, 3).wait_recv()

    sent = []

    def push(cond, s, t, part, way):
        if way == 0:
            cond = jnp.logical_and(cond, tp + 1 < n_tp)
        if way == 1:
            cond = jnp.logical_and(cond, tp > 0)
        pl.when(cond)(lambda: copy(s, t, part, way).start())
        sent.append((cond, s, t, part, way))

    def source_rows(s, t):
        return pl.ds(pl.multiple_of((s * n_tp + t) * SLOT, SLOT), SLOT)

    def select(s, t):
        slot = lax.broadcasted_iota(jnp.int32, (slots, tok), 0).astype(jnp.float32)
        base = (sp * slots).astype(jnp.float32)
        meta = metas[s, t]
        pick = jnp.zeros((slots, tok), jnp.float32)
        weight = jnp.zeros((slots, tok), jnp.float32)
        for k in range(TOP):
            hit = (meta[k : k + 1] - base) == slot
            pick = pick + jnp.where(hit, 1.0, 0.0)
            weight = weight + jnp.where(hit, meta[TOP + k : TOP + k + 1], 0.0)
        weight = jnp.broadcast_to(jnp.sum(weight, axis=1, keepdims=True), (slots, 128))
        pick = pick.astype(jnp.bfloat16)
        picks[s, t] = pick
        for e in range(local_experts):
            weights[e, source_rows(s, t)] = weight[e * SLOT : (e + 1) * SLOT]

        def body(i, carry):
            at = pl.ds(pl.multiple_of(i * chunk, chunk), chunk)
            got = jnp.dot(pick, every[s, t, :, at], preferred_element_type=jnp.float32)
            got = got.astype(jnp.bfloat16)
            for e in range(local_experts):
                held[e, source_rows(s, t), at] = got[e * SLOT : (e + 1) * SLOT]
            return carry

        lax.fori_loop(0, width // chunk, body, 0)

    yes = tp >= 0
    norm_rows(0)
    push(yes, sp, tp, 0, 2)
    for part in (1, 2):
        norm_rows(part)
        push(yes, sp, tp, part, 0)
        push(yes, sp, tp, part, 1)
        push(yes, sp, tp, part, 2)
    push(yes, sp, tp, 0, 0)
    push(yes, sp, tp, 0, 1)
    for part in (0, 1, 2):
        push(yes, sp, tp, part, 3)
    arrived(y_other, tp, 0)
    push(yes, y_other, tp, 0, 0)
    push(yes, y_other, tp, 0, 1)
    push(yes, y_other, tp, 0, 3)
    for number, by in enumerate(others):
        meta_copy(number, by).wait()
    select(sp, tp)

    def sides(dist):
        if dist == 0:
            return ((tp, yes),)
        return ((tp - dist, tp >= dist), (tp + dist, tp + dist < n_tp))

    def over_y(dist):
        for t, cond in sides(dist):
            for part in (1, 2):
                pl.when(cond)(functools.partial(arrived, y_other, t, part))
                push(cond, y_other, t, part, 3)
            pl.when(cond)(functools.partial(select, y_other, t))

    def cross(s, t):
        for part in (0, 1, 2):
            arrived(s, t, part)
        select(s, t)

    def over_core(s, dist):
        for t, cond in sides(dist):
            pl.when(cond)(functools.partial(cross, s, t))

    far_core = yo * 2 + (1 - core)
    for dist in range(1, n_tp):
        for s, part in ((sp, 1), (sp, 2), (sp, 0), (y_other, 0)):
            for way, (t, cond) in enumerate(sides(dist)):
                pl.when(cond)(functools.partial(arrived, s, t, part))
                push(cond, s, t, part, way)
                if part:
                    push(cond, s, t, part, 2)
                push(cond, s, t, part, 3)
        for t, cond in sides(dist):
            pl.when(cond)(functools.partial(select, sp, t))
        over_core(c_other, dist - 1)
        over_y(dist - 1)
        if dist > 1:
            over_core(far_core, dist - 2)
    over_core(c_other, n_tp - 1)
    if n_tp > 1:
        over_core(far_core, n_tp - 2)
    over_y(n_tp - 1)
    over_core(far_core, n_tp - 1)
    for cond, s, t, part, way in sent:
        pl.when(cond)(lambda s=s, t=t, part=part, way=way: copy(s, t, part, way).wait_send())

    def expert(e, carry):
        at = lax.rem(e, buffers)
        for c in weight_copies(e):
            c.wait()
        rows = held[e]
        gate_pre = jnp.dot(rows, wg[at], preferred_element_type=jnp.float32)
        upward = jnp.dot(rows, wu[at], preferred_element_type=jnp.float32)
        scale = jnp.concatenate([weights[e]] * (gate_pre.shape[1] // 128), axis=1)
        activated = (clamped_unit(gate_pre, upward) * scale).astype(jnp.bfloat16)

        def down(i, inner):
            cols = pl.ds(pl.multiple_of(i * chunk, chunk), chunk)
            term = jnp.dot(activated, wd[at, :, cols], preferred_element_type=jnp.float32)
            held[e, :, cols] = term.astype(jnp.bfloat16)
            return inner

        lax.fori_loop(0, width // chunk, down, 0)

        @pl.when(e + buffers < local_experts)
        def _():
            for c in weight_copies(e + buffers):
                c.start()

        return carry

    lax.fori_loop(0, local_experts, expert, 0)

    def combined(s, t, at):
        term = held[:, source_rows(s, t), at].reshape(slots, chunk)
        return lax.dot_general(picks[s, t], term, (((0,), (0,)), ((), ())),
                               preferred_element_type=jnp.float32)

    rows_of = [pl.ds(first, count) for first, count in cuts]
    rows_a = rows_of[0]
    ups, downs = (grp, sp, tp + 1), (grp, sp, tp - 1)
    up_ok, down_ok = tp + 1 < n_tp, tp > 0

    def remote(src, dst, s_sem, r_sem, target):
        return pltpu.make_async_remote_copy(
            src_ref=src, dst_ref=dst, send_sem=s_sem, recv_sem=r_sem,
            device_id=target, device_id_type=MESH)

    def core_copy(y, t):
        return remote(every.at[y * 2 + (1 - core), t], from_core.at[y, t],
                      csend.at[y, t], crecv.at[y, t], (grp, c_other, tp))

    def combine_away(y, t):
        s = y * 2 + (1 - core)

        def body(i, carry):
            at = pl.ds(pl.multiple_of(i * chunk, chunk), chunk)
            every[s, t, :, at] = combined(s, t, at).astype(jnp.bfloat16)
            return carry

        lax.fori_loop(0, width // chunk, body, 0)
        core_copy(y, t).start()

    order = []
    for dist in range(n_tp - 1, -1, -1):
        for side in (1, -1) if dist else (1,):
            t = tp + side * dist
            order.append((jnp.logical_and(t >= 0, t < n_tp), t, side, dist))

    def y_copy_b(part, t):
        rows = rows_of[part]
        return remote(work.at[yo, t, rows], yb.at[t, rows], ysend.at[part, t], yrecv.at[part, t],
                      (grp, y_other, tp))

    def y_copy_a():
        return remote(work.at[yo, tp, rows_a], ya, ysend.at[0, 0], yrecv.at[0, 0], (grp, y_other, tp))

    def local(y, t):
        s = y * 2 + core
        core_copy(y, t).wait_recv()

        def body(i, carry):
            at = pl.ds(pl.multiple_of(i * chunk, chunk), chunk)
            both = combined(s, t, at) + from_core[y, t, :, at].astype(jnp.float32)
            work[y, t, :, at] = both.astype(jnp.bfloat16)
            return carry

        lax.fori_loop(0, width // chunk, body, 0)

    def z_ends(part, y, t, slot):
        rows = rows_of[part]
        if part:
            return work.at[y, t, rows], zb.at[slot, rows], bsend.at[part, t], brecv.at[part, slot]
        return work.at[y, t, rows], za.at[y, slot], asend.at[y, t], arecv.at[y, slot]

    def z_copy(part, y, t, side):
        if side == 1:
            slot, target = t, ups
        else:
            slot, target = jnp.where(t == tp - 1, n_tp, t), downs
        return remote(*z_ends(part, y, t, slot), target)

    def take_z(part, y, t, slot):
        remote(*z_ends(part, y, t, slot), ups).wait_recv()
        dst, src = z_ends(part, y, t, slot)[:2]
        add_into(dst, src)

    def z_step(part, y, t, side):
        inner = tp > 0 if side == 1 else tp + 1 < n_tp
        pl.when(inner)(lambda: take_z(part, y, t, t))
        z_copy(part, y, t, side).start()

    def z_end(part, y):
        pl.when(down_ok)(lambda: take_z(part, y, tp, tp))
        pl.when(up_ok)(lambda: take_z(part, y, tp, n_tp))

    for y in (yo, yy):
        for ok, t, side, dist in order:
            pl.when(ok)(functools.partial(combine_away, y, t))
        if y is yo:
            for ok, t, side, dist in order:
                @pl.when(ok)
                def _(t=t):
                    local(yo, t)
                    y_copy_b(1, t).start()
                    y_copy_b(2, t).start()
    for ok, t, side, dist in order:
        @pl.when(ok)
        def _(t=t, side=side, dist=dist):
            local(yy, t)
            if dist:
                z_step(0, yo, t, side)
                z_step(0, yy, t, side)
            for part in (1, 2):
                y_copy_b(part, t).wait_recv()
                add_into(work.at[yy, t, rows_of[part]], yb.at[t, rows_of[part]])
                if dist:
                    z_step(part, yy, t, side)
    z_end(0, yo)
    y_copy_a().start()
    z_end(0, yy)
    z_end(1, yy)
    z_end(2, yy)
    y_copy_a().wait_recv()
    add_into(work.at[yy, tp, rows_a], ya)
    def finish(i, carry):
        at = pl.ds(pl.multiple_of(i * SLOT, SLOT), SLOT)
        total = work[yy, tp, at].astype(jnp.float32)
        out_ref[at] = (residual[at].astype(jnp.float32) + rms_scale(total, pgain_ref[...])).astype(out_ref.dtype)
        return carry

    lax.fori_loop(0, tok // SLOT, finish, 0)
    pl.when(has_next)(lambda: halo(tp).wait_send())
    for by in range(1, n_tp):
        to_first = (tp + by) % n_tp == 0
        pl.when(to_first)(lambda by=by: spread(by, False).wait_send())
        pl.when(jnp.logical_not(to_first))(lambda by=by: spread(by, True).wait_send())
    y_copy_a().wait_send()
    for ok, t, side, dist in order:
        @pl.when(ok)
        def _(t=t, side=side, dist=dist):
            core_copy(yo, t).wait_send()
            core_copy(yy, t).wait_send()
            y_copy_b(1, t).wait_send()
            y_copy_b(2, t).wait_send()
            if dist:
                z_copy(0, yo, t, side).wait_send()
                z_copy(0, yy, t, side).wait_send()
                z_copy(1, yy, t, side).wait_send()
                z_copy(2, yy, t, side).wait_send()


def token_meta(routes_ref, rweight_ref, n_experts):
    tok = routes_ref.shape[1]
    expert = lax.broadcasted_iota(jnp.int32, (n_experts, tok), 0)
    hits = [jnp.where(expert == routes_ref[k : k + 1], 1.0, 0.0) for k in range(TOP)]
    earlier = (lax.broadcasted_iota(jnp.int32, (tok, tok), 0)
               < lax.broadcasted_iota(jnp.int32, (tok, tok), 1))
    earlier = jnp.where(earlier, 1.0, 0.0).astype(jnp.bfloat16)
    before = jnp.dot(sum(hits).astype(jnp.bfloat16), earlier, preferred_element_type=jnp.float32)
    line = lax.broadcasted_iota(jnp.int32, (8, tok), 0)
    meta = jnp.zeros((8, tok), jnp.float32)
    for k in range(TOP):
        rank = jnp.sum(hits[k] * before, axis=0, keepdims=True)
        place = routes_ref[k : k + 1].astype(jnp.float32) * SLOT + rank
        meta = jnp.where(line == k, place, meta)
        meta = jnp.where(line == TOP + k, rweight_ref[k : k + 1], meta)
    return meta


def add_into(dst, src):
    rows = dst.shape[0]
    strip = 16

    def body(i, carry):
        at = pl.ds(pl.multiple_of(i * strip, strip), strip)
        dst[at] = (dst[at].astype(jnp.float32) + src[at].astype(jnp.float32)).astype(dst.dtype)
        return carry

    lax.fori_loop(0, rows // strip, body, 0)


def fused_layer(resid_in, pool_input, pool_weight, pool_scale, out_weight, mix_gain, ffn_gain,
                w_gate, w_up, w_down, routes, route_weight, post_gain):
    n_tp = lax.axis_size("tp")
    tok, width = resid_in.shape
    local_experts, _, hidden = w_gate.shape
    cuts = ((0, Y_FIRST), (Y_FIRST, Z_PART), (Y_FIRST + Z_PART, tok - Y_FIRST - Z_PART))
    an = cuts[0][1]
    vmem, hbm = pl.BlockSpec(memory_space=pltpu.VMEM), pl.BlockSpec(memory_space=pl.ANY)
    kind = resid_in.dtype
    slots, buffers = local_experts * SLOT, min(4, local_experts)
    channels = pool_input.shape[1]
    dma = pltpu.SemaphoreType.DMA
    return pl.pallas_call(
        functools.partial(layer_kernel, n_tp, cuts),
        out_shape=jax.ShapeDtypeStruct((tok, width), kind),
        in_specs=[hbm, hbm, vmem, hbm, hbm, vmem, vmem, vmem, vmem, vmem, hbm, hbm, hbm],
        out_specs=vmem,
        scratch_shapes=[
            pltpu.VMEM(pool_input.shape, kind),
            pltpu.VMEM((n_tp, tok + SLOT, channels), kind),
            pltpu.VMEM(pool_weight.shape, kind),
            pltpu.VMEM(out_weight.shape, kind),
            pltpu.VMEM((tok, width), kind),
            pltpu.VMEM((tok, n_tp * channels), kind),
            pltpu.VMEM((tok, width), jnp.float32),
            pltpu.VMEM((4, n_tp, tok, width), kind),
            pltpu.VMEM((4, n_tp, 8, tok), jnp.float32),
            pltpu.VMEM((4, n_tp, slots, tok), kind),
            pltpu.VMEM((local_experts, 4 * n_tp * SLOT, 128), jnp.float32),
            pltpu.VMEM((local_experts, 4 * n_tp * SLOT, width), kind),
            pltpu.VMEM((buffers, width, hidden), kind),
            pltpu.VMEM((buffers, width, hidden), kind),
            pltpu.VMEM((buffers, hidden, width), kind),
            pltpu.VMEM((2, n_tp, tok, width), kind),
            pltpu.VMEM((2, n_tp, tok, width), kind),
            pltpu.VMEM((2, n_tp + 1, an, width), kind),
            pltpu.VMEM((n_tp + 1, tok, width), kind),
            pltpu.VMEM((an, width), kind),
            pltpu.VMEM((n_tp, tok, width), kind),
            dma((n_tp,)),
            dma((n_tp,)),
            dma((1,)),
            dma((n_tp,)),
            dma((4,)),
            dma((4, n_tp, 3, 4)),
            dma((4, n_tp, 3)),
            dma((4 * n_tp - 1,)),
            dma((4 * n_tp - 1,)),
            dma((3, buffers)),
            dma((2, n_tp)),
            dma((2, n_tp)),
            dma((2, n_tp)),
            dma((2, n_tp + 1)),
            dma((3, n_tp)),
            dma((3, n_tp + 1)),
            dma((3, n_tp)),
            dma((3, n_tp)),
            dma((2, max(2, n_tp))),
        ],
        compiler_params=pltpu.CompilerParams(
            collective_id=0, has_side_effects=True, vmem_limit_bytes=58 * 2**20
        ),
        name="fused_layer",
    )(pool_input, pool_weight, pool_scale[None], out_weight, resid_in, mix_gain[None], ffn_gain[None],
      post_gain[None], routes.T, route_weight.T, w_gate, w_up, w_down)


def per_device(
    resid_in,
    pool_input,
    pool_weight,
    pool_scale,
    out_weight,
    mix_gain,
    ffn_gain,
    w_gate,
    w_up,
    w_down,
    routes,
    route_weight,
    post_gain,
):
    n_sp = lax.axis_size("sp")
    n_tp = lax.axis_size("tp")
    seg_rows, channels = pool_input.shape
    tok_rows, width = resid_in.shape
    if (
        n_sp == 4
        and n_tp == GROUPS
        and channels == GROUP_DIM
        and seg_rows == n_tp * 128
        and tok_rows == 128
        and w_gate.shape[2] <= 256
        and w_gate.shape[0] <= 8
        and width <= 2048
    ):
        return fused_layer(resid_in, pool_input, pool_weight, pool_scale, out_weight, mix_gain,
                           ffn_gain, w_gate, w_up, w_down, routes, route_weight, post_gain)
    pooled = routed_pool(pool_input, pool_weight, pool_scale)
    mix_out = jnp.dot(pooled, out_weight, preferred_element_type=jnp.float32)
    residual = (resid_in.astype(jnp.float32) + rms_scale(mix_out, mix_gain)).astype(jnp.bfloat16)
    normed = rms_scale(residual.astype(jnp.float32), ffn_gain).astype(jnp.bfloat16)
    local_experts = w_gate.shape[0]
    n_experts = local_experts * n_sp
    slot_total = n_experts * CAP
    flat_route = routes.reshape(-1)
    onehot = (flat_route[:, None] == lax.iota(jnp.int32, n_experts)[None, :]).astype(jnp.int32)
    slot_rank = jnp.sum((jnp.cumsum(onehot, axis=0) - onehot) * onehot, axis=1)
    slot_index = flat_route * CAP + slot_rank
    picker = slot_index[:, None] == lax.iota(jnp.int32, slot_total)[None, :]
    picker_rows = picker.astype(jnp.bfloat16)
    token_pick = jnp.sum(
        picker.reshape(tok_rows, TOP, slot_total).astype(jnp.float32), axis=1
    ).astype(jnp.bfloat16)
    buffer = lax.dot_general(
        token_pick, normed, (((0,), (0,)), ((), ())), preferred_element_type=jnp.float32
    )
    outgoing = buffer.astype(jnp.bfloat16).reshape(n_sp, local_experts * CAP, width)
    at_owner = lax.all_to_all(outgoing, "sp", split_axis=0, concat_axis=0, tiled=True)
    arrived = lax.all_gather(at_owner[:, None], "tp", axis=1, tiled=True)
    arrived = arrived.reshape(n_sp, n_tp, local_experts, CAP, width)
    gate_pre = jnp.einsum("sklcd,ldf->sklcf", arrived, w_gate, preferred_element_type=jnp.float32)
    upward = jnp.einsum("sklcd,ldf->sklcf", arrived, w_up, preferred_element_type=jnp.float32)
    activated = clamped_unit(gate_pre, upward).astype(jnp.bfloat16)
    terms = jnp.einsum("sklcf,lfd->kslcd", activated, w_down, preferred_element_type=jnp.float32)
    summed = lax.psum_scatter(
        terms.reshape(1 * lax.axis_size("tp"), n_sp, local_experts * CAP, width).astype(
            jnp.bfloat16
        ),
        "tp",
        scatter_dimension=0,
        tiled=True,
    ).astype(jnp.float32)
    results = summed[0].astype(jnp.bfloat16)
    returned = lax.all_to_all(results, "sp", split_axis=0, concat_axis=0, tiled=True).reshape(
        slot_total, width
    )
    gathered = jnp.dot(picker_rows, returned, preferred_element_type=jnp.float32)
    expert_mix = jnp.sum(gathered.reshape(tok_rows, TOP, width) * route_weight[:, :, None], axis=1)
    return (residual.astype(jnp.float32) + rms_scale(expert_mix, post_gain)).astype(jnp.bfloat16)


def solution(mesh):
    in_specs = (
        P(("grp", "sp", "tp"), None),
        P(("grp", "sp"), "tp"),
        P(),
        P(),
        P(),
        P(),
        P(),
        P("sp", None, "tp"),
        P("sp", None, "tp"),
        P("sp", "tp", None),
        P(("grp", "sp", "tp"), None),
        P(("grp", "sp", "tp"), None),
        P(),
    )
    out_specs = P(("grp", "sp", "tp"), None)
    return jax.shard_map(
        per_device, mesh=mesh, in_specs=in_specs, out_specs=out_specs, check_vma=False
    )
```

```python
import functools

import jax
import jax.numpy as jnp
from jax import lax
from jax.experimental import pallas as pl
from jax.experimental.pallas import tpu as pltpu
from jax.sharding import PartitionSpec as P

GROUPS = 4
GROUP_DIM = 256
TOP = 2
CAP = 9


pool_windows = (2, 4, 8, 16)
reach_back = 15
norm_eps = 1e-06
clamp_limit = 7.0
glu_alpha = 1.702


def passed_along(x, axis, by):
    size = lax.axis_size(axis)
    pairs = [(i, i + by) for i in range(size) if 0 <= i + by < size]
    return lax.ppermute(x, axis, pairs)


def rms_scale(values, gain_vec):
    inverse = lax.rsqrt(jnp.mean(values * values, axis=-1, keepdims=True) + norm_eps)
    return values * inverse * gain_vec


def clamped_unit(gate_pre, upward):
    gate_clip = jnp.minimum(gate_pre, clamp_limit)
    linear = jnp.clip(upward, -clamp_limit, clamp_limit)
    return gate_clip * jax.nn.sigmoid(glu_alpha * gate_clip) * (linear + 1.0)


SLOT = 16
HALVES = ((16, 16, 32), (16, 32, 16))
BACK = ((16, 16, 32), (16, 32, 16))
ORDER = (
    ("N", 0, 0), ("OZ", 0, 0), ("N", 0, 2), ("OY", 0, 2), ("N", 1, 4), ("OY", 0, 0), ("N", 1, 5),
    ("N", 0, 1), ("OZ", 0, 1), ("OY", 0, 1), ("OZ", 0, 2), ("F", 0, 1, 0, "own"), ("N", 1, 3),
    ("OC", 1), ("F", 0, 1, 1, "own"), ("X", 0), ("F", 0, 2, 0, "own"), ("F", 0, 1, 2, "own"),
    ("F", 0, 2, 1, "own"), ("F", 0, 2, 2, "own"), ("OC", 0), ("F", 0, 1, 0, "yo"),
    ("F", 0, 3, 1, "own"), ("YS", 0, 0), ("F", 0, 3, 2, "own"), ("OY", 1, 4), ("SA", 0, 0),
    ("F", 0, 3, 0, "own"), ("CO", 0, 2), ("SA", 1, 0), ("SA", 0, 2), ("OZ", 1, 5),
    ("F", 0, 2, 0, "yo"), ("YS", 0, 1), ("YS", 0, 2), ("CO", 0, 3), ("OY", 1, 3), ("OZ", 1, 4),
    ("CO", 0, 0), ("OZ", 1, 3), ("SA", 0, 3), ("FA", 0, 1), ("OY", 1, 5), ("FA", 0, 2),
    ("SA", 0, 1), ("F", 0, 3, 0, "yo"), ("YS", 0, 3), ("FA", 0, 0), ("F", 1, 1, 5, "own"),
    ("FA", 0, 3), ("CO", 0, 1), ("E", 0, 0), ("F", 1, 1, 4, "own"), ("E", 0, 1), ("E", 0, 2),
    ("X", 1), ("F", 1, 2, 5, "own"), ("E", 0, 3), ("E", 0, 4), ("E", 0, 5), ("F", 1, 2, 4, "own"),
    ("E", 0, 6), ("E", 0, 7), ("F", 1, 1, 3, "yo"), ("AW", 0, "yo", 3), ("AW", 0, "yo", 2),
    ("F", 1, 1, 3, "own"), ("AW", 0, "yy", 3), ("F", 1, 3, 5, "own"), ("AW", 0, "yy", 1),
    ("AW", 0, "yo", 1), ("CO", 1, 0), ("AW", 0, "yy", 2), ("F", 1, 3, 4, "own"), ("SY", 0, 3),
    ("RL", 0, 3), ("AW", 0, "yy", 0), ("F", 1, 2, 3, "yo"), ("SA", 1, 1), ("YS", 1, 0),
    ("YS", 1, 2), ("SY", 0, 2), ("F", 1, 2, 3, "own"), ("YS", 1, 1), ("RL", 0, 2), ("SY", 0, 1),
    ("FA", 1, 2), ("SA", 1, 2), ("FA", 1, 1), ("FA", 1, 0), ("F", 1, 3, 3, "yo"), ("YS", 1, 3),
    ("F", 1, 3, 3, "own"), ("CO", 1, 1), ("RL", 0, 1), ("FA", 1, 3), ("AW", 0, "yo", 0),
    ("CO", 1, 3), ("RT", 0, 3, 1), ("CO", 1, 2), ("SA", 1, 3), ("E", 1, 0), ("RT", 0, 3, 2),
    ("E", 1, 1), ("E", 1, 2), ("RT", 0, 2, 1), ("E", 1, 3), ("E", 1, 4), ("RT", 0, 2, 2),
    ("SY", 0, 0), ("E", 1, 5), ("E", 1, 6), ("E", 1, 7), ("RT", 0, 1, 1), ("AW", 1, "yo", 3),
    ("AW", 1, "yy", 0), ("RL", 0, 0), ("AW", 1, "yo", 2), ("RT", 0, 1, 2), ("AW", 1, "yy", 3),
    ("AW", 1, "yy", 2), ("SY", 1, 3), ("AW", 1, "yo", 1), ("RL", 1, 3), ("RH", 0), ("RT", 0, 0, 2),
    ("RT", 1, 3, 4), ("SY", 1, 2), ("RT", 1, 3, 5), ("AW", 1, "yy", 1), ("RL", 1, 2),
    ("RT", 0, 0, 1), ("RP", 0, 1), ("SY", 1, 1), ("RP", 0, 2), ("AW", 1, "yo", 0), ("RF", 0),
    ("RT", 1, 2, 4), ("RT", 1, 2, 5), ("SY", 1, 0), ("RL", 1, 1), ("RT", 1, 1, 4), ("RL", 1, 0),
    ("RT", 1, 1, 5), ("RH", 1), ("RT", 1, 0, 5), ("RT", 1, 0, 4), ("RP", 1, 4), ("RP", 1, 5),
    ("RF", 1),
)
MESH = pl.DeviceIdType.MESH


def coords():
    return lax.axis_index("grp"), lax.axis_index("sp"), lax.axis_index("tp")


def routed_pool(pool_input, pool_weight, pool_scale):
    n_tp = lax.axis_size("tp")
    seg_rows, channels = pool_input.shape
    last_rows = pool_input[seg_rows - reach_back :]
    before = passed_along(last_rows, "sp", 1)
    extended = jnp.concatenate([before, pool_input], axis=0).astype(jnp.float32)
    first_chan = lax.axis_index("tp") * channels
    chan_group = (first_chan + lax.iota(jnp.int32, channels)) // GROUP_DIM
    positions = lax.axis_index("sp") * seg_rows + lax.iota(jnp.int32, seg_rows)
    window = jnp.zeros((channels,), jnp.int32)
    for group_level, win_len in enumerate(pool_windows):
        window = jnp.where(chan_group == group_level, win_len, window)
    running = jnp.zeros((seg_rows, channels), jnp.float32)
    window_sum = running
    for offset in range(pool_windows[-1]):
        running = running + extended[reach_back - offset : reach_back - offset + seg_rows]
        if offset + 1 in pool_windows:
            window_sum = jnp.where(window[None, :] == offset + 1, running, window_sum)
    divisor = jnp.minimum(positions[:, None] + 1, window[None, :]).astype(jnp.float32)
    mixed_rows = (window_sum / divisor - extended[reach_back:]).astype(jnp.bfloat16)
    token_mixed = lax.all_to_all(mixed_rows, "tp", split_axis=0, concat_axis=1, tiled=True)
    tok_rows = token_mixed.shape[0]
    pooled = jnp.einsum(
        "tgc,gcd->tgd",
        token_mixed.reshape(tok_rows, GROUPS, GROUP_DIM),
        pool_weight,
        preferred_element_type=jnp.float32,
    )
    pooled = (
        (pooled * pool_scale.reshape(GROUPS, GROUP_DIM)).astype(jnp.bfloat16).reshape(tok_rows, -1)
    )
    return pooled


def layer_kernel(n_tp, cuts, rcuts, pool_ref, pw_ref, scale_ref, ow_ref, resid_ref, mgain_ref, fgain_ref,
                 pgain_ref, routes_ref, rweight_ref, wg_ref, wu_ref, wd_ref, out_ref,
                 pool, rows_in, pw, residual, pooled, mix,
                 every, metas, picks, weights, held, wg, wu, wd,
                 work, from_core, za, zb, ya, yb,
                 psend, precv, hsend, hrecv, fsem,
                 send, recv, msend, mrecv, wsem,
                 csend, crecv, asend, arecv, bsend, brecv, ysend, yrecv, own):
    grp, sp, tp = coords()
    yy, core = sp // 2, sp % 2
    yo = 1 - yy
    y_other = yo * 2 + core
    c_other = yy * 2 + (1 - core)
    tok, width = residual.shape
    local_experts, buffers = wg_ref.shape[0], wg.shape[0]
    slots = local_experts * SLOT
    chunk = width
    others = [(a, b) for a in range(4) for b in range(n_tp) if (a, b) != (0, 0)]

    def weight_copies(e):
        at = lax.rem(e, buffers)
        return [pltpu.make_async_copy(w.at[e], buf.at[at], wsem.at[i, at])
                for i, (w, buf) in enumerate(((wg_ref, wg), (wu_ref, wu), (wd_ref, wd)))]

    loads = [pltpu.make_async_copy(a, b, fsem.at[i]) for i, (a, b) in enumerate(
        ((pool_ref, pool), (pw_ref, pw), (resid_ref, residual)))]
    blocks = [(y, t) for y in range(2) for t in range(n_tp)]
    loads += [pltpu.make_async_copy(ow_ref.at[pl.ds(i * tok, tok)], from_core.at[y, t], fsem.at[3 + i])
              for i, (y, t) in enumerate(blocks)]
    for c in loads:
        c.start()
    barrier = pltpu.get_barrier_semaphore()
    for by in others:
        target = (grp, (sp + by[0]) % 4, (tp + by[1]) % n_tp)
        pl.semaphore_signal(barrier, inc=1, device_id=target, device_id_type=MESH)
    metas[sp, tp] = token_meta(routes_ref, rweight_ref, local_experts * 4)
    loads[0].wait()
    pl.semaphore_wait(barrier, len(others))

    def meta_copy(number, by):
        return pltpu.make_async_remote_copy(
            src_ref=metas.at[sp, tp], dst_ref=metas.at[sp, tp],
            send_sem=msend.at[number], recv_sem=mrecv.at[number],
            device_id=(grp, (sp + by[0]) % 4, (tp + by[1]) % n_tp), device_id_type=MESH)

    seg_rows, reach = pool.shape[0], SLOT
    first = tp == 0
    rest = tp > 0
    has_next = sp + 1 < 4

    def ends(to, whole, chan):
        if whole:
            at = pl.multiple_of(to * tok - reach, reach)
            return pool.at[pl.ds(at, tok + reach)], rows_in.at[chan]
        return pool.at[pl.ds(0, tok)], rows_in.at[chan, pl.ds(reach, tok)]

    def spread(by, whole):
        to = (tp + by) % n_tp
        src, dst = ends(to, whole, tp)
        return pltpu.make_async_remote_copy(
            src_ref=src, dst_ref=dst, send_sem=psend.at[by], recv_sem=precv.at[tp],
            device_id=(grp, sp, to), device_id_type=MESH)

    def landed(chan, whole):
        src, dst = ends(1 if whole else 0, whole, chan)
        return pltpu.make_async_remote_copy(
            src_ref=src, dst_ref=dst, send_sem=psend.at[0], recv_sem=precv.at[chan],
            device_id=(grp, sp, tp), device_id_type=MESH)

    def halo(chan):
        return pltpu.make_async_remote_copy(
            src_ref=pool.at[pl.ds(seg_rows - reach, reach)],
            dst_ref=rows_in.at[chan, pl.ds(0, reach)],
            send_sem=hsend.at[0], recv_sem=hrecv.at[chan],
            device_id=(grp, sp + 1, 0), device_id_type=MESH)

    def kept(whole):
        src, dst = ends(tp, whole, tp)
        return pltpu.make_async_copy(src, dst, own.at[0, 1])

    pl.when(has_next)(lambda: halo(tp).start())
    for by in range(1, n_tp):
        to_first = (tp + by) % n_tp == 0
        pl.when(to_first)(lambda by=by: spread(by, False).start())
        pl.when(jnp.logical_not(to_first))(lambda by=by: spread(by, True).start())
    pl.when(first)(lambda: kept(False).start())
    pl.when(rest)(lambda: kept(True).start())
    for number, by in enumerate(others):
        meta_copy(number, by).start()
    for e in range(min(buffers, local_experts)):
        for c in weight_copies(e):
            c.start()

    @pl.when(jnp.logical_and(first, sp == 0))
    def _():
        for chan in range(n_tp):
            rows_in[chan, pl.ds(0, reach)] = jnp.zeros((reach, rows_in.shape[2]), rows_in.dtype)

    loads[1].wait()
    start = (sp * n_tp + tp) * tok
    for group, window in enumerate(pool_windows):
        mine = tp == group
        if group:
            pl.when(mine)(lambda: kept(True).wait())
            pl.when(first)(lambda g=group: landed(g, False).wait_recv())
            pl.when(jnp.logical_and(rest, tp != group))(lambda g=group: landed(g, True).wait_recv())
        else:
            pl.when(mine)(lambda: kept(False).wait())
            pl.when(rest)(lambda: landed(0, True).wait_recv())
        pl.when(jnp.logical_and(first, sp > 0))(lambda g=group: halo(g).wait_recv())
        values = rows_in[group].astype(jnp.float32)
        total = values
        span = 1
        while span < window:
            total = total + jnp.concatenate([total[:span], total[:-span]], axis=0)
            span *= 2
        count = start + lax.broadcasted_iota(jnp.int32, (tok, values.shape[1]), 0) + 1
        divisor = jnp.minimum(count, window).astype(jnp.float32)
        mixed = (total[reach:] / divisor - values[reach:]).astype(jnp.bfloat16)
        product = jnp.dot(mixed, pw[group], preferred_element_type=jnp.float32)
        cols = slice(group * GROUP_DIM, (group + 1) * GROUP_DIM)
        pooled[:, cols] = (product * scale_ref[:, cols]).astype(jnp.bfloat16)
    for c in loads[3:]:
        c.wait()

    def project(i, carry):
        at = pl.ds(pl.multiple_of(i * 512, 512), 512)
        mix[:, at] = jnp.dot(pooled[...], from_core[:, :, :, at].reshape(pooled.shape[1], 512),
                             preferred_element_type=jnp.float32)
        return carry

    lax.fori_loop(0, width // 512, project, 0)
    loads[2].wait()

    def norm_rows(part):
        begin, count = cuts[part][:2]

        def body(i, carry):
            at = pl.ds(pl.multiple_of(begin + i * SLOT, SLOT), SLOT)
            after = residual[at].astype(jnp.float32) + rms_scale(mix[at], mgain_ref[...])
            after = after.astype(jnp.bfloat16)
            residual[at] = after
            every[sp, tp, at] = rms_scale(after.astype(jnp.float32), fgain_ref[...]).astype(jnp.bfloat16)
            return carry

        lax.fori_loop(0, count // SLOT, body, 0)

    def copy(s, t, part, way):
        target = [(grp, sp, tp + 1), (grp, sp, tp - 1), (grp, y_other, tp), (grp, c_other, tp)][way]
        first, count = cuts[part][:2]
        piece = every.at[s, t, pl.ds(first, count)]
        return pltpu.make_async_remote_copy(
            src_ref=piece, dst_ref=piece,
            send_sem=send.at[s, t, part, way], recv_sem=recv.at[s, t, part],
            device_id=target, device_id_type=MESH)

    def arrived(s, t, part):
        copy(s, t, part, 3).wait_recv()

    def allowed(cond, way):
        if way == 0:
            return jnp.logical_and(cond, tp + 1 < n_tp)
        if way == 1:
            return jnp.logical_and(cond, tp > 0)
        return cond

    def push(cond, s, t, part, way):
        pl.when(allowed(cond, way))(lambda: copy(s, t, part, way).start())

    def source_rows(s, t):
        return pl.ds(pl.multiple_of((s * n_tp + t) * SLOT, SLOT), SLOT)

    half = tok // 2
    rows_h = [pl.ds(h * half, half) for h in range(2)]
    parts_h = [[p for p, c in enumerate(cuts) if c[2] == h] for h in range(2)]
    rparts_h = [[p for p, c in enumerate(rcuts) if c[2] == h] for h in range(2)]

    def select(h, s, t):
        slot = lax.broadcasted_iota(jnp.int32, (slots, half), 0).astype(jnp.float32)
        base = (sp * slots).astype(jnp.float32)
        meta = metas[s, t, :, pl.ds(0, half)]
        pick = jnp.zeros((slots, half), jnp.float32)
        weight = jnp.zeros((slots, half), jnp.float32)
        for k in range(TOP):
            hit = (meta[4 * h + k : 4 * h + k + 1] - base) == slot
            pick = pick + jnp.where(hit, 1.0, 0.0)
            weight = weight + jnp.where(hit, meta[4 * h + TOP + k : 4 * h + TOP + k + 1], 0.0)
        weight = jnp.broadcast_to(jnp.sum(weight, axis=1, keepdims=True), (slots, 128))
        pick = pick.astype(jnp.bfloat16)
        picks[h, s, t] = pick
        for e in range(local_experts):
            weights[h, e, source_rows(s, t)] = weight[e * SLOT : (e + 1) * SLOT]

        def body(i, carry):
            at = pl.ds(pl.multiple_of(i * chunk, chunk), chunk)
            got = jnp.dot(pick, every[s, t, rows_h[h], at], preferred_element_type=jnp.float32)
            got = got.astype(jnp.bfloat16)
            for e in range(local_experts):
                held[h, e, source_rows(s, t), at] = got[e * SLOT : (e + 1) * SLOT]
            return carry

        lax.fori_loop(0, width // chunk, body, 0)

    yes = tp >= 0
    far_core = yo * 2 + (1 - core)

    def own_z(h, parts):
        for p in parts:
            push(yes, sp, tp, p, 0)
            push(yes, sp, tp, p, 1)

    def own_way(h, way):
        for p in parts_h[h]:
            push(yes, sp, tp, p, way)

    def crossed(h):
        p = parts_h[h][0]
        arrived(y_other, tp, p)
        push(yes, y_other, tp, p, 0)
        push(yes, y_other, tp, p, 1)
        push(yes, y_other, tp, p, 3)

    by_dist = [((tp, yes),)] + [
        ((tp - d, tp >= d), (tp + d, tp + d < n_tp)) for d in range(1, n_tp)]

    def sides(dist):
        return by_dist[dist]

    def over_y(h, dist):
        for t, cond in sides(dist):
            for p in parts_h[h][1:]:
                pl.when(cond)(functools.partial(arrived, y_other, t, p))
                push(cond, y_other, t, p, 3)
            pl.when(cond)(functools.partial(select, h, y_other, t))

    def cross(h, s, t):
        for p in parts_h[h]:
            arrived(s, t, p)
        select(h, s, t)

    def over_core(h, s, dist):
        for t, cond in sides(dist):
            pl.when(cond)(functools.partial(cross, h, s, t))

    def along(h, dist, p, s):
        for way, (t, cond) in enumerate(sides(dist)):
            pl.when(cond)(functools.partial(arrived, s, t, p))
            push(cond, s, t, p, way)
            if p != parts_h[h][0]:
                push(cond, s, t, p, 2)
            push(cond, s, t, p, 3)

    def select_along(h, dist):
        for t, cond in sides(dist):
            pl.when(cond)(functools.partial(select, h, sp, t))

    def sent_all(h):
        head, tail = parts_h[h][0], parts_h[h][1:]
        sent = [(yes, sp, tp, p, way) for p in parts_h[h] for way in range(4)]
        sent += [(yes, y_other, tp, head, way) for way in (0, 1, 3)]
        sent += [(yes, y_other, tp, p, 3) for p in tail]
        for dist in range(1, n_tp):
            for side, (t, cond) in enumerate(sides(dist)):
                sent += [(cond, sp, t, p, way) for p in tail for way in (side, 2, 3)]
                sent += [(cond, s, t, head, way) for s in (sp, y_other) for way in (side, 3)]
                sent += [(cond, y_other, t, p, 3) for p in tail]
        for cond, s, t, p, way in sent:
            pl.when(allowed(cond, way))(lambda s=s, t=t, p=p, way=way: copy(s, t, p, way).wait_send())

    def use_expert(h, e):
        at = lax.rem(e, buffers)
        rows = held[h, e]
        gate_pre = jnp.dot(rows, wg[at], preferred_element_type=jnp.float32)
        upward = jnp.dot(rows, wu[at], preferred_element_type=jnp.float32)
        scale = jnp.concatenate([weights[h, e]] * (gate_pre.shape[1] // 128), axis=1)
        activated = (clamped_unit(gate_pre, upward) * scale).astype(jnp.bfloat16)

        def down(i, inner):
            cols = pl.ds(pl.multiple_of(i * chunk, chunk), chunk)
            term = jnp.dot(activated, wd[at, :, cols], preferred_element_type=jnp.float32)
            held[h, e, :, cols] = term.astype(jnp.bfloat16)
            return inner

        lax.fori_loop(0, width // chunk, down, 0)

    def begin_weights(e, cond):
        @pl.when(cond)
        def _():
            for c in weight_copies(e):
                c.start()

    def end_weights(e, cond):
        @pl.when(cond)
        def _():
            for c in weight_copies(e):
                c.wait()

    def experts(h, between):
        def body(j, carry):
            e = local_experts - 1 - j if h else j
            end_weights(e, j >= buffers if h else j >= 0)
            use_expert(h, e)
            later = e - buffers if h else e + buffers
            begin_weights(later, jnp.logical_and(later >= 0, later < local_experts))
            for number, steps in between:
                pl.when(j == number)(functools.partial(run, steps))
            return carry

        lax.fori_loop(0, local_experts, body, 0)

    def combined(h, s, t, at):
        term = held[h, :, source_rows(s, t), at].reshape(slots, chunk)
        return lax.dot_general(picks[h, s, t], term, (((0,), (0,)), ((), ())),
                               preferred_element_type=jnp.float32)

    rows_of = [pl.ds(c[0], c[1]) for c in rcuts]
    ups, downs = (grp, sp, tp + 1), (grp, sp, tp - 1)
    up_ok, down_ok = tp + 1 < n_tp, tp > 0

    def remote(src, dst, s_sem, r_sem, target):
        return pltpu.make_async_remote_copy(
            src_ref=src, dst_ref=dst, send_sem=s_sem, recv_sem=r_sem,
            device_id=target, device_id_type=MESH)

    def core_copy(h, y, t):
        return remote(every.at[y * 2 + (1 - core), t, rows_h[h]], from_core.at[y, t, rows_h[h]],
                      csend.at[h, y, t], crecv.at[h, y, t], (grp, c_other, tp))

    def combine_away(h, y, t):
        s = y * 2 + (1 - core)

        def body(i, carry):
            at = pl.ds(pl.multiple_of(i * chunk, chunk), chunk)
            every[s, t, rows_h[h], at] = combined(h, s, t, at).astype(jnp.bfloat16)
            return carry

        lax.fori_loop(0, width // chunk, body, 0)
        core_copy(h, y, t).start()

    order = []
    for dist in range(n_tp - 1, -1, -1):
        for side in (1, -1) if dist else (1,):
            t = tp + side * dist
            order.append((jnp.logical_and(t >= 0, t < n_tp), t, side, dist))

    def y_copy_b(p, t):
        rows = rows_of[p]
        return remote(work.at[yo, t, rows], yb.at[t, rows], ysend.at[p, t], yrecv.at[p, t],
                      (grp, y_other, tp))

    def y_copy_a(h):
        p = rparts_h[h][0]
        return remote(work.at[yo, tp, rows_of[p]], ya.at[h, pl.ds(0, rcuts[p][1])], ysend.at[p, 0], yrecv.at[p, 0],
                      (grp, y_other, tp))

    def local(h, y, t):
        s = y * 2 + core
        core_copy(h, y, t).wait_recv()

        def body(i, carry):
            at = pl.ds(pl.multiple_of(i * chunk, chunk), chunk)
            both = combined(h, s, t, at) + from_core[y, t, rows_h[h], at].astype(jnp.float32)
            work[y, t, rows_h[h], at] = both.astype(jnp.bfloat16)
            return carry

        lax.fori_loop(0, width // chunk, body, 0)

    def z_ends(p, y, t, slot):
        rows, h = rows_of[p], rcuts[p][2]
        if p == rparts_h[h][0]:
            return work.at[y, t, rows], za.at[h, y, slot, pl.ds(0, rcuts[p][1])], asend.at[h, y, t], arecv.at[h, y, slot]
        return work.at[y, t, rows], zb.at[slot, rows], bsend.at[p, t], brecv.at[p, slot]

    def z_copy(p, y, t, side):
        if side == 1:
            slot, target = t, ups
        else:
            slot, target = jnp.where(t == tp - 1, n_tp, t), downs
        return remote(*z_ends(p, y, t, slot), target)

    def take_z(p, y, t, slot):
        remote(*z_ends(p, y, t, slot), ups).wait_recv()
        dst, src = z_ends(p, y, t, slot)[:2]
        add_into(dst, src)

    def z_step(p, y, t, side):
        inner = tp > 0 if side == 1 else tp + 1 < n_tp
        pl.when(inner)(lambda: take_z(p, y, t, t))
        z_copy(p, y, t, side).start()

    def z_end(p, y):
        pl.when(down_ok)(lambda: take_z(p, y, tp, tp))
        pl.when(up_ok)(lambda: take_z(p, y, tp, n_tp))

    def aways(h, y, want):
        for ok, t, side, dist in order:
            if dist == want:
                pl.when(ok)(functools.partial(combine_away, h, y, t))

    def send_y(h, dists):
        for ok, t, side, dist in order:
            if dist in dists:
                @pl.when(ok)
                def _(t=t):
                    local(h, yo, t)
                    for p in rparts_h[h][1:]:
                        y_copy_b(p, t).start()

    def reduce_local(h, want):
        head = rparts_h[h][0]
        for ok, t, side, dist in order:
            if dist != want:
                continue

            @pl.when(ok)
            def _(t=t, side=side, dist=dist):
                local(h, yy, t)
                if dist:
                    z_step(head, yo, t, side)
                    z_step(head, yy, t, side)

    def reduce_part(p, want):
        for ok, t, side, dist in order:
            if dist != want:
                continue

            @pl.when(ok)
            def _(t=t, side=side, dist=dist):
                y_copy_b(p, t).wait_recv()
                add_into(work.at[yy, t, rows_of[p]], yb.at[t, rows_of[p]])
                if dist:
                    z_step(p, yy, t, side)

    def reduce_head(h):
        head = rparts_h[h][0]
        z_end(head, yo)
        y_copy_a(h).start()
        z_end(head, yy)

    def reduce_last(h):
        head = rparts_h[h][0]
        y_copy_a(h).wait_recv()
        add_into(work.at[yy, tp, rows_of[head]], ya.at[h, pl.ds(0, rcuts[head][1])])
        finish_rows(h)

    def reduce_sent(h):
        head, tail = rparts_h[h][0], rparts_h[h][1:]
        y_copy_a(h).wait_send()
        for ok, t, side, dist in order:
            @pl.when(ok)
            def _(t=t, side=side, dist=dist):
                core_copy(h, yo, t).wait_send()
                core_copy(h, yy, t).wait_send()
                for p in tail:
                    y_copy_b(p, t).wait_send()
                if dist:
                    z_copy(head, yo, t, side).wait_send()
                    z_copy(head, yy, t, side).wait_send()
                    for p in tail:
                        z_copy(p, yy, t, side).wait_send()

    def finish_rows(h):
        def body(i, carry):
            at = pl.ds(pl.multiple_of(h * half + i * SLOT, SLOT), SLOT)
            total = work[yy, tp, at].astype(jnp.float32)
            done = residual[at].astype(jnp.float32) + rms_scale(total, pgain_ref[...])
            out_ref[at] = done.astype(out_ref.dtype)
            return carry

        lax.fori_loop(0, half // SLOT, body, 0)

    def step(kind, h, *at):
        if kind == "N":
            norm_rows(at[0])
        elif kind == "OZ":
            own_z(h, at)
        elif kind == "OY":
            push(yes, sp, tp, at[0], 2)
        elif kind == "OC":
            own_way(h, 3)
        elif kind == "X":
            crossed(h)
        elif kind == "F":
            along(h, at[0], at[1], sp if at[2] == "own" else y_other)
        elif kind == "SA":
            select_along(h, at[0])
        elif kind == "YS":
            over_y(h, at[0])
        elif kind == "CO":
            over_core(h, c_other, at[0])
        elif kind == "FA":
            over_core(h, far_core, at[0])
        elif kind == "W":
            sent_all(h)
        elif kind == "M":
            for number, by in enumerate(others):
                meta_copy(number, by).wait()
        elif kind == "AW":
            aways(h, yo if at[0] == "yo" else yy, at[1])
        elif kind == "SY":
            send_y(h, at)
        elif kind == "RL":
            reduce_local(h, at[0])
        elif kind == "RT":
            reduce_part(at[1], at[0])
        elif kind == "RH":
            reduce_head(h)
        elif kind == "RP":
            z_end(at[0], yy)
        elif kind == "RF":
            reduce_last(h)

    def run(steps):
        for one in steps:
            step(*one)

    todo, waited = [], set()
    for one in ORDER:
        if one[0] == "AW" and one[1] not in waited:
            waited.add(one[1])
            todo.append(("W", one[1]))
        if one[0] in ("SA", "YS", "CO", "FA") and "M" not in waited:
            waited.add("M")
            todo.append(("M", 0))
        todo.append(one)
    while todo:
        one = todo.pop(0)
        if one[0] != "E":
            step(*one)
            continue
        h, between, seen = one[1], [], 0
        while seen < local_experts - 1:
            one = todo.pop(0)
            if one[0] == "E":
                seen += 1
            elif between and between[-1][0] == seen:
                between[-1][1].append(one)
            else:
                between.append((seen, [one]))
        experts(h, between)
    reduce_sent(0)
    reduce_sent(1)
    pl.when(has_next)(lambda: halo(tp).wait_send())
    for by in range(1, n_tp):
        to_first = (tp + by) % n_tp == 0
        pl.when(to_first)(lambda by=by: spread(by, False).wait_send())
        pl.when(jnp.logical_not(to_first))(lambda by=by: spread(by, True).wait_send())


def cut_rows(halves):
    cuts, at = [], 0
    for h, counts in enumerate(halves):
        for count in counts:
            cuts.append((at, count, h))
            at += count
    return tuple(cuts)


def token_meta(routes_ref, rweight_ref, n_experts):
    tok = routes_ref.shape[1]
    expert = lax.broadcasted_iota(jnp.int32, (n_experts, tok), 0)
    hits = [jnp.where(expert == routes_ref[k : k + 1], 1.0, 0.0) for k in range(TOP)]
    earlier = (lax.broadcasted_iota(jnp.int32, (tok, tok), 0)
               < lax.broadcasted_iota(jnp.int32, (tok, tok), 1))
    earlier = jnp.where(earlier, 1.0, 0.0).astype(jnp.bfloat16)
    before = jnp.dot(sum(hits).astype(jnp.bfloat16), earlier, preferred_element_type=jnp.float32)
    half = tok // 2
    line = lax.broadcasted_iota(jnp.int32, (8, half), 0)
    meta = jnp.zeros((8, half), jnp.float32)
    for k in range(TOP):
        rank = jnp.sum(hits[k] * before, axis=0, keepdims=True)
        place = routes_ref[k : k + 1].astype(jnp.float32) * SLOT + rank
        weight = rweight_ref[k : k + 1]
        for h in range(2):
            lanes = slice(h * half, (h + 1) * half)
            meta = jnp.where(line == 4 * h + k, place[:, lanes], meta)
            meta = jnp.where(line == 4 * h + TOP + k, weight[:, lanes], meta)
    return jnp.concatenate([meta, jnp.zeros((8, tok - half), jnp.float32)], axis=1)


def add_into(dst, src):
    rows = dst.shape[0]
    strip = 16

    def body(i, carry):
        at = pl.ds(pl.multiple_of(i * strip, strip), strip)
        dst[at] = (dst[at].astype(jnp.float32) + src[at].astype(jnp.float32)).astype(dst.dtype)
        return carry

    lax.fori_loop(0, rows // strip, body, 0)


def fused_layer(resid_in, pool_input, pool_weight, pool_scale, out_weight, mix_gain, ffn_gain,
                w_gate, w_up, w_down, routes, route_weight, post_gain):
    n_tp = lax.axis_size("tp")
    tok, width = resid_in.shape
    local_experts, _, hidden = w_gate.shape
    cuts, rcuts = cut_rows(HALVES), cut_rows(BACK)
    parts, rparts = len(cuts), len(rcuts)
    heads = [counts[0] for counts in BACK]
    vmem, hbm = pl.BlockSpec(memory_space=pltpu.VMEM), pl.BlockSpec(memory_space=pl.ANY)
    kind = resid_in.dtype
    slots, buffers = local_experts * SLOT, min(4, local_experts)
    channels = pool_input.shape[1]
    dma = pltpu.SemaphoreType.DMA
    return pl.pallas_call(
        functools.partial(layer_kernel, n_tp, cuts, rcuts),
        out_shape=jax.ShapeDtypeStruct((tok, width), kind),
        in_specs=[hbm, hbm, vmem, hbm, hbm, vmem, vmem, vmem, vmem, vmem, hbm, hbm, hbm],
        out_specs=vmem,
        scratch_shapes=[
            pltpu.VMEM(pool_input.shape, kind),
            pltpu.VMEM((n_tp, tok + SLOT, channels), kind),
            pltpu.VMEM(pool_weight.shape, kind),
            pltpu.VMEM((tok, width), kind),
            pltpu.VMEM((tok, n_tp * channels), kind),
            pltpu.VMEM((tok, width), jnp.float32),
            pltpu.VMEM((4, n_tp, tok, width), kind),
            pltpu.VMEM((4, n_tp, 8, tok), jnp.float32),
            pltpu.VMEM((2, 4, n_tp, slots, tok // 2), kind),
            pltpu.VMEM((2, local_experts, 4 * n_tp * SLOT, 128), jnp.float32),
            pltpu.VMEM((2, local_experts, 4 * n_tp * SLOT, width), kind),
            pltpu.VMEM((buffers, width, hidden), kind),
            pltpu.VMEM((buffers, width, hidden), kind),
            pltpu.VMEM((buffers, hidden, width), kind),
            pltpu.VMEM((2, n_tp, tok, width), kind),
            pltpu.VMEM((2, n_tp, tok, width), kind),
            pltpu.VMEM((2, 2, n_tp + 1, max(heads), width), kind),
            pltpu.VMEM((n_tp + 1, tok, width), kind),
            pltpu.VMEM((2, max(heads), width), kind),
            pltpu.VMEM((n_tp, tok, width), kind),
            dma((n_tp,)),
            dma((n_tp,)),
            dma((1,)),
            dma((n_tp,)),
            dma((3 + 2 * n_tp,)),
            dma((4, n_tp, parts, 4)),
            dma((4, n_tp, parts)),
            dma((4 * n_tp - 1,)),
            dma((4 * n_tp - 1,)),
            dma((3, buffers)),
            dma((2, 2, n_tp)),
            dma((2, 2, n_tp)),
            dma((2, 2, n_tp)),
            dma((2, 2, n_tp + 1)),
            dma((rparts, n_tp)),
            dma((rparts, n_tp + 1)),
            dma((rparts, n_tp)),
            dma((rparts, n_tp)),
            dma((2, max(2, n_tp))),
        ],
        compiler_params=pltpu.CompilerParams(
            collective_id=0, has_side_effects=True, vmem_limit_bytes=60 * 2**20
        ),
        name="fused_layer",
    )(pool_input, pool_weight, pool_scale[None], out_weight, resid_in, mix_gain[None], ffn_gain[None],
      post_gain[None], routes.T, route_weight.T, w_gate, w_up, w_down)


def per_device(
    resid_in,
    pool_input,
    pool_weight,
    pool_scale,
    out_weight,
    mix_gain,
    ffn_gain,
    w_gate,
    w_up,
    w_down,
    routes,
    route_weight,
    post_gain,
):
    n_sp = lax.axis_size("sp")
    n_tp = lax.axis_size("tp")
    seg_rows, channels = pool_input.shape
    tok_rows, width = resid_in.shape
    if (
        n_sp == 4
        and n_tp == GROUPS
        and channels == GROUP_DIM
        and seg_rows == n_tp * 128
        and tok_rows == 128
        and w_gate.shape[2] <= 256
        and w_gate.shape[0] <= 8
        and width <= 2048
        and out_weight.shape[0] == 2 * n_tp * tok_rows
    ):
        return fused_layer(resid_in, pool_input, pool_weight, pool_scale, out_weight, mix_gain,
                           ffn_gain, w_gate, w_up, w_down, routes, route_weight, post_gain)
    pooled = routed_pool(pool_input, pool_weight, pool_scale)
    mix_out = jnp.dot(pooled, out_weight, preferred_element_type=jnp.float32)
    residual = (resid_in.astype(jnp.float32) + rms_scale(mix_out, mix_gain)).astype(jnp.bfloat16)
    normed = rms_scale(residual.astype(jnp.float32), ffn_gain).astype(jnp.bfloat16)
    local_experts = w_gate.shape[0]
    n_experts = local_experts * n_sp
    slot_total = n_experts * CAP
    flat_route = routes.reshape(-1)
    onehot = (flat_route[:, None] == lax.iota(jnp.int32, n_experts)[None, :]).astype(jnp.int32)
    slot_rank = jnp.sum((jnp.cumsum(onehot, axis=0) - onehot) * onehot, axis=1)
    slot_index = flat_route * CAP + slot_rank
    picker = slot_index[:, None] == lax.iota(jnp.int32, slot_total)[None, :]
    picker_rows = picker.astype(jnp.bfloat16)
    token_pick = jnp.sum(
        picker.reshape(tok_rows, TOP, slot_total).astype(jnp.float32), axis=1
    ).astype(jnp.bfloat16)
    buffer = lax.dot_general(
        token_pick, normed, (((0,), (0,)), ((), ())), preferred_element_type=jnp.float32
    )
    outgoing = buffer.astype(jnp.bfloat16).reshape(n_sp, local_experts * CAP, width)
    at_owner = lax.all_to_all(outgoing, "sp", split_axis=0, concat_axis=0, tiled=True)
    arrived = lax.all_gather(at_owner[:, None], "tp", axis=1, tiled=True)
    arrived = arrived.reshape(n_sp, n_tp, local_experts, CAP, width)
    gate_pre = jnp.einsum("sklcd,ldf->sklcf", arrived, w_gate, preferred_element_type=jnp.float32)
    upward = jnp.einsum("sklcd,ldf->sklcf", arrived, w_up, preferred_element_type=jnp.float32)
    activated = clamped_unit(gate_pre, upward).astype(jnp.bfloat16)
    terms = jnp.einsum("sklcf,lfd->kslcd", activated, w_down, preferred_element_type=jnp.float32)
    summed = lax.psum_scatter(
        terms.reshape(1 * lax.axis_size("tp"), n_sp, local_experts * CAP, width).astype(
            jnp.bfloat16
        ),
        "tp",
        scatter_dimension=0,
        tiled=True,
    ).astype(jnp.float32)
    results = summed[0].astype(jnp.bfloat16)
    returned = lax.all_to_all(results, "sp", split_axis=0, concat_axis=0, tiled=True).reshape(
        slot_total, width
    )
    gathered = jnp.dot(picker_rows, returned, preferred_element_type=jnp.float32)
    expert_mix = jnp.sum(gathered.reshape(tok_rows, TOP, width) * route_weight[:, :, None], axis=1)
    return (residual.astype(jnp.float32) + rms_scale(expert_mix, post_gain)).astype(jnp.bfloat16)


def solution(mesh):
    in_specs = (
        P(("grp", "sp", "tp"), None),
        P(("grp", "sp"), "tp"),
        P(),
        P(),
        P(),
        P(),
        P(),
        P("sp", None, "tp"),
        P("sp", None, "tp"),
        P("sp", "tp", None),
        P(("grp", "sp", "tp"), None),
        P(("grp", "sp", "tp"), None),
        P(),
    )
    out_specs = P(("grp", "sp", "tp"), None)
    return jax.shard_map(
        per_device, mesh=mesh, in_specs=in_specs, out_specs=out_specs, check_vma=False
    )
```

```python
import functools

import jax
import jax.numpy as jnp
from jax import lax
from jax.experimental import pallas as pl
from jax.experimental.pallas import tpu as pltpu
from jax.sharding import PartitionSpec as P

GROUPS = 4
GROUP_DIM = 256
TOP = 2
CAP = 9


pool_windows = (2, 4, 8, 16)
reach_back = 15
norm_eps = 1e-06
clamp_limit = 7.0
glu_alpha = 1.702


def passed_along(x, axis, by):
    size = lax.axis_size(axis)
    pairs = [(i, i + by) for i in range(size) if 0 <= i + by < size]
    return lax.ppermute(x, axis, pairs)


def rms_scale(values, gain_vec):
    inverse = lax.rsqrt(jnp.mean(values * values, axis=-1, keepdims=True) + norm_eps)
    return values * inverse * gain_vec


def clamped_unit(gate_pre, upward):
    gate_clip = jnp.minimum(gate_pre, clamp_limit)
    linear = jnp.clip(upward, -clamp_limit, clamp_limit)
    return gate_clip * jax.nn.sigmoid(glu_alpha * gate_clip) * (linear + 1.0)


SLOT = 16
HALVES = ((16, 16, 32), (16, 16, 32))
BACK = ((16, 16, 32), (16, 16, 32))
ORDER = (
    ("P", 0), ("N", 0, 2), ("OY", 0, 2), ("N", 0, 0), ("OY", 0, 0), ("N", 0, 1), ("OZ", 0, 2, 0),
    ("OZ", 0, 1, 1), ("OZ", 0, 1, 0), ("OY", 0, 1), ("OZ", 0, 0, 1), ("OZ", 0, 2, 1), ("P", 1),
    ("N", 1, 3), ("SA", 0, 0, 0), ("N", 1, 5), ("OZ", 0, 0, 0), ("F", 0, 1, 1, "own", 1),
    ("F", 0, 1, 2, "own", 0), ("X", 0), ("F", 0, 1, 1, "own", 0), ("F", 0, 1, 0, "own", 0),
    ("F", 0, 1, 2, "own", 1), ("YA", 0, 0, 2, 0), ("OC", 0), ("YA", 0, 1, 1, 1), ("CO", 0, 0, 0),
    ("F", 0, 1, 0, "own", 1), ("SA", 0, 1, 0), ("N", 1, 4), ("F", 0, 2, 2, "own", 0), ("OY", 1, 4),
    ("SA", 1, 0, 0), ("YA", 0, 0, 1, 0), ("YA", 0, 1, 2, 0), ("OC", 1), ("F", 0, 1, 0, "yo", 0),
    ("F", 0, 2, 1, "own", 1), ("CO", 0, 1, 0), ("CO", 0, 1, 1), ("CO", 1, 0, 0), ("FA", 0, 0, 0),
    ("YA", 0, 1, 1, 0), ("YS", 0, 1, 0), ("F", 0, 2, 2, "own", 1), ("YS", 0, 0, 0),
    ("F", 0, 1, 0, "yo", 1), ("F", 0, 2, 1, "own", 0), ("YA", 0, 1, 2, 1), ("YS", 0, 1, 1),
    ("SA", 0, 1, 1), ("OZ", 1, 4, 1), ("OY", 1, 3), ("FA", 0, 1, 0), ("F", 0, 2, 0, "own", 0),
    ("FA", 0, 1, 1), ("F", 0, 3, 1, "own", 1), ("E", 0, 0), ("F", 0, 2, 0, "own", 1),
    ("SA", 0, 2, 1), ("E", 0, 0), ("E", 0, 0), ("F", 0, 3, 2, "own", 0), ("F", 0, 2, 0, "yo", 0),
    ("E", 0, 0), ("F", 0, 3, 2, "own", 1), ("OZ", 1, 4, 0), ("YA", 0, 2, 2, 0), ("E", 0, 0),
    ("F", 0, 2, 0, "yo", 1), ("F", 0, 3, 1, "own", 0), ("YA", 1, 0, 4, 0), ("OY", 1, 5),
    ("YA", 0, 3, 1, 1), ("YA", 0, 2, 2, 1), ("YA", 0, 2, 1, 1), ("OZ", 1, 5, 0), ("OZ", 1, 5, 1),
    ("E", 0, 0), ("YA", 0, 2, 1, 0), ("F", 1, 1, 4, "own", 1), ("E", 0, 0), ("YA", 0, 3, 2, 0),
    ("F", 0, 3, 0, "own", 0), ("E", 0, 0), ("CO", 0, 2, 0), ("F", 0, 3, 0, "own", 1),
    ("CO", 0, 2, 1), ("FA", 0, 2, 1), ("YA", 0, 3, 2, 1), ("FA", 0, 2, 0), ("YA", 0, 3, 1, 0),
    ("F", 0, 3, 0, "yo", 0), ("SA", 0, 3, 1), ("F", 0, 3, 0, "yo", 1), ("SA", 0, 3, 0),
    ("YS", 0, 3, 1), ("CO", 0, 3, 1), ("CO", 0, 3, 0), ("SA", 0, 2, 0), ("YS", 0, 2, 0),
    ("F", 1, 1, 4, "own", 0), ("YS", 0, 2, 1), ("FA", 0, 3, 1), ("FA", 0, 3, 0), ("YS", 0, 3, 0),
    ("E", 0, 1), ("E", 0, 1), ("F", 1, 1, 5, "own", 1), ("OZ", 1, 3, 1), ("YA", 1, 0, 5, 0),
    ("F", 1, 1, 5, "own", 0), ("E", 0, 1), ("E", 0, 1), ("OZ", 1, 3, 0), ("X", 1),
    ("F", 1, 2, 4, "own", 0), ("F", 1, 2, 4, "own", 1), ("YA", 1, 1, 4, 1), ("E", 0, 1),
    ("E", 0, 1), ("E", 0, 1), ("F", 1, 2, 5, "own", 1), ("E", 0, 1), ("AW", 0, "yo", 3, 0),
    ("F", 1, 2, 5, "own", 0), ("AW", 0, "yy", 3, 0), ("YA", 1, 1, 4, 0), ("AW", 0, "yy", 2, 0),
    ("F", 1, 1, 3, "own", 1), ("AW", 0, "yy", 1, 0), ("AW", 0, "yo", 3, 1), ("FA", 1, 0, 0),
    ("AW", 0, "yy", 3, 1), ("AW", 0, "yo", 0, 0), ("AW", 0, "yo", 1, 1), ("F", 1, 1, 3, "own", 0),
    ("SY", 0, 3, 0), ("F", 1, 1, 3, "yo", 1), ("SA", 1, 1, 1), ("YA", 1, 1, 5, 1), ("RL", 0, 3, 0),
    ("AW", 0, "yy", 1, 1), ("YS", 1, 0, 0), ("SA", 1, 1, 0), ("F", 1, 1, 3, "yo", 0),
    ("AW", 0, "yo", 2, 0), ("SY", 0, 3, 1), ("RL", 0, 3, 1), ("YA", 1, 1, 5, 0), ("YS", 1, 1, 1),
    ("AW", 0, "yo", 1, 0), ("YS", 1, 1, 0), ("AW", 0, "yo", 2, 1), ("CO", 1, 1, 1),
    ("AW", 0, "yy", 2, 1), ("CO", 1, 1, 0), ("FA", 1, 1, 1), ("FA", 1, 1, 0), ("E", 1, 0),
    ("E", 1, 0), ("RT", 0, 3, 1, 0), ("F", 1, 3, 4, "own", 0), ("F", 1, 3, 4, "own", 1),
    ("YA", 1, 2, 4, 0), ("RT", 0, 3, 1, 1), ("F", 1, 3, 5, "own", 1), ("SY", 0, 2, 0), ("E", 1, 0),
    ("F", 1, 3, 5, "own", 0), ("RL", 0, 2, 0), ("SY", 0, 2, 1), ("RL", 0, 2, 1), ("YA", 1, 2, 4, 1),
    ("F", 1, 2, 3, "own", 1), ("F", 1, 2, 3, "own", 0), ("E", 1, 0), ("YA", 1, 2, 5, 0),
    ("E", 1, 0), ("RT", 0, 3, 2, 0), ("F", 1, 2, 3, "yo", 0), ("RT", 0, 3, 2, 1),
    ("F", 1, 2, 3, "yo", 1), ("SY", 0, 1, 0), ("SY", 0, 1, 1), ("E", 1, 0), ("E", 1, 0),
    ("RL", 0, 1, 0), ("YA", 1, 2, 5, 1), ("RL", 0, 1, 1), ("CO", 1, 2, 0), ("YA", 1, 3, 4, 0),
    ("CO", 1, 2, 1), ("E", 1, 0), ("F", 1, 3, 3, "own", 1), ("F", 1, 3, 3, "own", 0),
    ("YA", 1, 3, 4, 1), ("YA", 1, 3, 5, 1), ("SY", 0, 0, 0), ("F", 1, 3, 3, "yo", 1),
    ("FA", 1, 2, 1), ("SA", 1, 3, 1), ("SA", 1, 3, 0), ("F", 1, 3, 3, "yo", 0), ("YA", 1, 3, 5, 0),
    ("CO", 1, 3, 1), ("CO", 1, 3, 0), ("YS", 1, 3, 0), ("SA", 1, 2, 0), ("RT", 0, 2, 1, 0),
    ("FA", 1, 2, 0), ("RT", 0, 2, 1, 1), ("YS", 1, 3, 1), ("YS", 1, 2, 1), ("SA", 1, 2, 1),
    ("FA", 1, 3, 1), ("YS", 1, 2, 0), ("FA", 1, 3, 0), ("E", 1, 1), ("E", 1, 1), ("RT", 0, 2, 2, 1),
    ("RT", 0, 2, 2, 0), ("E", 1, 1), ("E", 1, 1), ("E", 1, 1), ("E", 1, 1), ("RT", 0, 1, 1, 0),
    ("RT", 0, 1, 1, 1), ("E", 1, 1), ("E", 1, 1), ("RT", 0, 1, 2, 1), ("AW", 1, "yo", 3, 0),
    ("AW", 1, "yo", 3, 1), ("RT", 0, 1, 2, 0), ("AW", 1, "yy", 3, 1), ("AW", 1, "yy", 3, 0),
    ("AW", 1, "yy", 2, 1), ("AW", 1, "yo", 2, 0), ("AW", 0, "yy", 0, 0), ("SY", 1, 3, 0),
    ("SY", 1, 3, 1), ("RL", 1, 3, 1), ("RL", 1, 3, 0), ("AW", 1, "yy", 2, 0), ("AW", 1, "yo", 1, 0),
    ("AW", 1, "yo", 1, 1), ("AW", 1, "yo", 2, 1), ("SY", 1, 2, 0), ("RT", 1, 3, 4, 1),
    ("RT", 1, 3, 4, 0), ("RL", 0, 0, 0), ("RH", 0), ("SY", 1, 2, 1), ("RL", 1, 2, 1),
    ("AW", 1, "yy", 1, 1), ("RT", 0, 0, 1, 0), ("SY", 1, 1, 0), ("AW", 1, "yo", 0, 0),
    ("SY", 1, 1, 1), ("RT", 1, 3, 5, 0), ("AW", 1, "yy", 1, 0), ("RT", 1, 3, 5, 1), ("RL", 1, 2, 0),
    ("RL", 1, 1, 1), ("AW", 1, "yy", 0, 0), ("RT", 1, 2, 4, 1), ("RP", 0, 1), ("RT", 0, 0, 2, 0),
    ("RT", 1, 2, 5, 0), ("SY", 1, 0, 0), ("RT", 1, 2, 4, 0), ("RL", 1, 1, 0), ("RP", 0, 2),
    ("RF", 0), ("RT", 1, 2, 5, 1), ("RT", 1, 1, 5, 0), ("RT", 1, 1, 4, 1), ("RT", 1, 1, 4, 0),
    ("RT", 1, 1, 5, 1), ("RL", 1, 0, 0), ("RT", 1, 0, 4, 0), ("RH", 1), ("RT", 1, 0, 5, 0),
    ("RP", 1, 5), ("RP", 1, 4), ("RF", 1),
)
MESH = pl.DeviceIdType.MESH


def coords():
    return lax.axis_index("grp"), lax.axis_index("sp"), lax.axis_index("tp")


def routed_pool(pool_input, pool_weight, pool_scale):
    n_tp = lax.axis_size("tp")
    seg_rows, channels = pool_input.shape
    last_rows = pool_input[seg_rows - reach_back :]
    before = passed_along(last_rows, "sp", 1)
    extended = jnp.concatenate([before, pool_input], axis=0).astype(jnp.float32)
    first_chan = lax.axis_index("tp") * channels
    chan_group = (first_chan + lax.iota(jnp.int32, channels)) // GROUP_DIM
    positions = lax.axis_index("sp") * seg_rows + lax.iota(jnp.int32, seg_rows)
    window = jnp.zeros((channels,), jnp.int32)
    for group_level, win_len in enumerate(pool_windows):
        window = jnp.where(chan_group == group_level, win_len, window)
    running = jnp.zeros((seg_rows, channels), jnp.float32)
    window_sum = running
    for offset in range(pool_windows[-1]):
        running = running + extended[reach_back - offset : reach_back - offset + seg_rows]
        if offset + 1 in pool_windows:
            window_sum = jnp.where(window[None, :] == offset + 1, running, window_sum)
    divisor = jnp.minimum(positions[:, None] + 1, window[None, :]).astype(jnp.float32)
    mixed_rows = (window_sum / divisor - extended[reach_back:]).astype(jnp.bfloat16)
    token_mixed = lax.all_to_all(mixed_rows, "tp", split_axis=0, concat_axis=1, tiled=True)
    tok_rows = token_mixed.shape[0]
    pooled = jnp.einsum(
        "tgc,gcd->tgd",
        token_mixed.reshape(tok_rows, GROUPS, GROUP_DIM),
        pool_weight,
        preferred_element_type=jnp.float32,
    )
    pooled = (
        (pooled * pool_scale.reshape(GROUPS, GROUP_DIM)).astype(jnp.bfloat16).reshape(tok_rows, -1)
    )
    return pooled


def layer_kernel(n_tp, cuts, rcuts, pool_ref, pw_ref, scale_ref, ow_ref, resid_ref, mgain_ref, fgain_ref,
                 pgain_ref, routes_ref, rweight_ref, wg_ref, wu_ref, wd_ref, out_ref,
                 pool, rows_in, pw, residual, pooled, mix,
                 every, metas, picks, weights, held, wg, wu, wd,
                 work, from_core, za, zb, ya, yb,
                 psend, precv, hsend, hrecv, fsem,
                 send, recv, msend, mrecv, wsem,
                 csend, crecv, asend, arecv, bsend, brecv, ysend, yrecv, own):
    grp, sp, tp = coords()
    yy, core = sp // 2, sp % 2
    yo = 1 - yy
    y_other = yo * 2 + core
    c_other = yy * 2 + (1 - core)
    tok, width = residual.shape
    local_experts, buffers = wg_ref.shape[0], wg.shape[0]
    slots = local_experts * SLOT
    chunk = width
    others = [(a, b) for a in range(4) for b in range(n_tp) if (a, b) != (0, 0)]

    def weight_copies(e):
        at = lax.rem(e, buffers)
        return [pltpu.make_async_copy(w.at[e], buf.at[at], wsem.at[i, at])
                for i, (w, buf) in enumerate(((wg_ref, wg), (wu_ref, wu), (wd_ref, wd)))]

    loads = [pltpu.make_async_copy(a, b, fsem.at[i]) for i, (a, b) in enumerate(
        ((pool_ref, pool), (pw_ref, pw), (resid_ref, residual)))]
    blocks = [(y, t) for y in range(2) for t in range(n_tp)]
    loads += [pltpu.make_async_copy(ow_ref.at[pl.ds(i * tok, tok)], from_core.at[y, t], fsem.at[3 + i])
              for i, (y, t) in enumerate(blocks)]
    for c in loads:
        c.start()
    barrier = pltpu.get_barrier_semaphore()
    for by in others:
        target = (grp, (sp + by[0]) % 4, (tp + by[1]) % n_tp)
        pl.semaphore_signal(barrier, inc=1, device_id=target, device_id_type=MESH)
    metas[sp, tp] = token_meta(routes_ref, rweight_ref, local_experts * 4)
    loads[0].wait()
    pl.semaphore_wait(barrier, len(others))

    def meta_copy(number, by):
        return pltpu.make_async_remote_copy(
            src_ref=metas.at[sp, tp], dst_ref=metas.at[sp, tp],
            send_sem=msend.at[number], recv_sem=mrecv.at[number],
            device_id=(grp, (sp + by[0]) % 4, (tp + by[1]) % n_tp), device_id_type=MESH)

    seg_rows, reach = pool.shape[0], SLOT
    first = tp == 0
    rest = tp > 0
    has_next = sp + 1 < 4

    half = tok // 2
    rows_h = [pl.ds(h * half, half) for h in range(2)]

    def ends(h, to, whole, chan):
        if h:
            at = pl.multiple_of(to * tok + half, half)
            return pool.at[pl.ds(at, half)], rows_in.at[chan, pl.ds(reach + half, half)]
        if whole:
            at = pl.multiple_of(to * tok - reach, reach)
            return pool.at[pl.ds(at, half + reach)], rows_in.at[chan, pl.ds(0, half + reach)]
        return pool.at[pl.ds(0, half)], rows_in.at[chan, pl.ds(reach, half)]

    def spread(h, by, whole):
        to = (tp + by) % n_tp
        src, dst = ends(h, to, whole, tp)
        return pltpu.make_async_remote_copy(
            src_ref=src, dst_ref=dst, send_sem=psend.at[h, by], recv_sem=precv.at[h, tp],
            device_id=(grp, sp, to), device_id_type=MESH)

    def landed(h, chan, whole):
        src, dst = ends(h, 1 if whole else 0, whole, chan)
        return pltpu.make_async_remote_copy(
            src_ref=src, dst_ref=dst, send_sem=psend.at[h, 0], recv_sem=precv.at[h, chan],
            device_id=(grp, sp, tp), device_id_type=MESH)

    def halo(chan):
        return pltpu.make_async_remote_copy(
            src_ref=pool.at[pl.ds(seg_rows - reach, reach)],
            dst_ref=rows_in.at[chan, pl.ds(0, reach)],
            send_sem=hsend.at[0], recv_sem=hrecv.at[chan],
            device_id=(grp, sp + 1, 0), device_id_type=MESH)

    def kept(h, whole):
        src, dst = ends(h, tp, whole, tp)
        return pltpu.make_async_copy(src, dst, own.at[h, 1])

    def each_spread(act):
        for h in range(2):
            for by in range(n_tp - 1, 0, -1):
                for to in (tp + by, tp - by):
                    rank = lax.rem(to - tp + n_tp, n_tp)
                    good = jnp.logical_and(to >= 0, to < n_tp)
                    if h:
                        pl.when(good)(lambda r=rank: act(spread(1, r, True)))
                        continue
                    pl.when(jnp.logical_and(good, to == 0))(lambda r=rank: act(spread(0, r, False)))
                    pl.when(jnp.logical_and(good, to > 0))(lambda r=rank: act(spread(0, r, True)))

    pl.when(has_next)(lambda: halo(tp).start())
    each_spread(lambda c: c.start())
    pl.when(first)(lambda: kept(0, False).start())
    pl.when(rest)(lambda: kept(0, True).start())
    kept(1, True).start()
    for number, by in enumerate(others):
        meta_copy(number, by).start()
    for e in range(min(buffers, local_experts)):
        for c in weight_copies(e):
            c.start()

    @pl.when(jnp.logical_and(first, sp == 0))
    def _():
        for chan in range(n_tp):
            rows_in[chan, pl.ds(0, reach)] = jnp.zeros((reach, rows_in.shape[2]), rows_in.dtype)

    start = (sp * n_tp + tp) * tok

    def pool_group(h, group, window):
        mine = tp == group
        if h:
            pl.when(mine)(lambda: kept(1, True).wait())
            pl.when(tp != group)(lambda: landed(1, group, True).wait_recv())
        else:
            pl.when(mine)(lambda: kept(0, group > 0).wait())
            if group:
                pl.when(first)(lambda: landed(0, group, False).wait_recv())
                pl.when(jnp.logical_and(rest, tp != group))(lambda: landed(0, group, True).wait_recv())
            else:
                pl.when(rest)(lambda: landed(0, 0, True).wait_recv())
            pl.when(jnp.logical_and(first, sp > 0))(lambda: halo(group).wait_recv())
        values = rows_in[group, pl.ds(h * half, half + reach)].astype(jnp.float32)
        total = values
        span = 1
        while span < window:
            total = total + jnp.concatenate([total[:span], total[:-span]], axis=0)
            span *= 2
        count = start + h * half + lax.broadcasted_iota(jnp.int32, (half, values.shape[1]), 0) + 1
        divisor = jnp.minimum(count, window).astype(jnp.float32)
        mixed = (total[reach:] / divisor - values[reach:]).astype(jnp.bfloat16)
        product = jnp.dot(mixed, pw[group], preferred_element_type=jnp.float32)
        cols = slice(group * GROUP_DIM, (group + 1) * GROUP_DIM)
        pooled[rows_h[h], cols] = (product * scale_ref[:, cols]).astype(jnp.bfloat16)

    def pool_half(h):
        if h == 0:
            loads[1].wait()
        for group, window in enumerate(pool_windows):
            pool_group(h, group, window)
        if h == 0:
            for c in loads[2:]:
                c.wait()

        def project(i, carry):
            at = pl.ds(pl.multiple_of(i * 1024, 1024), 1024)
            mix[rows_h[h], at] = jnp.dot(
                pooled[rows_h[h]], from_core[:, :, :, at].reshape(pooled.shape[1], 1024),
                preferred_element_type=jnp.float32)
            return carry

        lax.fori_loop(0, width // 1024, project, 0)

    def norm_rows(part):
        begin, count = cuts[part][:2]

        def body(i, carry):
            at = pl.ds(pl.multiple_of(begin + i * SLOT, SLOT), SLOT)
            after = residual[at].astype(jnp.float32) + rms_scale(mix[at], mgain_ref[...])
            after = after.astype(jnp.bfloat16)
            residual[at] = after
            every[sp, tp, at] = rms_scale(after.astype(jnp.float32), fgain_ref[...]).astype(jnp.bfloat16)
            return carry

        lax.fori_loop(0, count // SLOT, body, 0)

    def copy(s, t, part, way):
        target = [(grp, sp, tp + 1), (grp, sp, tp - 1), (grp, y_other, tp), (grp, c_other, tp)][way]
        first, count = cuts[part][:2]
        piece = every.at[s, t, pl.ds(first, count)]
        return pltpu.make_async_remote_copy(
            src_ref=piece, dst_ref=piece,
            send_sem=send.at[s, t, part, way], recv_sem=recv.at[s, t, part],
            device_id=target, device_id_type=MESH)

    def arrived(s, t, part):
        copy(s, t, part, 3).wait_recv()

    def allowed(cond, way):
        if way == 0:
            return jnp.logical_and(cond, tp + 1 < n_tp)
        if way == 1:
            return jnp.logical_and(cond, tp > 0)
        return cond

    def push(cond, s, t, part, way):
        pl.when(allowed(cond, way))(lambda: copy(s, t, part, way).start())

    def source_rows(s, t):
        return pl.ds(pl.multiple_of((t * 4 + s) * SLOT, SLOT), SLOT)

    half = tok // 2
    rows_h = [pl.ds(h * half, half) for h in range(2)]
    parts_h = [[p for p, c in enumerate(cuts) if c[2] == h] for h in range(2)]
    rparts_h = [[p for p, c in enumerate(rcuts) if c[2] == h] for h in range(2)]

    def select(h, s, t):
        slot = lax.broadcasted_iota(jnp.int32, (slots, half), 0).astype(jnp.float32)
        base = (sp * slots).astype(jnp.float32)
        meta = metas[s, t][:, h * half : (h + 1) * half]
        pick = jnp.zeros((slots, half), jnp.float32)
        weight = jnp.zeros((slots, half), jnp.float32)
        for k in range(TOP):
            hit = (meta[k : k + 1] - base) == slot
            pick = pick + jnp.where(hit, 1.0, 0.0)
            weight = weight + jnp.where(hit, meta[TOP + k : TOP + k + 1], 0.0)
        weight = jnp.broadcast_to(jnp.sum(weight, axis=1, keepdims=True), (slots, 128))
        pick = pick.astype(jnp.bfloat16)
        picks[h, s, t] = pick
        for e in range(local_experts):
            weights[h, e, source_rows(s, t)] = weight[e * SLOT : (e + 1) * SLOT]

        def body(i, carry):
            at = pl.ds(pl.multiple_of(i * chunk, chunk), chunk)
            got = jnp.dot(pick, every[s, t, rows_h[h], at], preferred_element_type=jnp.float32)
            got = got.astype(jnp.bfloat16)
            for e in range(local_experts):
                held[h, e, source_rows(s, t), at] = got[e * SLOT : (e + 1) * SLOT]
            return carry

        lax.fori_loop(0, width // chunk, body, 0)

    yes = tp >= 0
    far_core = yo * 2 + (1 - core)

    def own_way(h, way):
        for p in parts_h[h]:
            push(yes, sp, tp, p, way)

    def crossed(h):
        p = parts_h[h][0]
        arrived(y_other, tp, p)
        push(yes, y_other, tp, p, 0)
        push(yes, y_other, tp, p, 1)
        push(yes, y_other, tp, p, 3)

    by_dist = [((tp, yes),)] + [
        ((tp - d, tp >= d), (tp + d, tp + d < n_tp)) for d in range(1, n_tp)]

    def sides(dist):
        return by_dist[dist]

    def over_y(h, dist, p, side):
        t, cond = sides(dist)[side]
        pl.when(cond)(functools.partial(arrived, y_other, t, p))
        push(cond, y_other, t, p, 3)

    def select_from(h, s, dist, side):
        t, cond = sides(dist)[side]
        pl.when(cond)(functools.partial(select, h, s, t))

    def cross(h, s, t):
        for p in parts_h[h]:
            arrived(s, t, p)
        select(h, s, t)

    def over_core(h, s, dist, side):
        t, cond = sides(dist)[side]
        pl.when(cond)(functools.partial(cross, h, s, t))

    def along(h, dist, p, s, side):
        t, cond = sides(dist)[side]
        pl.when(cond)(functools.partial(arrived, s, t, p))
        push(cond, s, t, p, side)
        if p != parts_h[h][0]:
            push(cond, s, t, p, 2)
        push(cond, s, t, p, 3)

    def sent_all(h):
        head, tail = parts_h[h][0], parts_h[h][1:]
        sent = [(yes, sp, tp, p, way) for p in parts_h[h] for way in range(4)]
        sent += [(yes, y_other, tp, head, way) for way in (0, 1, 3)]
        sent += [(yes, y_other, tp, p, 3) for p in tail]
        for dist in range(1, n_tp):
            for side, (t, cond) in enumerate(sides(dist)):
                sent += [(cond, sp, t, p, way) for p in tail for way in (side, 2, 3)]
                sent += [(cond, s, t, head, way) for s in (sp, y_other) for way in (side, 3)]
                sent += [(cond, y_other, t, p, 3) for p in tail]
        for cond, s, t, p, way in sent:
            pl.when(allowed(cond, way))(lambda s=s, t=t, p=p, way=way: copy(s, t, p, way).wait_send())

    def use_expert(h, e, at_rows):
        at = lax.rem(e, buffers)
        rows = held[h, e, at_rows]
        gate_pre = jnp.dot(rows, wg[at], preferred_element_type=jnp.float32)
        upward = jnp.dot(rows, wu[at], preferred_element_type=jnp.float32)
        scale = jnp.concatenate([weights[h, e, at_rows]] * (gate_pre.shape[1] // 128), axis=1)
        activated = (clamped_unit(gate_pre, upward) * scale).astype(jnp.bfloat16)
        term = jnp.dot(activated, wd[at], preferred_element_type=jnp.float32)
        held[h, e, at_rows] = term.astype(jnp.bfloat16)

    def begin_weights(e, cond):
        @pl.when(cond)
        def _():
            for c in weight_copies(e):
                c.start()

    def end_weights(e, cond):
        @pl.when(cond)
        def _():
            for c in weight_copies(e):
                c.wait()

    def experts(h, far, between):
        pair = n_tp // 2
        group = tp // pair
        group = 1 - group if far else group
        count = pair * 4 * SLOT
        at_rows = pl.ds(pl.multiple_of(group * count, count), count)
        fresh = h == 0 and not far

        def body(j, carry):
            e = local_experts - 1 - j if far else j
            end_weights(e, j >= (0 if fresh else buffers))
            use_expert(h, e, at_rows)
            later = e - buffers if far else e + buffers
            begin_weights(later, jnp.logical_and(later >= 0, later < local_experts))
            for number, steps in between:
                pl.when(j == number)(functools.partial(run, steps))
            return carry

        lax.fori_loop(0, local_experts, body, 0)

    def combined(h, s, t, at):
        term = held[h, :, source_rows(s, t), at].reshape(slots, chunk)
        return lax.dot_general(picks[h, s, t], term, (((0,), (0,)), ((), ())),
                               preferred_element_type=jnp.float32)

    rows_of = [pl.ds(c[0], c[1]) for c in rcuts]
    ups, downs = (grp, sp, tp + 1), (grp, sp, tp - 1)
    up_ok, down_ok = tp + 1 < n_tp, tp > 0

    def remote(src, dst, s_sem, r_sem, target):
        return pltpu.make_async_remote_copy(
            src_ref=src, dst_ref=dst, send_sem=s_sem, recv_sem=r_sem,
            device_id=target, device_id_type=MESH)

    def core_copy(h, y, t):
        return remote(every.at[y * 2 + (1 - core), t, rows_h[h]], from_core.at[y, t, rows_h[h]],
                      csend.at[h, y, t], crecv.at[h, y, t], (grp, c_other, tp))

    def combine_away(h, y, t):
        s = y * 2 + (1 - core)

        def body(i, carry):
            at = pl.ds(pl.multiple_of(i * chunk, chunk), chunk)
            every[s, t, rows_h[h], at] = combined(h, s, t, at).astype(jnp.bfloat16)
            return carry

        lax.fori_loop(0, width // chunk, body, 0)
        core_copy(h, y, t).start()

    order = []
    for dist in range(n_tp - 1, -1, -1):
        for side in (1, -1) if dist else (1,):
            t = tp + side * dist
            order.append((jnp.logical_and(t >= 0, t < n_tp), t, side, (dist, int(side < 0))))

    def y_copy_b(p, t):
        rows = rows_of[p]
        return remote(work.at[yo, t, rows], yb.at[t, rows], ysend.at[p, t], yrecv.at[p, t],
                      (grp, y_other, tp))

    def y_copy_a(h):
        p = rparts_h[h][0]
        return remote(work.at[yo, tp, rows_of[p]], ya.at[h, pl.ds(0, rcuts[p][1])], ysend.at[p, 0], yrecv.at[p, 0],
                      (grp, y_other, tp))

    def local(h, y, t):
        s = y * 2 + core
        core_copy(h, y, t).wait_recv()

        def body(i, carry):
            at = pl.ds(pl.multiple_of(i * chunk, chunk), chunk)
            both = combined(h, s, t, at) + from_core[y, t, rows_h[h], at].astype(jnp.float32)
            work[y, t, rows_h[h], at] = both.astype(jnp.bfloat16)
            return carry

        lax.fori_loop(0, width // chunk, body, 0)

    def z_ends(p, y, t, slot):
        rows, h = rows_of[p], rcuts[p][2]
        if p == rparts_h[h][0]:
            return work.at[y, t, rows], za.at[h, y, slot, pl.ds(0, rcuts[p][1])], asend.at[h, y, t], arecv.at[h, y, slot]
        return work.at[y, t, rows], zb.at[slot, rows], bsend.at[p, t], brecv.at[p, slot]

    def z_copy(p, y, t, side):
        if side == 1:
            slot, target = t, ups
        else:
            slot, target = jnp.where(t == tp - 1, n_tp, t), downs
        return remote(*z_ends(p, y, t, slot), target)

    def take_z(p, y, t, slot):
        remote(*z_ends(p, y, t, slot), ups).wait_recv()
        dst, src = z_ends(p, y, t, slot)[:2]
        add_into(dst, src)

    def z_step(p, y, t, side):
        inner = tp > 0 if side == 1 else tp + 1 < n_tp
        pl.when(inner)(lambda: take_z(p, y, t, t))
        z_copy(p, y, t, side).start()

    def z_end(p, y):
        pl.when(down_ok)(lambda: take_z(p, y, tp, tp))
        pl.when(up_ok)(lambda: take_z(p, y, tp, n_tp))

    def aways(h, y, want):
        for ok, t, side, dist in order:
            if dist == want:
                pl.when(ok)(functools.partial(combine_away, h, y, t))

    def send_y(h, dists):
        for ok, t, side, dist in order:
            if dist == dists:
                @pl.when(ok)
                def _(t=t):
                    local(h, yo, t)
                    for p in rparts_h[h][1:]:
                        y_copy_b(p, t).start()

    def reduce_local(h, want):
        head = rparts_h[h][0]
        for ok, t, side, dist in order:
            if dist != want:
                continue

            @pl.when(ok)
            def _(t=t, side=side, dist=dist):
                local(h, yy, t)
                if dist[0]:
                    z_step(head, yo, t, side)
                    z_step(head, yy, t, side)

    def reduce_part(p, want):
        for ok, t, side, dist in order:
            if dist != want:
                continue

            @pl.when(ok)
            def _(t=t, side=side, dist=dist):
                y_copy_b(p, t).wait_recv()
                add_into(work.at[yy, t, rows_of[p]], yb.at[t, rows_of[p]])
                if dist[0]:
                    z_step(p, yy, t, side)

    def reduce_head(h):
        head = rparts_h[h][0]
        z_end(head, yo)
        y_copy_a(h).start()
        z_end(head, yy)

    def reduce_last(h):
        head = rparts_h[h][0]
        y_copy_a(h).wait_recv()
        add_into(work.at[yy, tp, rows_of[head]], ya.at[h, pl.ds(0, rcuts[head][1])])
        finish_rows(h)

    def reduce_sent(h):
        head, tail = rparts_h[h][0], rparts_h[h][1:]
        y_copy_a(h).wait_send()
        for ok, t, side, dist in order:
            @pl.when(ok)
            def _(t=t, side=side, dist=dist):
                core_copy(h, yo, t).wait_send()
                core_copy(h, yy, t).wait_send()
                for p in tail:
                    y_copy_b(p, t).wait_send()
                if dist[0]:
                    z_copy(head, yo, t, side).wait_send()
                    z_copy(head, yy, t, side).wait_send()
                    for p in tail:
                        z_copy(p, yy, t, side).wait_send()

    def finish_rows(h):
        def body(i, carry):
            at = pl.ds(pl.multiple_of(h * half + i * SLOT, SLOT), SLOT)
            total = work[yy, tp, at].astype(jnp.float32)
            done = residual[at].astype(jnp.float32) + rms_scale(total, pgain_ref[...])
            out_ref[at] = done.astype(out_ref.dtype)
            return carry

        lax.fori_loop(0, half // SLOT, body, 0)

    def step(kind, h, *at):
        if kind == "P":
            pool_half(h)
        elif kind == "N":
            norm_rows(at[0])
        elif kind == "OZ":
            push(yes, sp, tp, at[0], at[1])
        elif kind == "OY":
            push(yes, sp, tp, at[0], 2)
        elif kind == "OC":
            own_way(h, 3)
        elif kind == "X":
            crossed(h)
        elif kind == "F":
            along(h, at[0], at[1], sp if at[2] == "own" else y_other, at[3])
        elif kind == "SA":
            select_from(h, sp, *at)
        elif kind == "YA":
            over_y(h, *at)
        elif kind == "YS":
            select_from(h, y_other, *at)
        elif kind == "CO":
            over_core(h, c_other, *at)
        elif kind == "FA":
            over_core(h, far_core, *at)
        elif kind == "W":
            sent_all(h)
        elif kind == "M":
            for number, by in enumerate(others):
                meta_copy(number, by).wait()
        elif kind == "AW":
            aways(h, yo if at[0] == "yo" else yy, at[1:])
        elif kind == "SY":
            send_y(h, at)
        elif kind == "RL":
            reduce_local(h, at)
        elif kind == "RT":
            reduce_part(at[1], (at[0], at[2]))
        elif kind == "RH":
            reduce_head(h)
        elif kind == "RP":
            z_end(at[0], yy)
        elif kind == "RF":
            reduce_last(h)

    def run(steps):
        for one in steps:
            step(*one)

    todo, waited = [], set()
    for one in ORDER:
        if one[0] == "AW" and one[1] not in waited:
            waited.add(one[1])
            todo.append(("W", one[1]))
        if one[0] in ("SA", "YS", "CO", "FA") and "M" not in waited:
            waited.add("M")
            todo.append(("M", 0))
        todo.append(one)
    while todo:
        one = todo.pop(0)
        if one[0] != "E":
            step(*one)
            continue
        h, far, between, seen = one[1], one[2] > 0, [], 0
        while seen < local_experts - 1:
            one = todo.pop(0)
            if one[0] == "E":
                seen += 1
            elif between and between[-1][0] == seen:
                between[-1][1].append(one)
            else:
                between.append((seen, [one]))
        experts(h, far, between)
    reduce_sent(0)
    reduce_sent(1)
    pl.when(has_next)(lambda: halo(tp).wait_send())
    each_spread(lambda c: c.wait_send())


def cut_rows(halves):
    cuts, at = [], 0
    for h, counts in enumerate(halves):
        for count in counts:
            cuts.append((at, count, h))
            at += count
    return tuple(cuts)


def token_meta(routes_ref, rweight_ref, n_experts):
    tok = routes_ref.shape[1]
    expert = lax.broadcasted_iota(jnp.int32, (n_experts, tok), 0)
    hits = [jnp.where(expert == routes_ref[k : k + 1], 1.0, 0.0) for k in range(TOP)]
    earlier = (lax.broadcasted_iota(jnp.int32, (tok, tok), 0)
               < lax.broadcasted_iota(jnp.int32, (tok, tok), 1))
    earlier = jnp.where(earlier, 1.0, 0.0).astype(jnp.bfloat16)
    before = jnp.dot(sum(hits).astype(jnp.bfloat16), earlier, preferred_element_type=jnp.float32)
    line = lax.broadcasted_iota(jnp.int32, (2 * TOP, tok), 0)
    meta = jnp.zeros((2 * TOP, tok), jnp.float32)
    for k in range(TOP):
        rank = jnp.sum(hits[k] * before, axis=0, keepdims=True)
        place = routes_ref[k : k + 1].astype(jnp.float32) * SLOT + rank
        meta = jnp.where(line == k, place, meta)
        meta = jnp.where(line == TOP + k, rweight_ref[k : k + 1], meta)
    return meta


def add_into(dst, src):
    rows = dst.shape[0]
    strip = 16

    def body(i, carry):
        at = pl.ds(pl.multiple_of(i * strip, strip), strip)
        dst[at] = (dst[at].astype(jnp.float32) + src[at].astype(jnp.float32)).astype(dst.dtype)
        return carry

    lax.fori_loop(0, rows // strip, body, 0)


def fused_layer(resid_in, pool_input, pool_weight, pool_scale, out_weight, mix_gain, ffn_gain,
                w_gate, w_up, w_down, routes, route_weight, post_gain):
    n_tp = lax.axis_size("tp")
    tok, width = resid_in.shape
    local_experts, _, hidden = w_gate.shape
    cuts, rcuts = cut_rows(HALVES), cut_rows(BACK)
    parts, rparts = len(cuts), len(rcuts)
    heads = [counts[0] for counts in BACK]
    vmem, hbm = pl.BlockSpec(memory_space=pltpu.VMEM), pl.BlockSpec(memory_space=pl.ANY)
    kind = resid_in.dtype
    slots, buffers = local_experts * SLOT, min(4, local_experts)
    channels = pool_input.shape[1]
    dma = pltpu.SemaphoreType.DMA
    return pl.pallas_call(
        functools.partial(layer_kernel, n_tp, cuts, rcuts),
        out_shape=jax.ShapeDtypeStruct((tok, width), kind),
        in_specs=[hbm, hbm, vmem, hbm, hbm, vmem, vmem, vmem, vmem, vmem, hbm, hbm, hbm],
        out_specs=vmem,
        scratch_shapes=[
            pltpu.VMEM(pool_input.shape, kind),
            pltpu.VMEM((n_tp, tok + SLOT, channels), kind),
            pltpu.VMEM(pool_weight.shape, kind),
            pltpu.VMEM((tok, width), kind),
            pltpu.VMEM((tok, n_tp * channels), kind),
            pltpu.VMEM((tok, width), jnp.float32),
            pltpu.VMEM((4, n_tp, tok, width), kind),
            pltpu.VMEM((4, n_tp, 2 * TOP, tok), jnp.float32),
            pltpu.VMEM((2, 4, n_tp, slots, tok // 2), kind),
            pltpu.VMEM((2, local_experts, 4 * n_tp * SLOT, 128), jnp.float32),
            pltpu.VMEM((2, local_experts, 4 * n_tp * SLOT, width), kind),
            pltpu.VMEM((buffers, width, hidden), kind),
            pltpu.VMEM((buffers, width, hidden), kind),
            pltpu.VMEM((buffers, hidden, width), kind),
            pltpu.VMEM((2, n_tp, tok, width), kind),
            pltpu.VMEM((2, n_tp, tok, width), kind),
            pltpu.VMEM((2, 2, n_tp + 1, max(heads), width), kind),
            pltpu.VMEM((n_tp + 1, tok, width), kind),
            pltpu.VMEM((2, max(heads), width), kind),
            pltpu.VMEM((n_tp, tok, width), kind),
            dma((2, n_tp)),
            dma((2, n_tp)),
            dma((1,)),
            dma((n_tp,)),
            dma((3 + 2 * n_tp,)),
            dma((4, n_tp, parts, 4)),
            dma((4, n_tp, parts)),
            dma((4 * n_tp - 1,)),
            dma((4 * n_tp - 1,)),
            dma((3, buffers)),
            dma((2, 2, n_tp)),
            dma((2, 2, n_tp)),
            dma((2, 2, n_tp)),
            dma((2, 2, n_tp + 1)),
            dma((rparts, n_tp)),
            dma((rparts, n_tp + 1)),
            dma((rparts, n_tp)),
            dma((rparts, n_tp)),
            dma((2, max(2, n_tp))),
        ],
        compiler_params=pltpu.CompilerParams(
            collective_id=0, has_side_effects=True, vmem_limit_bytes=60 * 2**20
        ),
        name="fused_layer",
    )(pool_input, pool_weight, pool_scale[None], out_weight, resid_in, mix_gain[None], ffn_gain[None],
      post_gain[None], routes.T, route_weight.T, w_gate, w_up, w_down)


def per_device(
    resid_in,
    pool_input,
    pool_weight,
    pool_scale,
    out_weight,
    mix_gain,
    ffn_gain,
    w_gate,
    w_up,
    w_down,
    routes,
    route_weight,
    post_gain,
):
    n_sp = lax.axis_size("sp")
    n_tp = lax.axis_size("tp")
    seg_rows, channels = pool_input.shape
    tok_rows, width = resid_in.shape
    if (
        n_sp == 4
        and n_tp == GROUPS
        and channels == GROUP_DIM
        and seg_rows == n_tp * 128
        and tok_rows == 128
        and w_gate.shape[2] <= 256
        and w_gate.shape[0] <= 8
        and width <= 2048
        and out_weight.shape[0] == 2 * n_tp * tok_rows
    ):
        return fused_layer(resid_in, pool_input, pool_weight, pool_scale, out_weight, mix_gain,
                           ffn_gain, w_gate, w_up, w_down, routes, route_weight, post_gain)
    pooled = routed_pool(pool_input, pool_weight, pool_scale)
    mix_out = jnp.dot(pooled, out_weight, preferred_element_type=jnp.float32)
    residual = (resid_in.astype(jnp.float32) + rms_scale(mix_out, mix_gain)).astype(jnp.bfloat16)
    normed = rms_scale(residual.astype(jnp.float32), ffn_gain).astype(jnp.bfloat16)
    local_experts = w_gate.shape[0]
    n_experts = local_experts * n_sp
    slot_total = n_experts * CAP
    flat_route = routes.reshape(-1)
    onehot = (flat_route[:, None] == lax.iota(jnp.int32, n_experts)[None, :]).astype(jnp.int32)
    slot_rank = jnp.sum((jnp.cumsum(onehot, axis=0) - onehot) * onehot, axis=1)
    slot_index = flat_route * CAP + slot_rank
    picker = slot_index[:, None] == lax.iota(jnp.int32, slot_total)[None, :]
    picker_rows = picker.astype(jnp.bfloat16)
    token_pick = jnp.sum(
        picker.reshape(tok_rows, TOP, slot_total).astype(jnp.float32), axis=1
    ).astype(jnp.bfloat16)
    buffer = lax.dot_general(
        token_pick, normed, (((0,), (0,)), ((), ())), preferred_element_type=jnp.float32
    )
    outgoing = buffer.astype(jnp.bfloat16).reshape(n_sp, local_experts * CAP, width)
    at_owner = lax.all_to_all(outgoing, "sp", split_axis=0, concat_axis=0, tiled=True)
    arrived = lax.all_gather(at_owner[:, None], "tp", axis=1, tiled=True)
    arrived = arrived.reshape(n_sp, n_tp, local_experts, CAP, width)
    gate_pre = jnp.einsum("sklcd,ldf->sklcf", arrived, w_gate, preferred_element_type=jnp.float32)
    upward = jnp.einsum("sklcd,ldf->sklcf", arrived, w_up, preferred_element_type=jnp.float32)
    activated = clamped_unit(gate_pre, upward).astype(jnp.bfloat16)
    terms = jnp.einsum("sklcf,lfd->kslcd", activated, w_down, preferred_element_type=jnp.float32)
    summed = lax.psum_scatter(
        terms.reshape(1 * lax.axis_size("tp"), n_sp, local_experts * CAP, width).astype(
            jnp.bfloat16
        ),
        "tp",
        scatter_dimension=0,
        tiled=True,
    ).astype(jnp.float32)
    results = summed[0].astype(jnp.bfloat16)
    returned = lax.all_to_all(results, "sp", split_axis=0, concat_axis=0, tiled=True).reshape(
        slot_total, width
    )
    gathered = jnp.dot(picker_rows, returned, preferred_element_type=jnp.float32)
    expert_mix = jnp.sum(gathered.reshape(tok_rows, TOP, width) * route_weight[:, :, None], axis=1)
    return (residual.astype(jnp.float32) + rms_scale(expert_mix, post_gain)).astype(jnp.bfloat16)


def solution(mesh):
    in_specs = (
        P(("grp", "sp", "tp"), None),
        P(("grp", "sp"), "tp"),
        P(),
        P(),
        P(),
        P(),
        P(),
        P("sp", None, "tp"),
        P("sp", None, "tp"),
        P("sp", "tp", None),
        P(("grp", "sp", "tp"), None),
        P(("grp", "sp", "tp"), None),
        P(),
    )
    out_specs = P(("grp", "sp", "tp"), None)
    return jax.shard_map(
        per_device, mesh=mesh, in_specs=in_specs, out_specs=out_specs, check_vma=False
    )
```

```python
import functools

import jax
import jax.numpy as jnp
from jax import lax
from jax.experimental import pallas as pl
from jax.experimental.pallas import tpu as pltpu
from jax.sharding import PartitionSpec as P

GROUPS = 4
GROUP_DIM = 256
TOP = 2
CAP = 9


pool_windows = (2, 4, 8, 16)
reach_back = 15
norm_eps = 1e-06
clamp_limit = 7.0
glu_alpha = 1.702


def passed_along(x, axis, by):
    size = lax.axis_size(axis)
    pairs = [(i, i + by) for i in range(size) if 0 <= i + by < size]
    return lax.ppermute(x, axis, pairs)


def rms_scale(values, gain_vec):
    inverse = lax.rsqrt(jnp.mean(values * values, axis=-1, keepdims=True) + norm_eps)
    return values * inverse * gain_vec


def clamped_unit(gate_pre, upward):
    gate_clip = jnp.minimum(gate_pre, clamp_limit)
    linear = jnp.clip(upward, -clamp_limit, clamp_limit)
    return gate_clip * jax.nn.sigmoid(glu_alpha * gate_clip) * (linear + 1.0)


SLOT = 16
HALVES = ((16, 16, 32), (16, 16, 32))
BACK = ((16, 16, 32), (16, 16, 32))
ORDER = (
    ("P", 0), ("N", 0, 1), ("OY", 0, 1), ("N", 0, 0), ("OZ", 0, 1, 1), ("OZ", 0, 1, 0), ("N", 0, 2),
    ("OY", 0, 2), ("OZ", 0, 2, 1), ("OZ", 0, 2, 0), ("P", 1), ("F", 0, 1, 1, "own", 1),
    ("OZ", 0, 0, 0), ("F", 0, 1, 1, "own", 0), ("OZ", 0, 0, 1), ("OY", 0, 0),
    ("F", 0, 1, 2, "own", 0), ("N", 1, 3), ("F", 0, 1, 2, "own", 1), ("SA", 0, 0, 0),
    ("YA", 0, 0, 2, 0), ("N", 1, 5), ("F", 0, 1, 0, "own", 0), ("YA", 0, 1, 1, 1), ("X", 0),
    ("F", 0, 1, 0, "own", 1), ("F", 0, 2, 1, "own", 1), ("F", 0, 2, 1, "own", 0), ("OC", 0),
    ("CO", 0, 1, 0), ("N", 1, 4), ("YA", 0, 0, 1, 0), ("FA", 0, 0, 0), ("F", 0, 2, 2, "own", 0),
    ("YA", 0, 1, 1, 0), ("F", 0, 2, 2, "own", 1), ("CO", 0, 0, 0), ("F", 0, 1, 0, "yo", 1),
    ("OY", 1, 4), ("SA", 0, 1, 0), ("YA", 0, 1, 2, 0), ("SA", 1, 0, 0), ("OC", 1),
    ("F", 0, 1, 0, "yo", 0), ("YS", 0, 1, 0), ("YS", 0, 0, 0), ("F", 0, 2, 0, "own", 1),
    ("OY", 1, 3), ("SA", 0, 1, 1), ("F", 0, 2, 0, "own", 0), ("YA", 0, 1, 2, 1), ("YS", 0, 1, 1),
    ("F", 0, 3, 1, "own", 0), ("CO", 0, 2, 1), ("F", 0, 3, 1, "own", 1), ("CO", 0, 1, 1),
    ("FA", 0, 1, 0), ("CO", 1, 0, 0), ("OZ", 1, 4, 1), ("FA", 0, 1, 1), ("SA", 0, 2, 0),
    ("E", 0, 0), ("OZ", 1, 4, 0), ("E", 0, 0), ("E", 0, 0), ("F", 0, 3, 2, "own", 0),
    ("CO", 0, 2, 0), ("F", 0, 3, 2, "own", 1), ("YA", 0, 2, 2, 0), ("E", 0, 0), ("OY", 1, 5),
    ("YA", 0, 2, 2, 1), ("F", 0, 2, 0, "yo", 1), ("F", 0, 2, 0, "yo", 0), ("OZ", 1, 5, 1),
    ("YA", 0, 2, 1, 1), ("YA", 0, 2, 1, 0), ("OZ", 1, 5, 0), ("E", 0, 0), ("SA", 0, 2, 1),
    ("E", 0, 0), ("E", 0, 0), ("E", 0, 0), ("YA", 0, 3, 1, 1), ("YA", 1, 0, 4, 0),
    ("F", 1, 1, 4, "own", 1), ("F", 0, 3, 0, "own", 0), ("YA", 0, 3, 1, 0),
    ("F", 0, 3, 0, "own", 1), ("FA", 0, 2, 0), ("F", 1, 1, 4, "own", 0), ("SA", 0, 3, 1),
    ("SA", 0, 3, 0), ("YA", 0, 3, 2, 0), ("YA", 0, 3, 2, 1), ("F", 0, 3, 0, "yo", 0),
    ("YS", 0, 3, 0), ("FA", 0, 2, 1), ("F", 0, 3, 0, "yo", 1), ("YS", 0, 3, 1), ("CO", 0, 3, 1),
    ("CO", 0, 3, 0), ("YS", 0, 2, 0), ("FA", 0, 3, 0), ("YS", 0, 2, 1), ("FA", 0, 3, 1),
    ("E", 0, 1), ("E", 0, 1), ("F", 1, 1, 5, "own", 0), ("F", 1, 1, 5, "own", 1), ("OZ", 1, 3, 0),
    ("E", 0, 1), ("OZ", 1, 3, 1), ("YA", 1, 0, 5, 0), ("X", 1), ("E", 0, 1), ("YS", 1, 0, 0),
    ("YA", 1, 1, 4, 1), ("F", 1, 2, 4, "own", 0), ("E", 0, 1), ("F", 1, 2, 4, "own", 1),
    ("E", 0, 1), ("E", 0, 1), ("F", 1, 2, 5, "own", 0), ("F", 1, 2, 5, "own", 1), ("E", 0, 1),
    ("AW", 0, "yo", 3, 0), ("AW", 0, "yo", 3, 1), ("AW", 0, "yo", 2, 1), ("AW", 0, "yy", 3, 1),
    ("F", 1, 1, 3, "own", 0), ("YA", 1, 1, 5, 0), ("AW", 0, "yy", 3, 0), ("FA", 1, 0, 0),
    ("AW", 0, "yo", 1, 1), ("YA", 1, 1, 4, 0), ("F", 1, 1, 3, "own", 1), ("SY", 0, 3, 1),
    ("AW", 0, "yo", 2, 0), ("F", 1, 1, 3, "yo", 0), ("SA", 1, 1, 1), ("SA", 1, 1, 0),
    ("SY", 0, 3, 0), ("AW", 0, "yy", 2, 1), ("YA", 1, 1, 5, 1), ("F", 1, 1, 3, "yo", 1),
    ("YS", 1, 1, 1), ("RL", 0, 3, 0), ("YS", 1, 1, 0), ("AW", 0, "yy", 1, 0), ("AW", 0, "yy", 1, 1),
    ("RL", 0, 3, 1), ("AW", 0, "yy", 2, 0), ("YA", 1, 2, 4, 0), ("CO", 1, 1, 0), ("FA", 1, 1, 0),
    ("F", 1, 3, 4, "own", 0), ("CO", 1, 1, 1), ("F", 1, 3, 4, "own", 1), ("FA", 1, 1, 1),
    ("E", 1, 0), ("E", 1, 0), ("RT", 0, 3, 1, 1), ("RT", 0, 3, 1, 0), ("YA", 1, 2, 5, 1),
    ("YA", 1, 2, 4, 1), ("E", 1, 0), ("F", 1, 3, 5, "own", 0), ("F", 1, 3, 5, "own", 1),
    ("YA", 1, 2, 5, 0), ("SY", 0, 2, 0), ("RL", 0, 2, 0), ("AW", 0, "yo", 0, 0),
    ("AW", 0, "yo", 1, 0), ("SY", 0, 2, 1), ("F", 1, 2, 3, "own", 1), ("RL", 0, 2, 1),
    ("F", 1, 2, 3, "own", 0), ("E", 1, 0), ("E", 1, 0), ("RT", 0, 3, 2, 1), ("RT", 0, 3, 2, 0),
    ("F", 1, 2, 3, "yo", 0), ("F", 1, 2, 3, "yo", 1), ("SY", 0, 1, 1), ("CO", 1, 2, 0), ("E", 1, 0),
    ("YS", 1, 2, 1), ("E", 1, 0), ("SY", 0, 1, 0), ("YA", 1, 3, 4, 1), ("RL", 0, 1, 0),
    ("F", 1, 3, 3, "own", 1), ("YA", 1, 3, 4, 0), ("SY", 0, 0, 0), ("E", 1, 0), ("CO", 1, 3, 1),
    ("YA", 1, 3, 5, 1), ("F", 1, 3, 3, "own", 0), ("YA", 1, 3, 5, 0), ("F", 1, 3, 3, "yo", 1),
    ("FA", 1, 2, 0), ("RL", 0, 1, 1), ("SA", 1, 2, 1), ("SA", 1, 3, 1), ("SA", 1, 2, 0),
    ("RT", 0, 2, 1, 0), ("FA", 1, 2, 1), ("CO", 1, 2, 1), ("YS", 1, 3, 1), ("F", 1, 3, 3, "yo", 0),
    ("SA", 1, 3, 0), ("YS", 1, 3, 0), ("CO", 1, 3, 0), ("RT", 0, 2, 1, 1), ("YS", 1, 2, 0),
    ("FA", 1, 3, 1), ("FA", 1, 3, 0), ("E", 1, 1), ("E", 1, 1), ("RT", 0, 2, 2, 0), ("E", 1, 1),
    ("RT", 0, 2, 2, 1), ("E", 1, 1), ("E", 1, 1), ("E", 1, 1), ("RT", 0, 1, 1, 0),
    ("RT", 0, 1, 1, 1), ("E", 1, 1), ("E", 1, 1), ("AW", 1, "yo", 3, 1), ("AW", 1, "yo", 2, 1),
    ("RT", 0, 1, 2, 0), ("AW", 1, "yo", 3, 0), ("AW", 1, "yo", 1, 1), ("RT", 0, 1, 2, 1),
    ("AW", 1, "yy", 3, 1), ("AW", 1, "yy", 3, 0), ("AW", 1, "yo", 2, 0), ("SY", 1, 3, 1),
    ("AW", 1, "yo", 0, 0), ("SY", 1, 3, 0), ("RL", 1, 3, 0), ("AW", 1, "yy", 2, 0),
    ("AW", 1, "yy", 2, 1), ("SY", 1, 2, 0), ("AW", 1, "yy", 1, 0), ("AW", 1, "yy", 1, 1),
    ("AW", 1, "yy", 0, 0), ("RL", 1, 3, 1), ("RT", 1, 3, 4, 1), ("AW", 1, "yo", 1, 0),
    ("SY", 1, 2, 1), ("RL", 1, 2, 0), ("RT", 1, 3, 5, 1), ("SY", 1, 1, 1), ("AW", 0, "yy", 0, 0),
    ("RL", 0, 0, 0), ("RL", 1, 2, 1), ("RT", 1, 2, 5, 1), ("SY", 1, 1, 0), ("RT", 0, 0, 2, 0),
    ("RP", 0, 2), ("RH", 0), ("RT", 1, 3, 4, 0), ("RT", 1, 2, 4, 1), ("RT", 1, 3, 5, 0),
    ("RT", 1, 2, 4, 0), ("RT", 1, 2, 5, 0), ("RL", 1, 1, 0), ("RL", 1, 1, 1), ("RT", 1, 1, 4, 0),
    ("SY", 1, 0, 0), ("RT", 0, 0, 1, 0), ("RT", 1, 1, 5, 1), ("RT", 1, 1, 5, 0), ("RP", 0, 1),
    ("RF", 0), ("RT", 1, 1, 4, 1), ("RL", 1, 0, 0), ("RH", 1), ("RT", 1, 0, 5, 0),
    ("RT", 1, 0, 4, 0), ("RP", 1, 5), ("RP", 1, 4), ("RF", 1),
)
MESH = pl.DeviceIdType.MESH


def coords():
    return lax.axis_index("grp"), lax.axis_index("sp"), lax.axis_index("tp")


def routed_pool(pool_input, pool_weight, pool_scale):
    n_tp = lax.axis_size("tp")
    seg_rows, channels = pool_input.shape
    last_rows = pool_input[seg_rows - reach_back :]
    before = passed_along(last_rows, "sp", 1)
    extended = jnp.concatenate([before, pool_input], axis=0).astype(jnp.float32)
    first_chan = lax.axis_index("tp") * channels
    chan_group = (first_chan + lax.iota(jnp.int32, channels)) // GROUP_DIM
    positions = lax.axis_index("sp") * seg_rows + lax.iota(jnp.int32, seg_rows)
    window = jnp.zeros((channels,), jnp.int32)
    for group_level, win_len in enumerate(pool_windows):
        window = jnp.where(chan_group == group_level, win_len, window)
    running = jnp.zeros((seg_rows, channels), jnp.float32)
    window_sum = running
    for offset in range(pool_windows[-1]):
        running = running + extended[reach_back - offset : reach_back - offset + seg_rows]
        if offset + 1 in pool_windows:
            window_sum = jnp.where(window[None, :] == offset + 1, running, window_sum)
    divisor = jnp.minimum(positions[:, None] + 1, window[None, :]).astype(jnp.float32)
    mixed_rows = (window_sum / divisor - extended[reach_back:]).astype(jnp.bfloat16)
    token_mixed = lax.all_to_all(mixed_rows, "tp", split_axis=0, concat_axis=1, tiled=True)
    tok_rows = token_mixed.shape[0]
    pooled = jnp.einsum(
        "tgc,gcd->tgd",
        token_mixed.reshape(tok_rows, GROUPS, GROUP_DIM),
        pool_weight,
        preferred_element_type=jnp.float32,
    )
    pooled = (
        (pooled * pool_scale.reshape(GROUPS, GROUP_DIM)).astype(jnp.bfloat16).reshape(tok_rows, -1)
    )
    return pooled


def layer_kernel(n_tp, cuts, rcuts, pool_ref, pw_ref, scale_ref, ow_ref, resid_ref, mgain_ref, fgain_ref,
                 pgain_ref, routes_ref, rweight_ref, wg_ref, wu_ref, wd_ref, out_ref,
                 pool, rows_in, pw, residual, pooled, mix,
                 every, metas, picks, weights, held, wg, wu, wd,
                 work, from_core, za, zb, ya, yb,
                 psend, precv, hsend, hrecv, fsem,
                 send, recv, msend, mrecv, wsem,
                 csend, crecv, asend, arecv, bsend, brecv, ysend, yrecv, own):
    grp, sp, tp = coords()
    yy, core = sp // 2, sp % 2
    yo = 1 - yy
    y_other = yo * 2 + core
    c_other = yy * 2 + (1 - core)
    tok, width = residual.shape
    local_experts, buffers = wg_ref.shape[0], wg.shape[0]
    slots = local_experts * SLOT
    chunk = width
    others = [(a, b) for a in range(4) for b in range(n_tp) if (a, b) != (0, 0)]

    def weight_copies(e):
        at = lax.rem(e, buffers)
        return [pltpu.make_async_copy(w.at[e], buf.at[at], wsem.at[i, at])
                for i, (w, buf) in enumerate(((wg_ref, wg), (wu_ref, wu), (wd_ref, wd)))]

    loads = [pltpu.make_async_copy(a, b, fsem.at[i]) for i, (a, b) in enumerate(
        ((pool_ref, pool), (pw_ref, pw), (resid_ref, residual)))]
    blocks = [(y, t) for y in range(2) for t in range(n_tp)]
    loads += [pltpu.make_async_copy(ow_ref.at[pl.ds(i * tok, tok)], from_core.at[y, t], fsem.at[3 + i])
              for i, (y, t) in enumerate(blocks)]
    for c in loads:
        c.start()
    barrier = pltpu.get_barrier_semaphore()
    for by in others:
        target = (grp, (sp + by[0]) % 4, (tp + by[1]) % n_tp)
        pl.semaphore_signal(barrier, inc=1, device_id=target, device_id_type=MESH)
    metas[sp, tp] = token_meta(routes_ref, rweight_ref, local_experts * 4)
    loads[0].wait()
    pl.semaphore_wait(barrier, len(others))

    def meta_copy(number, by):
        return pltpu.make_async_remote_copy(
            src_ref=metas.at[sp, tp], dst_ref=metas.at[sp, tp],
            send_sem=msend.at[number], recv_sem=mrecv.at[number],
            device_id=(grp, (sp + by[0]) % 4, (tp + by[1]) % n_tp), device_id_type=MESH)

    seg_rows, reach = pool.shape[0], SLOT
    first = tp == 0
    rest = tp > 0
    has_next = sp + 1 < 4

    half = tok // 2
    rows_h = [pl.ds(h * half, half) for h in range(2)]

    def ends(h, to, whole, chan):
        if h:
            at = pl.multiple_of(to * tok + half, half)
            return pool.at[pl.ds(at, half)], rows_in.at[chan, pl.ds(reach + half, half)]
        if whole:
            at = pl.multiple_of(to * tok - reach, reach)
            return pool.at[pl.ds(at, half + reach)], rows_in.at[chan, pl.ds(0, half + reach)]
        return pool.at[pl.ds(0, half)], rows_in.at[chan, pl.ds(reach, half)]

    def spread(h, by, whole):
        to = (tp + by) % n_tp
        src, dst = ends(h, to, whole, tp)
        return pltpu.make_async_remote_copy(
            src_ref=src, dst_ref=dst, send_sem=psend.at[h, by], recv_sem=precv.at[h, tp],
            device_id=(grp, sp, to), device_id_type=MESH)

    def landed(h, chan, whole):
        src, dst = ends(h, 1 if whole else 0, whole, chan)
        return pltpu.make_async_remote_copy(
            src_ref=src, dst_ref=dst, send_sem=psend.at[h, 0], recv_sem=precv.at[h, chan],
            device_id=(grp, sp, tp), device_id_type=MESH)

    def halo(chan):
        return pltpu.make_async_remote_copy(
            src_ref=pool.at[pl.ds(seg_rows - reach, reach)],
            dst_ref=rows_in.at[chan, pl.ds(0, reach)],
            send_sem=hsend.at[0], recv_sem=hrecv.at[chan],
            device_id=(grp, sp + 1, 0), device_id_type=MESH)

    def kept(h, whole):
        src, dst = ends(h, tp, whole, tp)
        return pltpu.make_async_copy(src, dst, own.at[h, 1])

    def each_spread(act):
        for h in range(2):
            for by in range(n_tp - 1, 0, -1):
                for to in (tp + by, tp - by):
                    rank = lax.rem(to - tp + n_tp, n_tp)
                    good = jnp.logical_and(to >= 0, to < n_tp)
                    if h:
                        pl.when(good)(lambda r=rank: act(spread(1, r, True)))
                        continue
                    pl.when(jnp.logical_and(good, to == 0))(lambda r=rank: act(spread(0, r, False)))
                    pl.when(jnp.logical_and(good, to > 0))(lambda r=rank: act(spread(0, r, True)))

    pl.when(has_next)(lambda: halo(tp).start())
    each_spread(lambda c: c.start())
    pl.when(first)(lambda: kept(0, False).start())
    pl.when(rest)(lambda: kept(0, True).start())
    kept(1, True).start()
    for number, by in enumerate(others):
        meta_copy(number, by).start()
    for e in range(min(buffers, local_experts)):
        for c in weight_copies(e):
            c.start()

    @pl.when(jnp.logical_and(first, sp == 0))
    def _():
        for chan in range(n_tp):
            rows_in[chan, pl.ds(0, reach)] = jnp.zeros((reach, rows_in.shape[2]), rows_in.dtype)

    start = (sp * n_tp + tp) * tok

    def pool_group(h, group, window):
        mine = tp == group
        if h:
            pl.when(mine)(lambda: kept(1, True).wait())
            pl.when(tp != group)(lambda: landed(1, group, True).wait_recv())
        else:
            pl.when(mine)(lambda: kept(0, group > 0).wait())
            if group:
                pl.when(first)(lambda: landed(0, group, False).wait_recv())
                pl.when(jnp.logical_and(rest, tp != group))(lambda: landed(0, group, True).wait_recv())
            else:
                pl.when(rest)(lambda: landed(0, 0, True).wait_recv())
            pl.when(jnp.logical_and(first, sp > 0))(lambda: halo(group).wait_recv())
        values = rows_in[group, pl.ds(h * half, half + reach)].astype(jnp.float32)
        total = values
        span = 1
        while span < window:
            total = total + jnp.concatenate([total[:span], total[:-span]], axis=0)
            span *= 2
        count = start + h * half + lax.broadcasted_iota(jnp.int32, (half, values.shape[1]), 0) + 1
        divisor = jnp.minimum(count, window).astype(jnp.float32)
        mixed = (total[reach:] / divisor - values[reach:]).astype(jnp.bfloat16)
        product = jnp.dot(mixed, pw[group], preferred_element_type=jnp.float32)
        cols = slice(group * GROUP_DIM, (group + 1) * GROUP_DIM)
        pooled[rows_h[h], cols] = (product * scale_ref[:, cols]).astype(jnp.bfloat16)

    def pool_half(h):
        if h == 0:
            loads[1].wait()
        for group, window in enumerate(pool_windows):
            pool_group(h, group, window)
        if h == 0:
            for c in loads[2:]:
                c.wait()

        def project(i, carry):
            at = pl.ds(pl.multiple_of(i * width, width), width)
            mix[rows_h[h], at] = jnp.dot(
                pooled[rows_h[h]], from_core[:, :, :, at].reshape(pooled.shape[1], width),
                preferred_element_type=jnp.float32)
            return carry

        project(0, 0)

    def norm_rows(part):
        begin, count = cuts[part][:2]

        def body(i, carry):
            at = pl.ds(pl.multiple_of(begin + i * SLOT, SLOT), SLOT)
            after = residual[at].astype(jnp.float32) + rms_scale(mix[at], mgain_ref[...])
            after = after.astype(jnp.bfloat16)
            residual[at] = after
            every[sp, tp, at] = rms_scale(after.astype(jnp.float32), fgain_ref[...]).astype(jnp.bfloat16)
            return carry

        lax.fori_loop(0, count // SLOT, body, 0)

    def copy(s, t, part, way):
        target = [(grp, sp, tp + 1), (grp, sp, tp - 1), (grp, y_other, tp), (grp, c_other, tp)][way]
        first, count = cuts[part][:2]
        piece = every.at[s, t, pl.ds(first, count)]
        return pltpu.make_async_remote_copy(
            src_ref=piece, dst_ref=piece,
            send_sem=send.at[s, t, part, way], recv_sem=recv.at[s, t, part],
            device_id=target, device_id_type=MESH)

    def arrived(s, t, part):
        copy(s, t, part, 3).wait_recv()

    def allowed(cond, way):
        if way == 0:
            return jnp.logical_and(cond, tp + 1 < n_tp)
        if way == 1:
            return jnp.logical_and(cond, tp > 0)
        return cond

    def push(cond, s, t, part, way):
        pl.when(allowed(cond, way))(lambda: copy(s, t, part, way).start())

    def source_rows(s, t):
        return pl.ds(pl.multiple_of((t * 4 + s) * SLOT, SLOT), SLOT)

    half = tok // 2
    rows_h = [pl.ds(h * half, half) for h in range(2)]
    parts_h = [[p for p, c in enumerate(cuts) if c[2] == h] for h in range(2)]
    rparts_h = [[p for p, c in enumerate(rcuts) if c[2] == h] for h in range(2)]

    def select(h, s, t):
        slot = lax.broadcasted_iota(jnp.int32, (slots, half), 0).astype(jnp.float32)
        base = (sp * slots).astype(jnp.float32)
        meta = metas[s, t][:, h * half : (h + 1) * half]
        pick = jnp.zeros((slots, half), jnp.float32)
        weight = jnp.zeros((slots, half), jnp.float32)
        for k in range(TOP):
            hit = (meta[k : k + 1] - base) == slot
            pick = pick + jnp.where(hit, 1.0, 0.0)
            weight = weight + jnp.where(hit, meta[TOP + k : TOP + k + 1], 0.0)
        weight = jnp.broadcast_to(jnp.sum(weight, axis=1, keepdims=True), (slots, 128))
        pick = pick.astype(jnp.bfloat16)
        picks[h, s, t] = pick
        for e in range(local_experts):
            weights[h, e, source_rows(s, t)] = weight[e * SLOT : (e + 1) * SLOT]

        def body(i, carry):
            at = pl.ds(pl.multiple_of(i * chunk, chunk), chunk)
            got = jnp.dot(pick, every[s, t, rows_h[h], at], preferred_element_type=jnp.float32)
            got = got.astype(jnp.bfloat16)
            for e in range(local_experts):
                held[h, e, source_rows(s, t), at] = got[e * SLOT : (e + 1) * SLOT]
            return carry

        lax.fori_loop(0, width // chunk, body, 0)

    yes = tp >= 0
    far_core = yo * 2 + (1 - core)

    def own_way(h, way):
        for p in parts_h[h]:
            push(yes, sp, tp, p, way)

    def crossed(h):
        p = parts_h[h][0]
        arrived(y_other, tp, p)
        push(yes, y_other, tp, p, 0)
        push(yes, y_other, tp, p, 1)
        push(yes, y_other, tp, p, 3)

    by_dist = [((tp, yes),)] + [
        ((tp - d, tp >= d), (tp + d, tp + d < n_tp)) for d in range(1, n_tp)]

    def sides(dist):
        return by_dist[dist]

    def over_y(h, dist, p, side):
        t, cond = sides(dist)[side]
        pl.when(cond)(functools.partial(arrived, y_other, t, p))
        push(cond, y_other, t, p, 3)

    def select_from(h, s, dist, side):
        t, cond = sides(dist)[side]
        pl.when(cond)(functools.partial(select, h, s, t))

    def cross(h, s, t):
        for p in parts_h[h]:
            arrived(s, t, p)
        select(h, s, t)

    def over_core(h, s, dist, side):
        t, cond = sides(dist)[side]
        pl.when(cond)(functools.partial(cross, h, s, t))

    def along(h, dist, p, s, side):
        t, cond = sides(dist)[side]
        pl.when(cond)(functools.partial(arrived, s, t, p))
        push(cond, s, t, p, side)
        if p != parts_h[h][0]:
            push(cond, s, t, p, 2)
        push(cond, s, t, p, 3)

    def sent_all(h):
        head, tail = parts_h[h][0], parts_h[h][1:]
        sent = [(yes, sp, tp, p, way) for p in parts_h[h] for way in range(4)]
        sent += [(yes, y_other, tp, head, way) for way in (0, 1, 3)]
        sent += [(yes, y_other, tp, p, 3) for p in tail]
        for dist in range(1, n_tp):
            for side, (t, cond) in enumerate(sides(dist)):
                sent += [(cond, sp, t, p, way) for p in tail for way in (side, 2, 3)]
                sent += [(cond, s, t, head, way) for s in (sp, y_other) for way in (side, 3)]
                sent += [(cond, y_other, t, p, 3) for p in tail]
        for cond, s, t, p, way in sent:
            pl.when(allowed(cond, way))(lambda s=s, t=t, p=p, way=way: copy(s, t, p, way).wait_send())

    def use_expert(h, e, at_rows):
        at = lax.rem(e, buffers)
        rows = held[h, e, at_rows]
        gate_pre = jnp.dot(rows, wg[at], preferred_element_type=jnp.float32)
        upward = jnp.dot(rows, wu[at], preferred_element_type=jnp.float32)
        scale = jnp.concatenate([weights[h, e, at_rows]] * (gate_pre.shape[1] // 128), axis=1)
        activated = (clamped_unit(gate_pre, upward) * scale).astype(jnp.bfloat16)
        term = jnp.dot(activated, wd[at], preferred_element_type=jnp.float32)
        held[h, e, at_rows] = term.astype(jnp.bfloat16)

    def begin_weights(e, cond):
        @pl.when(cond)
        def _():
            for c in weight_copies(e):
                c.start()

    def end_weights(e, cond):
        @pl.when(cond)
        def _():
            for c in weight_copies(e):
                c.wait()

    def experts(h, far, between):
        pair = n_tp // 2
        group = tp // pair
        group = 1 - group if far else group
        count = pair * 4 * SLOT
        at_rows = pl.ds(pl.multiple_of(group * count, count), count)
        fresh = h == 0 and not far

        def body(j, carry):
            e = local_experts - 1 - j if far else j
            end_weights(e, j >= (0 if fresh else buffers))
            use_expert(h, e, at_rows)
            later = e - buffers if far else e + buffers
            begin_weights(later, jnp.logical_and(later >= 0, later < local_experts))
            for number, steps in between:
                pl.when(j == number)(functools.partial(run, steps))
            return carry

        lax.fori_loop(0, local_experts, body, 0)

    def combined(h, s, t, at):
        term = held[h, :, source_rows(s, t), at].reshape(slots, chunk)
        return lax.dot_general(picks[h, s, t], term, (((0,), (0,)), ((), ())),
                               preferred_element_type=jnp.float32)

    rows_of = [pl.ds(c[0], c[1]) for c in rcuts]
    ups, downs = (grp, sp, tp + 1), (grp, sp, tp - 1)
    up_ok, down_ok = tp + 1 < n_tp, tp > 0

    def remote(src, dst, s_sem, r_sem, target):
        return pltpu.make_async_remote_copy(
            src_ref=src, dst_ref=dst, send_sem=s_sem, recv_sem=r_sem,
            device_id=target, device_id_type=MESH)

    def core_copy(h, y, t):
        return remote(every.at[y * 2 + (1 - core), t, rows_h[h]], from_core.at[y, t, rows_h[h]],
                      csend.at[h, y, t], crecv.at[h, y, t], (grp, c_other, tp))

    def combine_away(h, y, t):
        s = y * 2 + (1 - core)

        def body(i, carry):
            at = pl.ds(pl.multiple_of(i * chunk, chunk), chunk)
            every[s, t, rows_h[h], at] = combined(h, s, t, at).astype(jnp.bfloat16)
            return carry

        lax.fori_loop(0, width // chunk, body, 0)
        core_copy(h, y, t).start()

    order = []
    for dist in range(n_tp - 1, -1, -1):
        for side in (1, -1) if dist else (1,):
            t = tp + side * dist
            order.append((jnp.logical_and(t >= 0, t < n_tp), t, side, (dist, int(side < 0))))

    def y_copy_b(p, t):
        rows = rows_of[p]
        return remote(work.at[yo, t, rows], yb.at[t, rows], ysend.at[p, t], yrecv.at[p, t],
                      (grp, y_other, tp))

    def y_copy_a(h):
        p = rparts_h[h][0]
        return remote(work.at[yo, tp, rows_of[p]], ya.at[h, pl.ds(0, rcuts[p][1])], ysend.at[p, 0], yrecv.at[p, 0],
                      (grp, y_other, tp))

    def local(h, y, t):
        s = y * 2 + core
        core_copy(h, y, t).wait_recv()

        def body(i, carry):
            at = pl.ds(pl.multiple_of(i * chunk, chunk), chunk)
            both = combined(h, s, t, at) + from_core[y, t, rows_h[h], at].astype(jnp.float32)
            work[y, t, rows_h[h], at] = both.astype(jnp.bfloat16)
            return carry

        lax.fori_loop(0, width // chunk, body, 0)

    def z_ends(p, y, t, slot):
        rows, h = rows_of[p], rcuts[p][2]
        if p == rparts_h[h][0]:
            return work.at[y, t, rows], za.at[h, y, slot, pl.ds(0, rcuts[p][1])], asend.at[h, y, t], arecv.at[h, y, slot]
        return work.at[y, t, rows], zb.at[slot, rows], bsend.at[p, t], brecv.at[p, slot]

    def z_copy(p, y, t, side):
        if side == 1:
            slot, target = t, ups
        else:
            slot, target = jnp.where(t == tp - 1, n_tp, t), downs
        return remote(*z_ends(p, y, t, slot), target)

    def take_z(p, y, t, slot):
        remote(*z_ends(p, y, t, slot), ups).wait_recv()
        dst, src = z_ends(p, y, t, slot)[:2]
        add_into(dst, src)

    def z_step(p, y, t, side):
        inner = tp > 0 if side == 1 else tp + 1 < n_tp
        pl.when(inner)(lambda: take_z(p, y, t, t))
        z_copy(p, y, t, side).start()

    def z_end(p, y):
        pl.when(down_ok)(lambda: take_z(p, y, tp, tp))
        pl.when(up_ok)(lambda: take_z(p, y, tp, n_tp))

    def aways(h, y, want):
        for ok, t, side, dist in order:
            if dist == want:
                pl.when(ok)(functools.partial(combine_away, h, y, t))

    def send_y(h, dists):
        for ok, t, side, dist in order:
            if dist == dists:
                @pl.when(ok)
                def _(t=t):
                    local(h, yo, t)
                    for p in rparts_h[h][1:]:
                        y_copy_b(p, t).start()

    def reduce_local(h, want):
        head = rparts_h[h][0]
        for ok, t, side, dist in order:
            if dist != want:
                continue

            @pl.when(ok)
            def _(t=t, side=side, dist=dist):
                local(h, yy, t)
                if dist[0]:
                    z_step(head, yo, t, side)
                    z_step(head, yy, t, side)

    def reduce_part(p, want):
        for ok, t, side, dist in order:
            if dist != want:
                continue

            @pl.when(ok)
            def _(t=t, side=side, dist=dist):
                y_copy_b(p, t).wait_recv()
                add_into(work.at[yy, t, rows_of[p]], yb.at[t, rows_of[p]])
                if dist[0]:
                    z_step(p, yy, t, side)

    def reduce_head(h):
        head = rparts_h[h][0]
        z_end(head, yo)
        y_copy_a(h).start()
        z_end(head, yy)

    def reduce_last(h):
        head = rparts_h[h][0]
        y_copy_a(h).wait_recv()
        add_into(work.at[yy, tp, rows_of[head]], ya.at[h, pl.ds(0, rcuts[head][1])])
        finish_rows(h)

    def reduce_sent(h):
        head, tail = rparts_h[h][0], rparts_h[h][1:]
        y_copy_a(h).wait_send()
        for ok, t, side, dist in order:
            @pl.when(ok)
            def _(t=t, side=side, dist=dist):
                core_copy(h, yo, t).wait_send()
                core_copy(h, yy, t).wait_send()
                for p in tail:
                    y_copy_b(p, t).wait_send()
                if dist[0]:
                    z_copy(head, yo, t, side).wait_send()
                    z_copy(head, yy, t, side).wait_send()
                    for p in tail:
                        z_copy(p, yy, t, side).wait_send()

    def finish_rows(h):
        def body(i, carry):
            at = pl.ds(pl.multiple_of(h * half + i * SLOT, SLOT), SLOT)
            total = work[yy, tp, at].astype(jnp.float32)
            done = residual[at].astype(jnp.float32) + rms_scale(total, pgain_ref[...])
            out_ref[at] = done.astype(out_ref.dtype)
            return carry

        lax.fori_loop(0, half // SLOT, body, 0)

    def step(kind, h, *at):
        if kind == "P":
            pool_half(h)
        elif kind == "N":
            norm_rows(at[0])
        elif kind == "OZ":
            push(yes, sp, tp, at[0], at[1])
        elif kind == "OY":
            push(yes, sp, tp, at[0], 2)
        elif kind == "OC":
            own_way(h, 3)
        elif kind == "X":
            crossed(h)
        elif kind == "F":
            along(h, at[0], at[1], sp if at[2] == "own" else y_other, at[3])
        elif kind == "SA":
            select_from(h, sp, *at)
        elif kind == "YA":
            over_y(h, *at)
        elif kind == "YS":
            select_from(h, y_other, *at)
        elif kind == "CO":
            over_core(h, c_other, *at)
        elif kind == "FA":
            over_core(h, far_core, *at)
        elif kind == "W":
            sent_all(h)
        elif kind == "WP":
            pl.when(has_next)(lambda: halo(tp).wait_send())
            each_spread(lambda c: c.wait_send())
        elif kind == "WR":
            reduce_sent(h)
        elif kind == "M":
            for number, by in enumerate(others):
                meta_copy(number, by).wait()
        elif kind == "AW":
            aways(h, yo if at[0] == "yo" else yy, at[1:])
        elif kind == "SY":
            send_y(h, at)
        elif kind == "RL":
            reduce_local(h, at)
        elif kind == "RT":
            reduce_part(at[1], (at[0], at[2]))
        elif kind == "RH":
            reduce_head(h)
        elif kind == "RP":
            z_end(at[0], yy)
        elif kind == "RF":
            reduce_last(h)

    def run(steps):
        for one in steps:
            step(*one)

    todo, waited = [], set()
    for one in ORDER:
        if one[0] in ("SA", "YS", "CO", "FA") and "M" not in waited:
            waited.add("M")
            todo.append(("M", 0))
        todo.append(one)
    late = [i for i, one in enumerate(todo) if one[:2] == ("RT", 1)]
    todo.insert(late[len(late) * 2 // 3] + 1, ("W", 1))
    todo.insert(late[len(late) // 3] + 1, ("W", 0))
    todo.insert(late[0] + 1, ("WP", 0))
    todo.insert(todo.index(("RF", 0)) + 1, ("WR", 0))
    while todo:
        one = todo.pop(0)
        if one[0] != "E":
            step(*one)
            continue
        h, far, between, seen = one[1], one[2] > 0, [], 0
        while seen < local_experts - 1:
            one = todo.pop(0)
            if one[0] == "E":
                seen += 1
            elif between and between[-1][0] == seen:
                between[-1][1].append(one)
            else:
                between.append((seen, [one]))
        experts(h, far, between)
    reduce_sent(1)


def cut_rows(halves):
    cuts, at = [], 0
    for h, counts in enumerate(halves):
        for count in counts:
            cuts.append((at, count, h))
            at += count
    return tuple(cuts)


def token_meta(routes_ref, rweight_ref, n_experts):
    tok = routes_ref.shape[1]
    expert = lax.broadcasted_iota(jnp.int32, (n_experts, tok), 0)
    hits = [jnp.where(expert == routes_ref[k : k + 1], 1.0, 0.0) for k in range(TOP)]
    earlier = (lax.broadcasted_iota(jnp.int32, (tok, tok), 0)
               < lax.broadcasted_iota(jnp.int32, (tok, tok), 1))
    earlier = jnp.where(earlier, 1.0, 0.0).astype(jnp.bfloat16)
    before = jnp.dot(sum(hits).astype(jnp.bfloat16), earlier, preferred_element_type=jnp.float32)
    line = lax.broadcasted_iota(jnp.int32, (2 * TOP, tok), 0)
    meta = jnp.zeros((2 * TOP, tok), jnp.float32)
    for k in range(TOP):
        rank = jnp.sum(hits[k] * before, axis=0, keepdims=True)
        place = routes_ref[k : k + 1].astype(jnp.float32) * SLOT + rank
        meta = jnp.where(line == k, place, meta)
        meta = jnp.where(line == TOP + k, rweight_ref[k : k + 1], meta)
    return meta


def add_into(dst, src):
    rows = dst.shape[0]
    strip = 16

    def body(i, carry):
        at = pl.ds(pl.multiple_of(i * strip, strip), strip)
        dst[at] = (dst[at].astype(jnp.float32) + src[at].astype(jnp.float32)).astype(dst.dtype)
        return carry

    lax.fori_loop(0, rows // strip, body, 0)


def fused_layer(resid_in, pool_input, pool_weight, pool_scale, out_weight, mix_gain, ffn_gain,
                w_gate, w_up, w_down, routes, route_weight, post_gain):
    n_tp = lax.axis_size("tp")
    tok, width = resid_in.shape
    local_experts, _, hidden = w_gate.shape
    cuts, rcuts = cut_rows(HALVES), cut_rows(BACK)
    parts, rparts = len(cuts), len(rcuts)
    heads = [counts[0] for counts in BACK]
    vmem, hbm = pl.BlockSpec(memory_space=pltpu.VMEM), pl.BlockSpec(memory_space=pl.ANY)
    kind = resid_in.dtype
    slots, buffers = local_experts * SLOT, min(4, local_experts)
    channels = pool_input.shape[1]
    dma = pltpu.SemaphoreType.DMA
    return pl.pallas_call(
        functools.partial(layer_kernel, n_tp, cuts, rcuts),
        out_shape=jax.ShapeDtypeStruct((tok, width), kind),
        in_specs=[hbm, hbm, vmem, hbm, hbm, vmem, vmem, vmem, vmem, vmem, hbm, hbm, hbm],
        out_specs=vmem,
        scratch_shapes=[
            pltpu.VMEM(pool_input.shape, kind),
            pltpu.VMEM((n_tp, tok + SLOT, channels), kind),
            pltpu.VMEM(pool_weight.shape, kind),
            pltpu.VMEM((tok, width), kind),
            pltpu.VMEM((tok, n_tp * channels), kind),
            pltpu.VMEM((tok, width), jnp.float32),
            pltpu.VMEM((4, n_tp, tok, width), kind),
            pltpu.VMEM((4, n_tp, 2 * TOP, tok), jnp.float32),
            pltpu.VMEM((2, 4, n_tp, slots, tok // 2), kind),
            pltpu.VMEM((2, local_experts, 4 * n_tp * SLOT, 128), jnp.float32),
            pltpu.VMEM((2, local_experts, 4 * n_tp * SLOT, width), kind),
            pltpu.VMEM((buffers, width, hidden), kind),
            pltpu.VMEM((buffers, width, hidden), kind),
            pltpu.VMEM((buffers, hidden, width), kind),
            pltpu.VMEM((2, n_tp, tok, width), kind),
            pltpu.VMEM((2, n_tp, tok, width), kind),
            pltpu.VMEM((2, 2, n_tp + 1, max(heads), width), kind),
            pltpu.VMEM((n_tp + 1, tok, width), kind),
            pltpu.VMEM((2, max(heads), width), kind),
            pltpu.VMEM((n_tp, tok, width), kind),
            dma((2, n_tp)),
            dma((2, n_tp)),
            dma((1,)),
            dma((n_tp,)),
            dma((3 + 2 * n_tp,)),
            dma((4, n_tp, parts, 4)),
            dma((4, n_tp, parts)),
            dma((4 * n_tp - 1,)),
            dma((4 * n_tp - 1,)),
            dma((3, buffers)),
            dma((2, 2, n_tp)),
            dma((2, 2, n_tp)),
            dma((2, 2, n_tp)),
            dma((2, 2, n_tp + 1)),
            dma((rparts, n_tp)),
            dma((rparts, n_tp + 1)),
            dma((rparts, n_tp)),
            dma((rparts, n_tp)),
            dma((2, max(2, n_tp))),
        ],
        compiler_params=pltpu.CompilerParams(
            collective_id=0, has_side_effects=True, vmem_limit_bytes=60 * 2**20
        ),
        name="fused_layer",
    )(pool_input, pool_weight, pool_scale[None], out_weight, resid_in, mix_gain[None], ffn_gain[None],
      post_gain[None], routes.T, route_weight.T, w_gate, w_up, w_down)


def per_device(
    resid_in,
    pool_input,
    pool_weight,
    pool_scale,
    out_weight,
    mix_gain,
    ffn_gain,
    w_gate,
    w_up,
    w_down,
    routes,
    route_weight,
    post_gain,
):
    n_sp = lax.axis_size("sp")
    n_tp = lax.axis_size("tp")
    seg_rows, channels = pool_input.shape
    tok_rows, width = resid_in.shape
    if (
        n_sp == 4
        and n_tp == GROUPS
        and channels == GROUP_DIM
        and seg_rows == n_tp * 128
        and tok_rows == 128
        and w_gate.shape[2] <= 256
        and w_gate.shape[0] <= 8
        and width <= 2048
        and out_weight.shape[0] == 2 * n_tp * tok_rows
    ):
        return fused_layer(resid_in, pool_input, pool_weight, pool_scale, out_weight, mix_gain,
                           ffn_gain, w_gate, w_up, w_down, routes, route_weight, post_gain)
    pooled = routed_pool(pool_input, pool_weight, pool_scale)
    mix_out = jnp.dot(pooled, out_weight, preferred_element_type=jnp.float32)
    residual = (resid_in.astype(jnp.float32) + rms_scale(mix_out, mix_gain)).astype(jnp.bfloat16)
    normed = rms_scale(residual.astype(jnp.float32), ffn_gain).astype(jnp.bfloat16)
    local_experts = w_gate.shape[0]
    n_experts = local_experts * n_sp
    slot_total = n_experts * CAP
    flat_route = routes.reshape(-1)
    onehot = (flat_route[:, None] == lax.iota(jnp.int32, n_experts)[None, :]).astype(jnp.int32)
    slot_rank = jnp.sum((jnp.cumsum(onehot, axis=0) - onehot) * onehot, axis=1)
    slot_index = flat_route * CAP + slot_rank
    picker = slot_index[:, None] == lax.iota(jnp.int32, slot_total)[None, :]
    picker_rows = picker.astype(jnp.bfloat16)
    token_pick = jnp.sum(
        picker.reshape(tok_rows, TOP, slot_total).astype(jnp.float32), axis=1
    ).astype(jnp.bfloat16)
    buffer = lax.dot_general(
        token_pick, normed, (((0,), (0,)), ((), ())), preferred_element_type=jnp.float32
    )
    outgoing = buffer.astype(jnp.bfloat16).reshape(n_sp, local_experts * CAP, width)
    at_owner = lax.all_to_all(outgoing, "sp", split_axis=0, concat_axis=0, tiled=True)
    arrived = lax.all_gather(at_owner[:, None], "tp", axis=1, tiled=True)
    arrived = arrived.reshape(n_sp, n_tp, local_experts, CAP, width)
    gate_pre = jnp.einsum("sklcd,ldf->sklcf", arrived, w_gate, preferred_element_type=jnp.float32)
    upward = jnp.einsum("sklcd,ldf->sklcf", arrived, w_up, preferred_element_type=jnp.float32)
    activated = clamped_unit(gate_pre, upward).astype(jnp.bfloat16)
    terms = jnp.einsum("sklcf,lfd->kslcd", activated, w_down, preferred_element_type=jnp.float32)
    summed = lax.psum_scatter(
        terms.reshape(1 * lax.axis_size("tp"), n_sp, local_experts * CAP, width).astype(
            jnp.bfloat16
        ),
        "tp",
        scatter_dimension=0,
        tiled=True,
    ).astype(jnp.float32)
    results = summed[0].astype(jnp.bfloat16)
    returned = lax.all_to_all(results, "sp", split_axis=0, concat_axis=0, tiled=True).reshape(
        slot_total, width
    )
    gathered = jnp.dot(picker_rows, returned, preferred_element_type=jnp.float32)
    expert_mix = jnp.sum(gathered.reshape(tok_rows, TOP, width) * route_weight[:, :, None], axis=1)
    return (residual.astype(jnp.float32) + rms_scale(expert_mix, post_gain)).astype(jnp.bfloat16)


def solution(mesh):
    in_specs = (
        P(("grp", "sp", "tp"), None),
        P(("grp", "sp"), "tp"),
        P(),
        P(),
        P(),
        P(),
        P(),
        P("sp", None, "tp"),
        P("sp", None, "tp"),
        P("sp", "tp", None),
        P(("grp", "sp", "tp"), None),
        P(("grp", "sp", "tp"), None),
        P(),
    )
    out_specs = P(("grp", "sp", "tp"), None)
    return jax.shard_map(
        per_device, mesh=mesh, in_specs=in_specs, out_specs=out_specs, check_vma=False
    )
```

```python
import functools

import jax
import jax.numpy as jnp
from jax import lax
from jax.experimental import pallas as pl
from jax.experimental.pallas import tpu as pltpu
from jax.sharding import PartitionSpec as P

GROUPS = 4
GROUP_DIM = 256
TOP = 2
CAP = 9


pool_windows = (2, 4, 8, 16)
reach_back = 15
norm_eps = 1e-06
clamp_limit = 7.0
glu_alpha = 1.702


def passed_along(x, axis, by):
    size = lax.axis_size(axis)
    pairs = [(i, i + by) for i in range(size) if 0 <= i + by < size]
    return lax.ppermute(x, axis, pairs)


def rms_scale(values, gain_vec):
    inverse = lax.rsqrt(jnp.mean(values * values, axis=-1, keepdims=True) + norm_eps)
    return values * inverse * gain_vec


def clamped_unit(gate_pre, upward):
    gate_clip = jnp.minimum(gate_pre, clamp_limit)
    linear = jnp.clip(upward, -clamp_limit, clamp_limit)
    return gate_clip * jax.nn.sigmoid(glu_alpha * gate_clip) * (linear + 1.0)


SLOT = 16
HALVES = ((16, 32, 16), (16, 16, 32))
BACK = ((16, 16, 32), (16, 16, 32))
ORDER = (
    ("P", 0), ("N", 0, 2), ("OZ", 0, 2, 1), ("OY", 0, 2), ("OZ", 0, 2, 0), ("N", 0, 0),
    ("OZ", 0, 0, 1), ("OY", 0, 0), ("N", 0, 1), ("OZ", 0, 1, 0), ("OZ", 0, 0, 0), ("OC", 0),
    ("OY", 0, 1), ("OZ", 0, 1, 1), ("F", 0, 1, 2, "own", 0), ("P", 1), ("F", 0, 1, 2, "own", 1),
    ("F", 0, 1, 1, "own", 0), ("X", 0), ("F", 0, 1, 0, "own", 0), ("YA", 0, 0, 2, 0),
    ("F", 0, 1, 1, "own", 1), ("F", 0, 1, 0, "own", 1), ("N", 1, 5), ("N", 1, 4),
    ("F", 0, 2, 2, "own", 0), ("SA", 0, 1, 0), ("OY", 1, 4), ("N", 1, 3), ("F", 0, 1, 0, "yo", 1),
    ("CO", 0, 1, 0), ("SA", 0, 1, 1), ("YA", 0, 1, 2, 1), ("SA", 1, 0, 0), ("YA", 0, 0, 1, 0),
    ("YA", 0, 1, 2, 0), ("OC", 1), ("CO", 0, 1, 1), ("F", 0, 2, 2, "own", 1),
    ("F", 0, 2, 1, "own", 0), ("CO", 0, 0, 0), ("YA", 0, 1, 1, 0), ("F", 0, 1, 0, "yo", 0),
    ("YS", 0, 0, 0), ("FA", 0, 0, 0), ("FA", 0, 1, 0), ("YS", 0, 1, 0), ("F", 0, 2, 0, "own", 0),
    ("OZ", 1, 4, 0), ("SA", 0, 0, 0), ("YA", 0, 1, 1, 1), ("F", 0, 2, 1, "own", 1), ("YS", 0, 1, 1),
    ("F", 0, 2, 0, "yo", 1), ("F", 0, 2, 0, "own", 1), ("OY", 1, 3), ("OZ", 1, 5, 1),
    ("FA", 0, 1, 1), ("E", 0, 0), ("E", 0, 0), ("OZ", 1, 4, 1), ("E", 0, 0),
    ("F", 0, 3, 2, "own", 0), ("YA", 0, 2, 2, 1), ("F", 0, 3, 2, "own", 1), ("E", 0, 0),
    ("CO", 0, 2, 1), ("F", 0, 3, 1, "own", 1), ("F", 0, 3, 1, "own", 0), ("CO", 1, 0, 0),
    ("E", 0, 0), ("YA", 0, 2, 2, 0), ("YA", 0, 2, 1, 1), ("F", 0, 2, 0, "yo", 0), ("CO", 0, 2, 0),
    ("YA", 0, 3, 2, 0), ("OY", 1, 5), ("SA", 0, 2, 0), ("YA", 0, 2, 1, 0), ("OZ", 1, 5, 0),
    ("E", 0, 0), ("F", 0, 3, 0, "own", 0), ("E", 0, 0), ("FA", 0, 2, 1), ("SA", 0, 2, 1),
    ("F", 0, 3, 0, "own", 1), ("FA", 0, 2, 0), ("YA", 0, 3, 2, 1), ("YS", 0, 2, 1),
    ("F", 1, 1, 4, "own", 0), ("CO", 0, 3, 0), ("F", 0, 3, 0, "yo", 1), ("YA", 0, 3, 1, 0),
    ("E", 0, 0), ("YA", 0, 3, 1, 1), ("SA", 0, 3, 1), ("CO", 0, 3, 1), ("YS", 0, 3, 1),
    ("F", 0, 3, 0, "yo", 0), ("YS", 0, 2, 0), ("YA", 1, 0, 4, 0), ("YS", 0, 3, 0),
    ("F", 1, 1, 5, "own", 1), ("SA", 0, 3, 0), ("FA", 0, 3, 1), ("FA", 0, 3, 0), ("OZ", 1, 3, 1),
    ("E", 0, 1), ("E", 0, 1), ("F", 1, 1, 4, "own", 1), ("F", 1, 1, 5, "own", 0), ("OZ", 1, 3, 0),
    ("X", 1), ("E", 0, 1), ("E", 0, 1), ("YA", 1, 0, 5, 0), ("E", 0, 1),
    ("F", 1, 2, 4, "own", 0), ("F", 1, 2, 5, "own", 1), ("E", 0, 1), ("E", 0, 1), ("E", 0, 1),
    ("YA", 1, 1, 5, 1), ("F", 1, 2, 5, "own", 0), ("AW", 0, "yo", 3, 1), ("AW", 0, "yo", 3, 0),
    ("AW", 0, "yy", 3, 1), ("F", 1, 2, 4, "own", 1), ("AW", 0, "yy", 3, 0), ("AW", 0, "yo", 2, 1),
    ("FA", 1, 0, 0), ("YA", 1, 1, 4, 0), ("AW", 0, "yy", 1, 0), ("AW", 0, "yo", 2, 0),
    ("AW", 0, "yo", 1, 1), ("F", 1, 1, 3, "own", 0), ("F", 1, 1, 3, "own", 1), ("SY", 0, 3, 0),
    ("YA", 1, 1, 4, 1), ("YS", 1, 0, 0), ("F", 1, 1, 3, "yo", 1), ("YA", 1, 1, 5, 0),
    ("SY", 0, 3, 1), ("F", 1, 1, 3, "yo", 0), ("YS", 1, 1, 0), ("RL", 0, 3, 1), ("RL", 0, 3, 0),
    ("AW", 0, "yy", 1, 1), ("YS", 1, 1, 1), ("SA", 1, 1, 0), ("AW", 0, "yy", 2, 0), ("SA", 1, 1, 1),
    ("CO", 1, 1, 1), ("CO", 1, 1, 0), ("FA", 1, 1, 1), ("FA", 1, 1, 0), ("AW", 0, "yy", 2, 1),
    ("E", 1, 0), ("E", 1, 0), ("RT", 0, 3, 1, 0), ("F", 1, 3, 5, "own", 1), ("YA", 1, 2, 5, 0),
    ("F", 1, 3, 4, "own", 1), ("RT", 0, 3, 1, 1), ("SY", 0, 2, 0), ("F", 1, 3, 4, "own", 0),
    ("F", 1, 3, 5, "own", 0), ("RL", 0, 2, 0), ("SY", 0, 2, 1), ("RL", 0, 2, 1), ("YA", 1, 2, 4, 1),
    ("E", 1, 0), ("F", 1, 2, 3, "own", 1), ("F", 1, 2, 3, "own", 0), ("AW", 0, "yo", 0, 0),
    ("E", 1, 0), ("RT", 0, 3, 2, 0), ("E", 1, 0), ("F", 1, 2, 3, "yo", 1), ("RT", 0, 3, 2, 1),
    ("AW", 0, "yo", 1, 0), ("F", 1, 2, 3, "yo", 0), ("E", 1, 0), ("SY", 0, 1, 1), ("E", 1, 0),
    ("RL", 0, 1, 1), ("SA", 1, 2, 0), ("YA", 1, 2, 5, 1), ("SY", 0, 1, 0), ("YA", 1, 3, 5, 1),
    ("YA", 1, 2, 4, 0), ("SY", 0, 0, 0), ("F", 1, 3, 3, "own", 0), ("RL", 0, 1, 0), ("E", 1, 0),
    ("YA", 1, 3, 5, 0), ("FA", 1, 2, 0), ("CO", 1, 2, 1), ("F", 1, 3, 3, "own", 1), ("SA", 1, 3, 1),
    ("FA", 1, 2, 1), ("F", 1, 3, 3, "yo", 1), ("YA", 1, 3, 4, 0), ("YS", 1, 2, 0),
    ("YA", 1, 3, 4, 1), ("F", 1, 3, 3, "yo", 0), ("CO", 1, 3, 0), ("SA", 1, 2, 1), ("YS", 1, 3, 1),
    ("SA", 1, 3, 0), ("RT", 0, 2, 1, 0), ("CO", 1, 3, 1), ("YS", 1, 2, 1), ("CO", 1, 2, 0),
    ("FA", 1, 3, 1), ("RT", 0, 2, 1, 1), ("YS", 1, 3, 0), ("FA", 1, 3, 0), ("E", 1, 1), ("E", 1, 1),
    ("RT", 0, 2, 2, 0), ("RT", 0, 2, 2, 1), ("E", 1, 1), ("E", 1, 1), ("RT", 0, 1, 1, 0),
    ("RT", 0, 1, 1, 1), ("E", 1, 1), ("E", 1, 1), ("E", 1, 1), ("RT", 0, 1, 2, 0), ("E", 1, 1),
    ("AW", 1, "yo", 3, 0), ("AW", 1, "yy", 3, 0), ("AW", 1, "yo", 2, 0), ("AW", 1, "yy", 2, 0),
    ("RT", 0, 1, 2, 1), ("AW", 1, "yo", 3, 1), ("AW", 1, "yy", 3, 1), ("AW", 1, "yo", 2, 1),
    ("AW", 1, "yy", 2, 1), ("AW", 0, "yy", 0, 0), ("SY", 1, 3, 1), ("SY", 1, 3, 0), ("RL", 1, 3, 1),
    ("AW", 1, "yo", 1, 1), ("RL", 1, 3, 0), ("SY", 1, 2, 1), ("AW", 1, "yy", 1, 0),
    ("AW", 1, "yy", 1, 1), ("RL", 1, 2, 1), ("RT", 1, 3, 5, 1), ("AW", 1, "yo", 1, 0),
    ("AW", 1, "yo", 0, 0), ("RT", 1, 3, 4, 1), ("SY", 1, 2, 0), ("RL", 1, 2, 0), ("SY", 1, 1, 1),
    ("RT", 1, 3, 4, 0), ("SY", 1, 1, 0), ("RL", 0, 0, 0), ("RH", 0), ("RT", 0, 0, 2, 0),
    ("RP", 0, 2), ("RT", 1, 2, 5, 1), ("AW", 1, "yy", 0, 0), ("RT", 1, 3, 5, 0), ("SY", 1, 0, 0),
    ("RT", 1, 2, 4, 0), ("RT", 1, 2, 5, 0), ("RT", 1, 2, 4, 1), ("RL", 1, 1, 1), ("RL", 1, 1, 0),
    ("RL", 1, 0, 0), ("RT", 1, 1, 5, 1), ("RT", 0, 0, 1, 0), ("RT", 1, 1, 5, 0), ("RT", 1, 1, 4, 1),
    ("RT", 1, 1, 4, 0), ("RH", 1), ("RP", 0, 1), ("RT", 1, 0, 5, 0), ("RP", 1, 5), ("RF", 0),
    ("RT", 1, 0, 4, 0), ("RP", 1, 4), ("RF", 1),
)
MESH = pl.DeviceIdType.MESH


def coords():
    return lax.axis_index("grp"), lax.axis_index("sp"), lax.axis_index("tp")


def routed_pool(pool_input, pool_weight, pool_scale):
    n_tp = lax.axis_size("tp")
    seg_rows, channels = pool_input.shape
    last_rows = pool_input[seg_rows - reach_back :]
    before = passed_along(last_rows, "sp", 1)
    extended = jnp.concatenate([before, pool_input], axis=0).astype(jnp.float32)
    first_chan = lax.axis_index("tp") * channels
    chan_group = (first_chan + lax.iota(jnp.int32, channels)) // GROUP_DIM
    positions = lax.axis_index("sp") * seg_rows + lax.iota(jnp.int32, seg_rows)
    window = jnp.zeros((channels,), jnp.int32)
    for group_level, win_len in enumerate(pool_windows):
        window = jnp.where(chan_group == group_level, win_len, window)
    running = jnp.zeros((seg_rows, channels), jnp.float32)
    window_sum = running
    for offset in range(pool_windows[-1]):
        running = running + extended[reach_back - offset : reach_back - offset + seg_rows]
        if offset + 1 in pool_windows:
            window_sum = jnp.where(window[None, :] == offset + 1, running, window_sum)
    divisor = jnp.minimum(positions[:, None] + 1, window[None, :]).astype(jnp.float32)
    mixed_rows = (window_sum / divisor - extended[reach_back:]).astype(jnp.bfloat16)
    token_mixed = lax.all_to_all(mixed_rows, "tp", split_axis=0, concat_axis=1, tiled=True)
    tok_rows = token_mixed.shape[0]
    pooled = jnp.einsum(
        "tgc,gcd->tgd",
        token_mixed.reshape(tok_rows, GROUPS, GROUP_DIM),
        pool_weight,
        preferred_element_type=jnp.float32,
    )
    pooled = (
        (pooled * pool_scale.reshape(GROUPS, GROUP_DIM)).astype(jnp.bfloat16).reshape(tok_rows, -1)
    )
    return pooled


def layer_kernel(n_tp, cuts, rcuts, pool_ref, pw_ref, scale_ref, ow_ref, resid_ref, mgain_ref, fgain_ref,
                 pgain_ref, routes_ref, rweight_ref, wg_ref, wu_ref, wd_ref, out_ref,
                 pool, rows_in, pw, residual, pooled, mix,
                 every, metas, picks, weights, held, wg, wu, wd,
                 work, from_core, za, zb, ya, yb,
                 psend, precv, hsend, hrecv, fsem,
                 send, recv, msend, mrecv, wsem,
                 csend, crecv, asend, arecv, bsend, brecv, ysend, yrecv, own):
    grp, sp, tp = coords()
    yy, core = sp // 2, sp % 2
    yo = 1 - yy
    y_other = yo * 2 + core
    c_other = yy * 2 + (1 - core)
    tok, width = residual.shape
    local_experts, buffers = wg_ref.shape[0], wg.shape[0]
    slots = local_experts * SLOT
    chunk = width
    others = [(a, b) for a in range(4) for b in range(n_tp) if (a, b) != (0, 0)]

    def weight_copies(e):
        at = lax.rem(e, buffers)
        return [pltpu.make_async_copy(w.at[e], buf.at[at], wsem.at[i, at])
                for i, (w, buf) in enumerate(((wg_ref, wg), (wu_ref, wu), (wd_ref, wd)))]

    loads = [pltpu.make_async_copy(a, b, fsem.at[i]) for i, (a, b) in enumerate(
        ((pool_ref, pool), (pw_ref, pw), (resid_ref, residual)))]
    blocks = [(y, t) for y in range(2) for t in range(n_tp)]
    loads += [pltpu.make_async_copy(ow_ref.at[pl.ds(i * tok, tok)], from_core.at[y, t], fsem.at[3 + i])
              for i, (y, t) in enumerate(blocks)]
    for c in loads:
        c.start()
    barrier = pltpu.get_barrier_semaphore()
    for by in others:
        target = (grp, (sp + by[0]) % 4, (tp + by[1]) % n_tp)
        pl.semaphore_signal(barrier, inc=1, device_id=target, device_id_type=MESH)
    metas[sp, tp] = token_meta(routes_ref, rweight_ref, local_experts * 4)
    loads[0].wait()
    pl.semaphore_wait(barrier, len(others))

    def meta_copy(number, by):
        return pltpu.make_async_remote_copy(
            src_ref=metas.at[sp, tp], dst_ref=metas.at[sp, tp],
            send_sem=msend.at[number], recv_sem=mrecv.at[number],
            device_id=(grp, (sp + by[0]) % 4, (tp + by[1]) % n_tp), device_id_type=MESH)

    seg_rows, reach = pool.shape[0], SLOT
    first = tp == 0
    rest = tp > 0
    has_next = sp + 1 < 4

    half = tok // 2
    rows_h = [pl.ds(h * half, half) for h in range(2)]

    def ends(h, to, whole, chan):
        if h:
            at = pl.multiple_of(to * tok + half, half)
            return pool.at[pl.ds(at, half)], rows_in.at[chan, pl.ds(reach + half, half)]
        if whole:
            at = pl.multiple_of(to * tok - reach, reach)
            return pool.at[pl.ds(at, half + reach)], rows_in.at[chan, pl.ds(0, half + reach)]
        return pool.at[pl.ds(0, half)], rows_in.at[chan, pl.ds(reach, half)]

    def spread(h, by, whole):
        to = (tp + by) % n_tp
        src, dst = ends(h, to, whole, tp)
        return pltpu.make_async_remote_copy(
            src_ref=src, dst_ref=dst, send_sem=psend.at[h, by], recv_sem=precv.at[h, tp],
            device_id=(grp, sp, to), device_id_type=MESH)

    def landed(h, chan, whole):
        src, dst = ends(h, 1 if whole else 0, whole, chan)
        return pltpu.make_async_remote_copy(
            src_ref=src, dst_ref=dst, send_sem=psend.at[h, 0], recv_sem=precv.at[h, chan],
            device_id=(grp, sp, tp), device_id_type=MESH)

    def halo(chan):
        return pltpu.make_async_remote_copy(
            src_ref=pool.at[pl.ds(seg_rows - reach, reach)],
            dst_ref=rows_in.at[chan, pl.ds(0, reach)],
            send_sem=hsend.at[0], recv_sem=hrecv.at[chan],
            device_id=(grp, sp + 1, 0), device_id_type=MESH)

    def kept(h, whole):
        src, dst = ends(h, tp, whole, tp)
        return pltpu.make_async_copy(src, dst, own.at[h, 1])

    def each_spread(act):
        for h in range(2):
            for by in range(n_tp - 1, 0, -1):
                for to in (tp + by, tp - by):
                    rank = lax.rem(to - tp + n_tp, n_tp)
                    good = jnp.logical_and(to >= 0, to < n_tp)
                    if h:
                        pl.when(good)(lambda r=rank: act(spread(1, r, True)))
                        continue
                    pl.when(jnp.logical_and(good, to == 0))(lambda r=rank: act(spread(0, r, False)))
                    pl.when(jnp.logical_and(good, to > 0))(lambda r=rank: act(spread(0, r, True)))

    pl.when(has_next)(lambda: halo(tp).start())
    each_spread(lambda c: c.start())
    pl.when(first)(lambda: kept(0, False).start())
    pl.when(rest)(lambda: kept(0, True).start())
    kept(1, True).start()
    for number, by in enumerate(others):
        meta_copy(number, by).start()
    for e in range(min(buffers, local_experts)):
        for c in weight_copies(e):
            c.start()

    @pl.when(jnp.logical_and(first, sp == 0))
    def _():
        for chan in range(n_tp):
            rows_in[chan, pl.ds(0, reach)] = jnp.zeros((reach, rows_in.shape[2]), rows_in.dtype)

    start = (sp * n_tp + tp) * tok

    def pool_group(h, group, window):
        mine = tp == group
        if h:
            pl.when(mine)(lambda: kept(1, True).wait())
            pl.when(tp != group)(lambda: landed(1, group, True).wait_recv())
        else:
            pl.when(mine)(lambda: kept(0, group > 0).wait())
            if group:
                pl.when(first)(lambda: landed(0, group, False).wait_recv())
                pl.when(jnp.logical_and(rest, tp != group))(lambda: landed(0, group, True).wait_recv())
            else:
                pl.when(rest)(lambda: landed(0, 0, True).wait_recv())
            pl.when(jnp.logical_and(first, sp > 0))(lambda: halo(group).wait_recv())
        values = rows_in[group, pl.ds(h * half, half + reach)].astype(jnp.float32)
        total = values
        span = 1
        while span < window:
            total = total + jnp.concatenate([total[:span], total[:-span]], axis=0)
            span *= 2
        count = start + h * half + lax.broadcasted_iota(jnp.int32, (half, values.shape[1]), 0) + 1
        divisor = jnp.minimum(count, window).astype(jnp.float32)
        mixed = (total[reach:] / divisor - values[reach:]).astype(jnp.bfloat16)
        product = jnp.dot(mixed, pw[group], preferred_element_type=jnp.float32)
        cols = slice(group * GROUP_DIM, (group + 1) * GROUP_DIM)
        pooled[rows_h[h], cols] = (product * scale_ref[:, cols]).astype(jnp.bfloat16)

    def pool_half(h):
        if h == 0:
            loads[1].wait()
        for group, window in enumerate(pool_windows):
            pool_group(h, group, window)
        if h == 0:
            for c in loads[2:]:
                c.wait()

        def project(i, carry):
            at = pl.ds(pl.multiple_of(i * width, width), width)
            mix[rows_h[h], at] = jnp.dot(
                pooled[rows_h[h]], from_core[:, :, :, at].reshape(pooled.shape[1], width),
                preferred_element_type=jnp.float32)
            return carry

        project(0, 0)

    def norm_rows(part):
        begin, count = cuts[part][:2]

        def body(i, carry):
            at = pl.ds(pl.multiple_of(begin + i * SLOT, SLOT), SLOT)
            after = residual[at].astype(jnp.float32) + rms_scale(mix[at], mgain_ref[...])
            after = after.astype(jnp.bfloat16)
            residual[at] = after
            every[sp, tp, at] = rms_scale(after.astype(jnp.float32), fgain_ref[...]).astype(jnp.bfloat16)
            return carry

        lax.fori_loop(0, count // SLOT, body, 0)

    def copy(s, t, part, way):
        target = [(grp, sp, tp + 1), (grp, sp, tp - 1), (grp, y_other, tp), (grp, c_other, tp)][way]
        first, count = cuts[part][:2]
        piece = every.at[s, t, pl.ds(first, count)]
        return pltpu.make_async_remote_copy(
            src_ref=piece, dst_ref=piece,
            send_sem=send.at[s, t, part, way], recv_sem=recv.at[s, t, part],
            device_id=target, device_id_type=MESH)

    def arrived(s, t, part):
        copy(s, t, part, 3).wait_recv()

    def allowed(cond, way):
        if way == 0:
            return jnp.logical_and(cond, tp + 1 < n_tp)
        if way == 1:
            return jnp.logical_and(cond, tp > 0)
        return cond

    def push(cond, s, t, part, way):
        pl.when(allowed(cond, way))(lambda: copy(s, t, part, way).start())

    def source_rows(s, t):
        return pl.ds(pl.multiple_of((t * 4 + s) * SLOT, SLOT), SLOT)

    half = tok // 2
    rows_h = [pl.ds(h * half, half) for h in range(2)]
    parts_h = [[p for p, c in enumerate(cuts) if c[2] == h] for h in range(2)]
    rparts_h = [[p for p, c in enumerate(rcuts) if c[2] == h] for h in range(2)]

    def select(h, s, t):
        slot = lax.broadcasted_iota(jnp.int32, (slots, half), 0).astype(jnp.float32)
        base = (sp * slots).astype(jnp.float32)
        meta = metas[s, t][:, h * half : (h + 1) * half]
        pick = jnp.zeros((slots, half), jnp.float32)
        weight = jnp.zeros((slots, half), jnp.float32)
        for k in range(TOP):
            hit = (meta[k : k + 1] - base) == slot
            pick = pick + jnp.where(hit, 1.0, 0.0)
            weight = weight + jnp.where(hit, meta[TOP + k : TOP + k + 1], 0.0)
        weight = jnp.broadcast_to(jnp.sum(weight, axis=1, keepdims=True), (slots, 128))
        pick = pick.astype(jnp.bfloat16)
        picks[h, s, t] = pick
        for e in range(local_experts):
            weights[h, e, source_rows(s, t)] = weight[e * SLOT : (e + 1) * SLOT]

        def body(i, carry):
            at = pl.ds(pl.multiple_of(i * chunk, chunk), chunk)
            got = jnp.dot(pick, every[s, t, rows_h[h], at], preferred_element_type=jnp.float32)
            got = got.astype(jnp.bfloat16)
            for e in range(local_experts):
                held[h, e, source_rows(s, t), at] = got[e * SLOT : (e + 1) * SLOT]
            return carry

        lax.fori_loop(0, width // chunk, body, 0)

    yes = tp >= 0
    far_core = yo * 2 + (1 - core)

    def own_way(h, way):
        for p in parts_h[h]:
            push(yes, sp, tp, p, way)

    def crossed(h):
        p = parts_h[h][0]
        arrived(y_other, tp, p)
        push(yes, y_other, tp, p, 0)
        push(yes, y_other, tp, p, 1)
        push(yes, y_other, tp, p, 3)

    by_dist = [((tp, yes),)] + [
        ((tp - d, tp >= d), (tp + d, tp + d < n_tp)) for d in range(1, n_tp)]

    def sides(dist):
        return by_dist[dist]

    def over_y(h, dist, p, side):
        t, cond = sides(dist)[side]
        pl.when(cond)(functools.partial(arrived, y_other, t, p))
        push(cond, y_other, t, p, 3)

    def select_from(h, s, dist, side):
        t, cond = sides(dist)[side]
        pl.when(cond)(functools.partial(select, h, s, t))

    def cross(h, s, t):
        for p in parts_h[h]:
            arrived(s, t, p)
        select(h, s, t)

    def over_core(h, s, dist, side):
        t, cond = sides(dist)[side]
        pl.when(cond)(functools.partial(cross, h, s, t))

    def along(h, dist, p, s, side):
        t, cond = sides(dist)[side]
        pl.when(cond)(functools.partial(arrived, s, t, p))
        push(cond, s, t, p, side)
        if p != parts_h[h][0]:
            push(cond, s, t, p, 2)
        push(cond, s, t, p, 3)

    def sent_all(h):
        head, tail = parts_h[h][0], parts_h[h][1:]
        sent = [(yes, sp, tp, p, way) for p in parts_h[h] for way in range(4)]
        sent += [(yes, y_other, tp, head, way) for way in (0, 1, 3)]
        sent += [(yes, y_other, tp, p, 3) for p in tail]
        for dist in range(1, n_tp):
            for side, (t, cond) in enumerate(sides(dist)):
                sent += [(cond, sp, t, p, way) for p in tail for way in (side, 2, 3)]
                sent += [(cond, s, t, head, way) for s in (sp, y_other) for way in (side, 3)]
                sent += [(cond, y_other, t, p, 3) for p in tail]
        for cond, s, t, p, way in sent:
            pl.when(allowed(cond, way))(lambda s=s, t=t, p=p, way=way: copy(s, t, p, way).wait_send())

    def use_expert(h, e, at_rows):
        at = lax.rem(e, buffers)
        rows = held[h, e, at_rows]
        gate_pre = jnp.dot(rows, wg[at], preferred_element_type=jnp.float32)
        upward = jnp.dot(rows, wu[at], preferred_element_type=jnp.float32)
        scale = jnp.concatenate([weights[h, e, at_rows]] * (gate_pre.shape[1] // 128), axis=1)
        activated = (clamped_unit(gate_pre, upward) * scale).astype(jnp.bfloat16)
        term = jnp.dot(activated, wd[at], preferred_element_type=jnp.float32)
        held[h, e, at_rows] = term.astype(jnp.bfloat16)

    def begin_weights(e, cond):
        @pl.when(cond)
        def _():
            for c in weight_copies(e):
                c.start()

    def end_weights(e, cond):
        @pl.when(cond)
        def _():
            for c in weight_copies(e):
                c.wait()

    def experts(h, far, between):
        pair = n_tp // 2
        group = tp // pair
        group = 1 - group if far else group
        count = pair * 4 * SLOT
        at_rows = pl.ds(pl.multiple_of(group * count, count), count)
        fresh = h == 0 and not far

        def body(j, carry):
            e = local_experts - 1 - j if far else j
            end_weights(e, j >= (0 if fresh else buffers))
            use_expert(h, e, at_rows)
            later = e - buffers if far else e + buffers
            begin_weights(later, jnp.logical_and(later >= 0, later < local_experts))
            for number, steps in between:
                pl.when(j == number)(functools.partial(run, steps))
            return carry

        lax.fori_loop(0, local_experts, body, 0)

    def combined(h, s, t, at):
        term = held[h, :, source_rows(s, t), at].reshape(slots, chunk)
        return lax.dot_general(picks[h, s, t], term, (((0,), (0,)), ((), ())),
                               preferred_element_type=jnp.float32)

    rows_of = [pl.ds(c[0], c[1]) for c in rcuts]
    ups, downs = (grp, sp, tp + 1), (grp, sp, tp - 1)
    up_ok, down_ok = tp + 1 < n_tp, tp > 0

    def remote(src, dst, s_sem, r_sem, target):
        return pltpu.make_async_remote_copy(
            src_ref=src, dst_ref=dst, send_sem=s_sem, recv_sem=r_sem,
            device_id=target, device_id_type=MESH)

    def core_copy(h, y, t):
        return remote(every.at[y * 2 + (1 - core), t, rows_h[h]], from_core.at[y, t, rows_h[h]],
                      csend.at[h, y, t], crecv.at[h, y, t], (grp, c_other, tp))

    def combine_away(h, y, t):
        s = y * 2 + (1 - core)

        def body(i, carry):
            at = pl.ds(pl.multiple_of(i * chunk, chunk), chunk)
            every[s, t, rows_h[h], at] = combined(h, s, t, at).astype(jnp.bfloat16)
            return carry

        lax.fori_loop(0, width // chunk, body, 0)
        core_copy(h, y, t).start()

    order = []
    for dist in range(n_tp - 1, -1, -1):
        for side in (1, -1) if dist else (1,):
            t = tp + side * dist
            order.append((jnp.logical_and(t >= 0, t < n_tp), t, side, (dist, int(side < 0))))

    def y_copy_b(p, t):
        rows = rows_of[p]
        return remote(work.at[yo, t, rows], yb.at[t, rows], ysend.at[p, t], yrecv.at[p, t],
                      (grp, y_other, tp))

    def y_copy_a(h):
        p = rparts_h[h][0]
        return remote(work.at[yo, tp, rows_of[p]], ya.at[h, pl.ds(0, rcuts[p][1])], ysend.at[p, 0], yrecv.at[p, 0],
                      (grp, y_other, tp))

    def local(h, y, t):
        s = y * 2 + core
        core_copy(h, y, t).wait_recv()

        def body(i, carry):
            at = pl.ds(pl.multiple_of(i * chunk, chunk), chunk)
            both = combined(h, s, t, at) + from_core[y, t, rows_h[h], at].astype(jnp.float32)
            work[y, t, rows_h[h], at] = both.astype(jnp.bfloat16)
            return carry

        lax.fori_loop(0, width // chunk, body, 0)

    def z_ends(p, y, t, slot):
        rows, h = rows_of[p], rcuts[p][2]
        if p == rparts_h[h][0]:
            return work.at[y, t, rows], za.at[h, y, slot, pl.ds(0, rcuts[p][1])], asend.at[h, y, t], arecv.at[h, y, slot]
        return work.at[y, t, rows], zb.at[slot, rows], bsend.at[p, t], brecv.at[p, slot]

    def z_copy(p, y, t, side):
        if side == 1:
            slot, target = t, ups
        else:
            slot, target = jnp.where(t == tp - 1, n_tp, t), downs
        return remote(*z_ends(p, y, t, slot), target)

    def take_z(p, y, t, slot):
        remote(*z_ends(p, y, t, slot), ups).wait_recv()
        dst, src = z_ends(p, y, t, slot)[:2]
        add_into(dst, src)

    def z_step(p, y, t, side):
        inner = tp > 0 if side == 1 else tp + 1 < n_tp
        pl.when(inner)(lambda: take_z(p, y, t, t))
        z_copy(p, y, t, side).start()

    def z_end(p, y):
        pl.when(down_ok)(lambda: take_z(p, y, tp, tp))
        pl.when(up_ok)(lambda: take_z(p, y, tp, n_tp))

    def aways(h, y, want):
        for ok, t, side, dist in order:
            if dist == want:
                pl.when(ok)(functools.partial(combine_away, h, y, t))

    def send_y(h, dists):
        for ok, t, side, dist in order:
            if dist == dists:
                @pl.when(ok)
                def _(t=t):
                    local(h, yo, t)
                    for p in rparts_h[h][1:]:
                        y_copy_b(p, t).start()

    def reduce_local(h, want):
        head = rparts_h[h][0]
        for ok, t, side, dist in order:
            if dist != want:
                continue

            @pl.when(ok)
            def _(t=t, side=side, dist=dist):
                local(h, yy, t)
                if dist[0]:
                    z_step(head, yo, t, side)
                    z_step(head, yy, t, side)

    def reduce_part(p, want):
        for ok, t, side, dist in order:
            if dist != want:
                continue

            @pl.when(ok)
            def _(t=t, side=side, dist=dist):
                y_copy_b(p, t).wait_recv()
                add_into(work.at[yy, t, rows_of[p]], yb.at[t, rows_of[p]])
                if dist[0]:
                    z_step(p, yy, t, side)

    def reduce_head(h):
        head = rparts_h[h][0]
        z_end(head, yo)
        y_copy_a(h).start()
        z_end(head, yy)

    def reduce_last(h):
        head = rparts_h[h][0]
        y_copy_a(h).wait_recv()
        add_into(work.at[yy, tp, rows_of[head]], ya.at[h, pl.ds(0, rcuts[head][1])])
        finish_rows(h)

    def reduce_sent(h):
        head, tail = rparts_h[h][0], rparts_h[h][1:]
        y_copy_a(h).wait_send()
        for ok, t, side, dist in order:
            @pl.when(ok)
            def _(t=t, side=side, dist=dist):
                core_copy(h, yo, t).wait_send()
                core_copy(h, yy, t).wait_send()
                for p in tail:
                    y_copy_b(p, t).wait_send()
                if dist[0]:
                    z_copy(head, yo, t, side).wait_send()
                    z_copy(head, yy, t, side).wait_send()
                    for p in tail:
                        z_copy(p, yy, t, side).wait_send()

    def finish_rows(h):
        def body(i, carry):
            at = pl.ds(pl.multiple_of(h * half + i * SLOT, SLOT), SLOT)
            total = work[yy, tp, at].astype(jnp.float32)
            done = residual[at].astype(jnp.float32) + rms_scale(total, pgain_ref[...])
            out_ref[at] = done.astype(out_ref.dtype)
            return carry

        lax.fori_loop(0, half // SLOT, body, 0)

    def step(kind, h, *at):
        if kind == "P":
            pool_half(h)
        elif kind == "N":
            norm_rows(at[0])
        elif kind == "OZ":
            push(yes, sp, tp, at[0], at[1])
        elif kind == "OY":
            push(yes, sp, tp, at[0], 2)
        elif kind == "OC":
            own_way(h, 3)
        elif kind == "X":
            crossed(h)
        elif kind == "F":
            along(h, at[0], at[1], sp if at[2] == "own" else y_other, at[3])
        elif kind == "SA":
            select_from(h, sp, *at)
        elif kind == "YA":
            over_y(h, *at)
        elif kind == "YS":
            select_from(h, y_other, *at)
        elif kind == "CO":
            over_core(h, c_other, *at)
        elif kind == "FA":
            over_core(h, far_core, *at)
        elif kind == "W":
            sent_all(h)
        elif kind == "WP":
            pl.when(has_next)(lambda: halo(tp).wait_send())
            each_spread(lambda c: c.wait_send())
        elif kind == "WR":
            reduce_sent(h)
        elif kind == "M":
            for number, by in enumerate(others):
                meta_copy(number, by).wait()
        elif kind == "AW":
            aways(h, yo if at[0] == "yo" else yy, at[1:])
        elif kind == "SY":
            send_y(h, at)
        elif kind == "RL":
            reduce_local(h, at)
        elif kind == "RT":
            reduce_part(at[1], (at[0], at[2]))
        elif kind == "RH":
            reduce_head(h)
        elif kind == "RP":
            z_end(at[0], yy)
        elif kind == "RF":
            reduce_last(h)

    def run(steps):
        for one in steps:
            step(*one)

    todo, waited = [], set()
    for one in ORDER:
        if one[0] in ("SA", "YS", "CO", "FA") and "M" not in waited:
            waited.add("M")
            todo.append(("M", 0))
        todo.append(one)
    late = [i for i, one in enumerate(todo) if one[:2] == ("RT", 1)]
    todo.insert(late[len(late) * 2 // 3] + 1, ("W", 1))
    todo.insert(late[len(late) // 3] + 1, ("W", 0))
    todo.insert(late[0] + 1, ("WP", 0))
    todo.insert(todo.index(("RF", 0)) + 1, ("WR", 0))
    while todo:
        one = todo.pop(0)
        if one[0] != "E":
            step(*one)
            continue
        h, far, between, seen = one[1], one[2] > 0, [], 0
        while seen < local_experts - 1:
            one = todo.pop(0)
            if one[0] == "E":
                seen += 1
            elif between and between[-1][0] == seen:
                between[-1][1].append(one)
            else:
                between.append((seen, [one]))
        experts(h, far, between)
    reduce_sent(1)


def cut_rows(halves):
    cuts, at = [], 0
    for h, counts in enumerate(halves):
        for count in counts:
            cuts.append((at, count, h))
            at += count
    return tuple(cuts)


def token_meta(routes_ref, rweight_ref, n_experts):
    tok = routes_ref.shape[1]
    expert = lax.broadcasted_iota(jnp.int32, (n_experts, tok), 0)
    hits = [jnp.where(expert == routes_ref[k : k + 1], 1.0, 0.0) for k in range(TOP)]
    earlier = (lax.broadcasted_iota(jnp.int32, (tok, tok), 0)
               < lax.broadcasted_iota(jnp.int32, (tok, tok), 1))
    earlier = jnp.where(earlier, 1.0, 0.0).astype(jnp.bfloat16)
    before = jnp.dot(sum(hits).astype(jnp.bfloat16), earlier, preferred_element_type=jnp.float32)
    line = lax.broadcasted_iota(jnp.int32, (2 * TOP, tok), 0)
    meta = jnp.zeros((2 * TOP, tok), jnp.float32)
    for k in range(TOP):
        rank = jnp.sum(hits[k] * before, axis=0, keepdims=True)
        place = routes_ref[k : k + 1].astype(jnp.float32) * SLOT + rank
        meta = jnp.where(line == k, place, meta)
        meta = jnp.where(line == TOP + k, rweight_ref[k : k + 1], meta)
    return meta


def add_into(dst, src):
    rows = dst.shape[0]
    strip = 16

    def body(i, carry):
        at = pl.ds(pl.multiple_of(i * strip, strip), strip)
        dst[at] = (dst[at].astype(jnp.float32) + src[at].astype(jnp.float32)).astype(dst.dtype)
        return carry

    lax.fori_loop(0, rows // strip, body, 0)


def fused_layer(resid_in, pool_input, pool_weight, pool_scale, out_weight, mix_gain, ffn_gain,
                w_gate, w_up, w_down, routes, route_weight, post_gain):
    n_tp = lax.axis_size("tp")
    tok, width = resid_in.shape
    local_experts, _, hidden = w_gate.shape
    cuts, rcuts = cut_rows(HALVES), cut_rows(BACK)
    parts, rparts = len(cuts), len(rcuts)
    heads = [counts[0] for counts in BACK]
    vmem, hbm = pl.BlockSpec(memory_space=pltpu.VMEM), pl.BlockSpec(memory_space=pl.ANY)
    kind = resid_in.dtype
    slots, buffers = local_experts * SLOT, min(4, local_experts)
    channels = pool_input.shape[1]
    dma = pltpu.SemaphoreType.DMA
    return pl.pallas_call(
        functools.partial(layer_kernel, n_tp, cuts, rcuts),
        out_shape=jax.ShapeDtypeStruct((tok, width), kind),
        in_specs=[hbm, hbm, vmem, hbm, hbm, vmem, vmem, vmem, vmem, vmem, hbm, hbm, hbm],
        out_specs=vmem,
        scratch_shapes=[
            pltpu.VMEM(pool_input.shape, kind),
            pltpu.VMEM((n_tp, tok + SLOT, channels), kind),
            pltpu.VMEM(pool_weight.shape, kind),
            pltpu.VMEM((tok, width), kind),
            pltpu.VMEM((tok, n_tp * channels), kind),
            pltpu.VMEM((tok, width), jnp.float32),
            pltpu.VMEM((4, n_tp, tok, width), kind),
            pltpu.VMEM((4, n_tp, 2 * TOP, tok), jnp.float32),
            pltpu.VMEM((2, 4, n_tp, slots, tok // 2), kind),
            pltpu.VMEM((2, local_experts, 4 * n_tp * SLOT, 128), jnp.float32),
            pltpu.VMEM((2, local_experts, 4 * n_tp * SLOT, width), kind),
            pltpu.VMEM((buffers, width, hidden), kind),
            pltpu.VMEM((buffers, width, hidden), kind),
            pltpu.VMEM((buffers, hidden, width), kind),
            pltpu.VMEM((2, n_tp, tok, width), kind),
            pltpu.VMEM((2, n_tp, tok, width), kind),
            pltpu.VMEM((2, 2, n_tp + 1, max(heads), width), kind),
            pltpu.VMEM((n_tp + 1, tok, width), kind),
            pltpu.VMEM((2, max(heads), width), kind),
            pltpu.VMEM((n_tp, tok, width), kind),
            dma((2, n_tp)),
            dma((2, n_tp)),
            dma((1,)),
            dma((n_tp,)),
            dma((3 + 2 * n_tp,)),
            dma((4, n_tp, parts, 4)),
            dma((4, n_tp, parts)),
            dma((4 * n_tp - 1,)),
            dma((4 * n_tp - 1,)),
            dma((3, buffers)),
            dma((2, 2, n_tp)),
            dma((2, 2, n_tp)),
            dma((2, 2, n_tp)),
            dma((2, 2, n_tp + 1)),
            dma((rparts, n_tp)),
            dma((rparts, n_tp + 1)),
            dma((rparts, n_tp)),
            dma((rparts, n_tp)),
            dma((2, max(2, n_tp))),
        ],
        compiler_params=pltpu.CompilerParams(
            collective_id=0, has_side_effects=True, vmem_limit_bytes=60 * 2**20
        ),
        name="fused_layer",
    )(pool_input, pool_weight, pool_scale[None], out_weight, resid_in, mix_gain[None], ffn_gain[None],
      post_gain[None], routes.T, route_weight.T, w_gate, w_up, w_down)


def per_device(
    resid_in,
    pool_input,
    pool_weight,
    pool_scale,
    out_weight,
    mix_gain,
    ffn_gain,
    w_gate,
    w_up,
    w_down,
    routes,
    route_weight,
    post_gain,
):
    n_sp = lax.axis_size("sp")
    n_tp = lax.axis_size("tp")
    seg_rows, channels = pool_input.shape
    tok_rows, width = resid_in.shape
    if (
        n_sp == 4
        and n_tp == GROUPS
        and channels == GROUP_DIM
        and seg_rows == n_tp * 128
        and tok_rows == 128
        and w_gate.shape[2] <= 256
        and w_gate.shape[0] <= 8
        and width <= 2048
        and out_weight.shape[0] == 2 * n_tp * tok_rows
    ):
        return fused_layer(resid_in, pool_input, pool_weight, pool_scale, out_weight, mix_gain,
                           ffn_gain, w_gate, w_up, w_down, routes, route_weight, post_gain)
    pooled = routed_pool(pool_input, pool_weight, pool_scale)
    mix_out = jnp.dot(pooled, out_weight, preferred_element_type=jnp.float32)
    residual = (resid_in.astype(jnp.float32) + rms_scale(mix_out, mix_gain)).astype(jnp.bfloat16)
    normed = rms_scale(residual.astype(jnp.float32), ffn_gain).astype(jnp.bfloat16)
    local_experts = w_gate.shape[0]
    n_experts = local_experts * n_sp
    slot_total = n_experts * CAP
    flat_route = routes.reshape(-1)
    onehot = (flat_route[:, None] == lax.iota(jnp.int32, n_experts)[None, :]).astype(jnp.int32)
    slot_rank = jnp.sum((jnp.cumsum(onehot, axis=0) - onehot) * onehot, axis=1)
    slot_index = flat_route * CAP + slot_rank
    picker = slot_index[:, None] == lax.iota(jnp.int32, slot_total)[None, :]
    picker_rows = picker.astype(jnp.bfloat16)
    token_pick = jnp.sum(
        picker.reshape(tok_rows, TOP, slot_total).astype(jnp.float32), axis=1
    ).astype(jnp.bfloat16)
    buffer = lax.dot_general(
        token_pick, normed, (((0,), (0,)), ((), ())), preferred_element_type=jnp.float32
    )
    outgoing = buffer.astype(jnp.bfloat16).reshape(n_sp, local_experts * CAP, width)
    at_owner = lax.all_to_all(outgoing, "sp", split_axis=0, concat_axis=0, tiled=True)
    arrived = lax.all_gather(at_owner[:, None], "tp", axis=1, tiled=True)
    arrived = arrived.reshape(n_sp, n_tp, local_experts, CAP, width)
    gate_pre = jnp.einsum("sklcd,ldf->sklcf", arrived, w_gate, preferred_element_type=jnp.float32)
    upward = jnp.einsum("sklcd,ldf->sklcf", arrived, w_up, preferred_element_type=jnp.float32)
    activated = clamped_unit(gate_pre, upward).astype(jnp.bfloat16)
    terms = jnp.einsum("sklcf,lfd->kslcd", activated, w_down, preferred_element_type=jnp.float32)
    summed = lax.psum_scatter(
        terms.reshape(1 * lax.axis_size("tp"), n_sp, local_experts * CAP, width).astype(
            jnp.bfloat16
        ),
        "tp",
        scatter_dimension=0,
        tiled=True,
    ).astype(jnp.float32)
    results = summed[0].astype(jnp.bfloat16)
    returned = lax.all_to_all(results, "sp", split_axis=0, concat_axis=0, tiled=True).reshape(
        slot_total, width
    )
    gathered = jnp.dot(picker_rows, returned, preferred_element_type=jnp.float32)
    expert_mix = jnp.sum(gathered.reshape(tok_rows, TOP, width) * route_weight[:, :, None], axis=1)
    return (residual.astype(jnp.float32) + rms_scale(expert_mix, post_gain)).astype(jnp.bfloat16)


def solution(mesh):
    in_specs = (
        P(("grp", "sp", "tp"), None),
        P(("grp", "sp"), "tp"),
        P(),
        P(),
        P(),
        P(),
        P(),
        P("sp", None, "tp"),
        P("sp", None, "tp"),
        P("sp", "tp", None),
        P(("grp", "sp", "tp"), None),
        P(("grp", "sp", "tp"), None),
        P(),
    )
    out_specs = P(("grp", "sp", "tp"), None)
    return jax.shard_map(
        per_device, mesh=mesh, in_specs=in_specs, out_specs=out_specs, check_vma=False
    )
```
